256 devices in a mesh: sp: 16 (over y, x), tp: 16 (over z, core).
Axes of the slice: x: 4, y: 4, z: 8, core: 2. Of those that a mesh axis runs over, the one named last changes fastest.
Arguments:
- mix_in: bfloat16 [16384, 2048], P('sp', 'tp'), may hold values from -8 to 8
- gate_in: bfloat16 [16384, 2048], P('sp', 'tp'), may hold values from -6 to 6
- conv_w: float32 [4, 2048], P(None, 'tp'), may hold values from -3 to 3
- conv_b: float32 [2048], P('tp'), may hold values from -3 to 3
- decay_param: float32 [2, 2048], P(None, 'tp')
- recur_gate: float32 [2, 32, 64, 64], P(None, 'tp'), may hold values from -0.75 to 0.75
- recur_bias: float32 [2, 2048], P(None, 'tp'), may hold values from -4 to 4
- input_gate: float32 [2, 32, 64, 64], P(None, 'tp'), may hold values from -0.75 to 0.75
- input_bias: float32 [2, 2048], P(None, 'tp'), may hold values from -4 to 4
- residual: bfloat16 [16384, 2048], P(('sp', 'tp')), may hold values from -6 to 6
- out_proj: bfloat16 [2048, 2048], replicated, may hold values from -0.125 to 0.125
- norm_gain: float32 [3, 2048], replicated, may hold values from 0.1 to 1.9
- routes: int32 [16384, 2], P('sp'), may hold values from 0 to 15, all different within a row; in each aligned block of 64 rows (0 to 63, 64 to 127, ...) at most 16 rows name the same one
- route_wt: float32 [16384, 2], P('sp'), may hold values from 0.1 to 1
- exp_gate: bfloat16 [16, 2048, 1024], P('sp', None, 'tp'), may hold values from -0.125 to 0.125
- exp_up: bfloat16 [16, 2048, 1024], P('sp', None, 'tp'), may hold values from -0.125 to 0.125
- exp_down: bfloat16 [16, 1024, 2048], P('sp', 'tp'), may hold values from -0.1875 to 0.1875
Outputs:
- final: bfloat16 [16384, 2048], P(('sp', 'tp'))
The draws below stay inside these ranges and needn't reach their ends.
Inputs may be any that keep to these rules, and one draw needn't show every extreme that they name: `routes`: in each aligned block of 64 tokens (the rows of one device in the expert layer) no expert is named more than 16 times, and in some block some expert exactly 16 times; a token's 2 experts differ.
All inputs are finite; a program needn't handle non-finite values.
Results may differ from the reference program's by a relative error of at most 0.008.
Values may be sent and summed in bfloat16 or wider, within the bound.
No kernel may reach another device: no remote copies, remote signals or barrier semaphores. Data moves between devices by JAX's collectives and lax.ppermute only.
A program may use at most 128 MiB of HBM per device.

```python
import math
import jax
import jax.numpy as jnp
import numpy as np
from jax import lax

D = 2048
WIDTH = 2048
HEAD = 64
FF = 1024
EXPERTS = 16
TOPK = 2
SEQ_DEV = 1024
HEADS = 32
SEQ = 16384
ROWS = 64
CAP = 16


def draw_decay_param(key, part):
    pick_key, slow_key, fast_key = jax.random.split(jax.random.fold_in(key, 17), 3)
    slow_share = 0.5
    chooser = jax.random.uniform(pick_key, (2, WIDTH), jnp.float32)
    slow_values = math.log(SEQ) + jax.random.uniform(slow_key, (2, WIDTH), jnp.float32, 0.7, 1.7)
    fast_values = jax.random.uniform(fast_key, (2, WIDTH), jnp.float32, 3.5, 5.0)
    return jnp.where(chooser < slow_share, slow_values, fast_values).astype(jnp.float32)


def draw_conv_w(key, part):
    tap_key = jax.random.fold_in(key, 31)
    values = jax.random.normal(tap_key, (4, WIDTH), jnp.float32)
    tap_scale = jnp.array([0.4, 0.4, 0.4, 1.2], jnp.float32)[:, None]
    return jnp.clip(values * tap_scale, -3.0, 3.0).astype(jnp.float32)


def draw_mix_in(key, part):
    value_key, scale_key, offset_key = jax.random.split(jax.random.fold_in(key, 23), 3)
    values = jax.random.normal(value_key, (SEQ, WIDTH), jnp.float32)
    spread = 0.8
    position = jnp.arange(SEQ, dtype=jnp.int32) % SEQ_DEV
    at_ends = jnp.logical_or(position < 2, position >= SEQ_DEV - 2)
    values = values * jnp.where(at_ends, 3.0, 1.0)[:, None]
    scales = jnp.exp(jax.random.uniform(scale_key, (SEQ // 64, 1, WIDTH), jnp.float32, -spread, spread))
    shaped = (values.reshape(SEQ // 64, 64, WIDTH) * scales).reshape(SEQ, WIDTH)
    offsets = jax.random.uniform(offset_key, (SEQ // SEQ_DEV, 1, WIDTH), jnp.float32, -1.5, 1.5)
    shifted = (shaped.reshape(SEQ // SEQ_DEV, SEQ_DEV, WIDTH) + offsets).reshape(SEQ, WIDTH)
    return jnp.clip(shifted, -8.0, 8.0).astype(jnp.bfloat16)


def level_of(key, extent, shards, smallest, high):
    loudness, own = 1.0, jax.random.fold_in(key, 6)
    for dim, parts in shards:
        draws = jnp.exp(jax.random.uniform(jax.random.fold_in(own, dim), (parts,), jnp.float32, smallest / len(shards), high / len(shards)))
        loudness = loudness * jnp.repeat(draws, extent[dim] // parts).reshape([-1 if axis == dim else 1 for axis in range(len(extent))])
    return loudness


def deal_out(stream_key, own, number, rows, count, top, reach, lean):
    sequence = jax.random.permutation(stream_key, count)
    crowded, ordinary = load_shares(count, rows * top, reach, lean, True), load_shares(count, rows * top, reach, lean, False)
    places = jnp.arange(count)

    def named(tallies, rotation):
        used = int((tallies > 0).sum())
        fixed = max(1, used // 4)
        passed = fixed + (places - fixed + rotation * (used - fixed)) % max(1, count - fixed)
        return jnp.zeros((count,), jnp.int32).at[sequence[jnp.where(places < fixed, places, passed)]].set(jnp.asarray(tallies, jnp.int32))

    tallies = jnp.where(number % 4 == 0, named(crowded, number // 4), named(ordinary, number - number // 4 - 1))
    mixed = jax.random.permutation(jax.random.fold_in(own, 3), count)
    source_of, sink = mixed[0:count // 2 * 2:2], mixed[1:count // 2 * 2:2]
    room = jnp.minimum(tallies[source_of] - 1, reach - tallies[sink]) // 2
    room = jnp.where((source_of == sequence[0]) | (sink == sequence[0]) | (tallies[sink] == 0), 0, jnp.maximum(room, 0))
    passed = jax.random.randint(jax.random.fold_in(own, 4), (count // 2,), 0, 1 << 20) % (room + 1)
    tallies = tallies.at[source_of].add(-passed).at[sink].add(passed)
    items = jnp.searchsorted(jnp.cumsum(tallies), jnp.arange(rows * top), side="right").astype(jnp.int32)
    table = items.reshape(top, rows).T
    table = table[jax.random.permutation(jax.random.fold_in(own, 1), rows)]
    rotation = jax.random.randint(jax.random.fold_in(own, 2), (rows, 1), 0, top)
    return jnp.take_along_axis(table, (jnp.arange(top)[None, :] + rotation) % top, axis=1)


def load_shares(count, total, most, lean, full):
    portions = [(1 << 20) // math.isqrt(standing ** lean) + 1 for standing in range(1, count + 1)]
    largest = most if full else min(most, max(-(-total // count), total * portions[0] // sum(portions)))
    least = 1 if total - largest >= count - 1 else 0
    holding, surplus = [largest] + [least] * (count - 1), total - largest - least * (count - 1)
    while surplus > 0:
        movable = [i for i in range(1, count) if holding[i] < largest] or [i for i in range(1, count) if holding[i] < most]
        pool, budget = sum([portions[i] for i in movable]), surplus
        for i in movable:
            more = min(most - holding[i], max(1, budget * portions[i] // pool), surplus)
            holding[i] = holding[i] + more
            surplus = surplus - more
    return np.array(holding)


def centred(stream_key, dims, deviation, limit, cuts=(), held_as=jnp.bfloat16):
    entries = jax.random.normal(stream_key, dims, jnp.float32) * deviation
    if len(cuts) > 0:
        entries = level_of(stream_key, dims, cuts, -0.22, 0.18) * entries
    return jnp.clip(entries, min=-limit, max=limit).astype(held_as)


def setup_inputs(seed: int = 0) -> dict:
    splits = jax.random.split(jax.random.key(seed), 18)
    mix_in = draw_mix_in(jax.random.fold_in(splits[17], 71), 0)
    gate_in = centred(splits[1], (SEQ, WIDTH), 1.0, 6.0, ((0, 16), (1, 16)))
    conv_w = draw_conv_w(jax.random.fold_in(splits[17], 71), 0)
    conv_b = centred(splits[3], (WIDTH,), 0.5, 3.0, ((0, 16),), jnp.float32)
    decay_param = draw_decay_param(jax.random.fold_in(splits[17], 71), 0)
    recur_gate = centred(splits[5], (2, HEADS, HEAD, HEAD), HEAD ** -0.5, 0.75, ((1, 16),), jnp.float32)
    recur_bias = centred(splits[6], (2, WIDTH), 1.0, 4.0, ((1, 16),), jnp.float32)
    input_gate = centred(splits[7], (2, HEADS, HEAD, HEAD), HEAD ** -0.5, 0.75, ((1, 16),), jnp.float32)
    input_bias = centred(splits[8], (2, WIDTH), 1.0, 4.0, ((1, 16),), jnp.float32)
    residual = centred(splits[9], (SEQ, D), 1.0, 6.0, ((0, 256),))
    out_proj = centred(splits[10], (WIDTH, D), WIDTH ** -0.5, 0.125)
    norm_gain = jnp.clip(1.0 + 0.18 * jax.random.normal(splits[11], (3, D), jnp.float32), 0.1, 1.9)
    routes_keys = jax.random.split(jax.random.fold_in(splits[12], 1), SEQ // ROWS)
    routes_turns = jax.random.permutation(jax.random.fold_in(splits[12], 3), SEQ // ROWS)
    routes = jax.vmap(lambda own, number: deal_out(jax.random.fold_in(splits[12], 2), own, number, ROWS, EXPERTS, TOPK, CAP, 2))(routes_keys, routes_turns).reshape((SEQ, TOPK))
    route_wt = jnp.clip(0.1 + 0.9 * jax.random.uniform(splits[13], (SEQ, TOPK), jnp.float32) ** level_of(splits[13], (SEQ, TOPK), ((0, 16),), -0.2, 0.2), 0.1, 1.0)
    exp_gate = centred(splits[14], (EXPERTS, D, FF), D ** -0.5, 0.125, ((0, 16), (2, 16)))
    exp_up = centred(splits[15], (EXPERTS, D, FF), D ** -0.5, 0.125, ((0, 16), (2, 16)))
    exp_down = centred(splits[16], (EXPERTS, FF, D), FF ** -0.5, 0.1875, ((0, 16), (1, 16)))
    return {"mix_in": mix_in, "gate_in": gate_in, "conv_w": conv_w, "conv_b": conv_b, "decay_param": decay_param, "recur_gate": recur_gate, "recur_bias": recur_bias, "input_gate": input_gate, "input_bias": input_bias, "residual": residual, "out_proj": out_proj, "norm_gain": norm_gain, "routes": routes, "route_wt": route_wt, "exp_gate": exp_gate, "exp_up": exp_up, "exp_down": exp_down}


EPSILON = 1e-06
HIGHEST_MODE = lax.Precision.HIGHEST

def norm_rows(values, gain):
    floats = values.astype(jnp.float32)
    return floats * lax.rsqrt(lax.optimization_barrier(jnp.mean(floats * floats, axis=-1, keepdims=True)) + EPSILON) * gain

def pair_join(earlier, later_pair):
    return (earlier[0] * later_pair[0], later_pair[0] * earlier[1] + later_pair[1])

def slot_table(route_rows, experts, capacity):
    row_count, top_count = route_rows.shape
    flattened = route_rows.reshape(row_count * top_count)
    matches = (flattened[:, None] == jnp.arange(experts, dtype=jnp.int32)[None, :]).astype(jnp.int32)
    earlier_hits = jnp.cumsum(matches, axis=0) - matches
    position = lax.optimization_barrier(jnp.sum(earlier_hits * matches, axis=1))
    return (flattened * capacity + position).reshape(row_count, top_count)

def coefficients(conv_out, recur_blocks, recur_bias, input_blocks, input_bias, decay_param):
    seq_len, channels = conv_out.shape
    heads, head_dim, _ = recur_blocks.shape
    blocked = conv_out.reshape(seq_len, heads, head_dim)
    recur_pre = jnp.einsum('lhi,hij->lhj', blocked, recur_blocks, precision=HIGHEST_MODE).reshape(seq_len, channels)
    input_pre = jnp.einsum('lhi,hij->lhj', blocked, input_blocks, precision=HIGHEST_MODE).reshape(seq_len, channels)
    recur_act = jax.nn.sigmoid(recur_pre + recur_bias)
    input_act = jax.nn.sigmoid(input_pre + input_bias)
    log_decay = -8.0 * recur_act * jax.nn.softplus(-decay_param)
    return (jnp.exp(log_decay), jnp.sqrt(-jnp.expm1(2.0 * log_decay)) * (input_act * conv_out))

def expert_apply(operands):
    tokens_in, gate_w, up_w, down_w = operands
    gate_act = jnp.dot(tokens_in, gate_w, preferred_element_type=jnp.float32)
    up_act = jnp.dot(tokens_in, up_w, preferred_element_type=jnp.float32)
    hidden = (jax.nn.silu(gate_act) * up_act).astype(jnp.bfloat16)
    return jnp.dot(hidden, down_w, preferred_element_type=jnp.float32).astype(jnp.bfloat16)

def reference(mix_in, gate_in, conv_w, conv_b, decay_param, recur_gate, recur_bias, input_gate, input_bias, residual, out_proj, norm_gain, routes, route_wt, exp_gate, exp_up, exp_down):
    seq_len = mix_in.shape[0]
    padded = jnp.pad(mix_in.astype(jnp.float32), ((2, 1), (0, 0)))
    conv_out = conv_b + padded[0:seq_len] * conv_w[0]
    for tap in range(1, conv_w.shape[0]):
        conv_out = conv_out + padded[tap:tap + seq_len] * conv_w[tap]
    state_sum = jnp.zeros_like(conv_out)
    for sense in range(2):
        decay, drive = coefficients(conv_out, recur_gate[sense], recur_bias[sense], input_gate[sense], input_bias[sense], decay_param[sense])
        if sense == 1:
            decay, drive = (jnp.flip(decay, 0), jnp.flip(drive, 0))
        _, states = lax.associative_scan(pair_join, (decay, drive), axis=0)
        if sense == 1:
            states = jnp.flip(states, 0)
        state_sum = state_sum + states
    mixed = (state_sum * jax.nn.gelu(gate_in.astype(jnp.float32))).astype(jnp.bfloat16)
    proj = jnp.dot(mixed, out_proj, preferred_element_type=jnp.float32).astype(jnp.bfloat16)
    proj = lax.optimization_barrier(proj)
    stream = (residual.astype(jnp.float32) + norm_rows(proj, norm_gain[0])).astype(jnp.bfloat16)
    stream = lax.optimization_barrier(stream)
    normed = norm_rows(stream, norm_gain[1]).astype(jnp.bfloat16)
    nblocks = seq_len // ROWS
    route_blocks = routes.reshape(nblocks, ROWS, TOPK)
    slots = jax.vmap(lambda block: slot_table(block, EXPERTS, CAP))(route_blocks)
    source_rows = jnp.repeat(jnp.arange(ROWS, dtype=jnp.int32), TOPK)

    def fill_table(slot_rows):
        empty = jnp.full((EXPERTS * CAP,), ROWS, jnp.int32)
        return empty.at[slot_rows.reshape(ROWS * TOPK)].set(source_rows)
    table = jax.vmap(fill_table)(slots)
    blocks_pad = jnp.concatenate([normed.reshape(nblocks, ROWS, D), jnp.zeros((nblocks, 1, D), jnp.bfloat16)], axis=1)
    dispatched = jnp.take_along_axis(blocks_pad, table[:, :, None], axis=1)
    by_expert = jnp.moveaxis(dispatched.reshape(nblocks, EXPERTS, CAP, D), 1, 0).reshape(EXPERTS, nblocks * CAP, D)
    results = lax.map(expert_apply, (by_expert, exp_gate, exp_up, exp_down)).reshape(EXPERTS, nblocks, CAP, D)
    slot_place = (slots % CAP).astype(jnp.int32)
    expert_ids = (slots // CAP).astype(jnp.int32)
    block_ids = jnp.arange(nblocks, dtype=jnp.int32)[:, None, None]
    picked = results[expert_ids, block_ids, slot_place]
    weights = route_wt.reshape(nblocks, ROWS, TOPK)[..., None]
    mixture = lax.optimization_barrier(jnp.sum(weights * picked.astype(jnp.float32), axis=2)).reshape(seq_len, D).astype(jnp.bfloat16)
    mixture = lax.optimization_barrier(mixture)
    return (stream.astype(jnp.float32) + norm_rows(mixture, norm_gain[2])).astype(jnp.bfloat16)
```

```python
import jax
import jax.numpy as jnp
from jax import lax
from jax.experimental import pallas as pl
from jax.experimental.pallas import tpu as pltpu
from jax.sharding import PartitionSpec as P

EPSILON = 1e-06
F32 = jnp.float32
BF16 = jnp.bfloat16
SEGS = 8
VMEM = pltpu.MemorySpace.VMEM


def whole():
    return pl.BlockSpec(memory_space=VMEM)


def params(mib):
    return pltpu.CompilerParams(vmem_limit_bytes=mib * 1024 * 1024)


def one_minus_square(log_decay, decay):
    y = 2.0 * log_decay
    series = 1.0 + y * (1.0 / 7.0)
    for k in (6.0, 5.0, 4.0, 3.0, 2.0):
        series = 1.0 + y * (1.0 / k) * series
    return jnp.where(y > -0.5, -y * series, 1.0 - decay * decay)


def softplus_of(x):
    u = jnp.exp(-jnp.abs(x))
    z = u / (2.0 + u)
    z2 = z * z
    series = jnp.full_like(z, 1.0 / 17.0)
    for k in (15.0, 13.0, 11.0, 9.0, 7.0, 5.0, 3.0, 1.0):
        series = 1.0 / k + z2 * series
    return jnp.maximum(x, 0.0) + 2.0 * z * series


def scan_kernel(
    mix, before, after, conv_w, conv_b, decay_param, recur_gate, recur_bias, input_gate, input_bias,
    h_f, p_f, h_b, p_b, seg, total,
    padded, conv, split, wide, wlow, pre, a_f, b_f, a_b, b_b,
):
    length = mix.shape[0]
    step = length // SEGS
    stride = step + 8
    padded[0:8, :] = jnp.zeros((8, 128), F32)
    padded[6:8, :] = before[...].astype(F32)
    padded[8 : 8 + length, :] = mix[...].astype(F32)
    padded[8 + length : 16 + length, :] = jnp.zeros((8, 128), F32)
    padded[8 + length : 10 + length, :] = after[...].astype(F32)
    zero = jnp.zeros((64, 64), F32)
    columns = []
    for sense in range(2):
        for gate in (recur_gate, input_gate):
            columns.append(
                jnp.concatenate(
                    [
                        jnp.concatenate([gate[sense, 0], zero], axis=1),
                        jnp.concatenate([zero, gate[sense, 1]], axis=1),
                    ],
                    axis=0,
                )
            )
    maps = jnp.concatenate(columns, axis=1)
    high = maps.astype(BF16)
    wide[0:128, :] = high
    wide[128:256, :] = high
    wlow[...] = (maps - high.astype(F32)).astype(BF16)

    rows = 64

    def convolve(k, carry):
        at = pl.multiple_of(k * rows, rows)
        out = conv_b[...] + padded[pl.ds(at + 6, rows), :] * conv_w[0:1, :]
        for tap in range(1, 4):
            out = out + padded[pl.ds(at + 6 + tap, rows), :] * conv_w[tap : tap + 1, :]
        conv[pl.ds(at, rows), :] = out
        top = out.astype(BF16)
        split[pl.ds(at, rows), 0:128] = top
        split[pl.ds(at, rows), 128:256] = (out - top.astype(F32)).astype(BF16)
        return carry

    lax.fori_loop(0, length // rows, convolve, 0)
    pre[...] = jnp.dot(split[...], wide[...], preferred_element_type=F32) + jnp.dot(
        split[:, 0:128], wlow[...], preferred_element_type=F32
    )
    rate = -8.0 * softplus_of(-decay_param[...])

    per = step // rows

    def gates(k, carry):
        at = pl.multiple_of(k * rows, rows)
        to = pl.multiple_of((k // per) * stride + (k % per) * rows, 8)
        signal = conv[pl.ds(at, rows), :]
        for sense, (a_ref, b_ref) in enumerate(((a_f, b_f), (a_b, b_b))):
            base = sense * 256
            recur = jax.nn.sigmoid(pre[pl.ds(at, rows), base : base + 128] + recur_bias[sense : sense + 1, :])
            inner = jax.nn.sigmoid(pre[pl.ds(at, rows), base + 128 : base + 256] + input_bias[sense : sense + 1, :])
            log_decay = recur * rate[sense : sense + 1, :]
            decay = jnp.exp(log_decay)
            a_ref[pl.ds(to, rows), :] = decay
            b_ref[pl.ds(to, rows), :] = jnp.sqrt(one_minus_square(log_decay, decay)) * (inner * signal)
        return carry

    lax.fori_loop(0, length // rows, gates, 0)

    def advance(t, carry):
        hf, pf, hb, pb = carry
        back = step - 1 - t
        af = a_f[pl.ds(t, SEGS, stride=stride), :]
        bf = b_f[pl.ds(t, SEGS, stride=stride), :]
        ab = a_b[pl.ds(back, SEGS, stride=stride), :]
        bb = b_b[pl.ds(back, SEGS, stride=stride), :]
        hf = af * hf + bf
        pf = pf * af
        hb = ab * hb + bb
        pb = pb * ab
        here = pl.multiple_of(t * SEGS, SEGS)
        there = pl.multiple_of(back * SEGS, SEGS)
        h_f[pl.ds(here, SEGS), :] = hf
        p_f[pl.ds(here, SEGS), :] = pf
        h_b[pl.ds(there, SEGS), :] = hb
        p_b[pl.ds(there, SEGS), :] = pb
        return hf, pf, hb, pb

    none = jnp.zeros((SEGS, 128), F32)
    ones = jnp.ones((SEGS, 128), F32)
    hf, pf, hb, pb = lax.fori_loop(0, step, advance, (none, ones, none, ones), unroll=8)

    sums = []
    for base, h, p, order in ((0, hf, pf, range(SEGS)), (16, hb, pb, reversed(range(SEGS)))):
        enter = jnp.zeros((1, 128), F32)
        factor = jnp.ones((1, 128), F32)
        for s in order:
            seg[base + s : base + s + 1, :] = enter
            seg[base + 8 + s : base + 9 + s, :] = factor
            enter = p[s : s + 1, :] * enter + h[s : s + 1, :]
            factor = p[s : s + 1, :] * factor
        sums += [factor, enter]
    both = jnp.concatenate(sums + [jnp.zeros((4, 128), F32)], axis=0)
    total[...] = jnp.broadcast_to(both[None], total.shape)


def mix_kernel(h_f, p_f, h_b, p_b, seg, totals, gate_in, out, natural):
    length = out.shape[0]
    step = length // SEGS
    stride = step + 8
    count = totals.shape[0]
    here = lax.axis_index("sp")
    enter_f = jnp.zeros((1, 128), F32)
    enter_b = jnp.zeros((1, 128), F32)
    for j in range(count):
        enter_f = jnp.where(j < here, totals[j, 0:1, :] * enter_f + totals[j, 1:2, :], enter_f)
        k = count - 1 - j
        enter_b = jnp.where(k > here, totals[k, 2:3, :] * enter_b + totals[k, 3:4, :], enter_b)
    into_f = seg[0:8, :] + seg[8:16, :] * enter_f
    into_b = seg[16:24, :] + seg[24:32, :] * enter_b

    def place(t, carry):
        at = pl.multiple_of(t * SEGS, SEGS)
        rows = pl.ds(at, SEGS)
        natural[pl.ds(t, SEGS, stride=stride), :] = (
            h_f[rows, :] + p_f[rows, :] * into_f + (h_b[rows, :] + p_b[rows, :] * into_b)
        )
        return carry

    lax.fori_loop(0, step, place, 0, unroll=8)
    for s in range(SEGS):
        gate = gate_in[s * step : (s + 1) * step, :].astype(F32)
        out[s * step : (s + 1) * step, :] = (
            natural[s * stride : s * stride + step, :] * jax.nn.gelu(gate)
        ).astype(BF16)


def scaled(values, gain):
    return values * lax.rsqrt(jnp.mean(values * values, axis=-1, keepdims=True) + EPSILON) * gain


def proj_kernel(mixed, weights, residual, gain, routes, stream_out, outgoing, acc):
    k = pl.program_id(0)

    @pl.when(k == 0)
    def _():
        acc[...] = jnp.zeros_like(acc)

    lanes = jnp.concatenate([mixed[j] for j in range(mixed.shape[0])], axis=1)
    acc[...] += jnp.dot(lanes, weights[...], preferred_element_type=F32)

    @pl.when(k == pl.num_programs(0) - 1)
    def _():
        proj = acc[...].astype(BF16).astype(F32)
        stream = (residual[...].astype(F32) + scaled(proj, gain[0:1, :])).astype(BF16)
        stream_out[...] = stream
        normed = scaled(stream.astype(F32), gain[1:2, :]).astype(BF16)
        rows = normed.shape[0]
        slots = outgoing.shape[0]
        experts = 16
        capacity = slots // experts
        first, second = routes[0:1, :], routes[1:2, :]
        ids = lax.broadcasted_iota(jnp.int32, (experts, rows), 0)
        hit0 = (ids == first).astype(F32)
        hit1 = (ids == second).astype(F32)
        r = lax.broadcasted_iota(jnp.int32, (rows, rows), 0)
        c = lax.broadcasted_iota(jnp.int32, (rows, rows), 1)
        earlier = jnp.dot((hit0 + hit1).astype(BF16), (r < c).astype(BF16), preferred_element_type=F32)
        slot0 = first * capacity + jnp.sum(hit0 * earlier, axis=0, keepdims=True).astype(jnp.int32)
        slot1 = second * capacity + jnp.sum(hit1 * earlier, axis=0, keepdims=True).astype(jnp.int32)
        places = lax.broadcasted_iota(jnp.int32, (slots, rows), 0)
        pick = jnp.where(jnp.logical_or(places == slot0, places == slot1), 1.0, 0.0).astype(BF16)
        outgoing[...] = jnp.dot(pick, normed, preferred_element_type=F32).astype(BF16)


def pack_kernel(gate, up, down, out):
    d = gate.shape[1]
    ff = down.shape[1]
    out[0:d, :] = jnp.concatenate([gate[0], up[0]], axis=1)
    for c in range(down.shape[2] // 128):
        out[d + c * ff : d + (c + 1) * ff, :] = down[0, :, c * 128 : (c + 1) * 128]


def expert_kernel(tokens, packed, out, acc):
    k = pl.program_id(0)
    width = tokens.shape[1]

    @pl.when(k == 0)
    def _():
        acc[...] = jnp.zeros_like(acc)

    x = tokens[...]
    rows = x.shape[0]
    low = lax.broadcasted_iota(jnp.int32, (rows, 128), 1) < 64
    hidden = []
    for pair in range(2):
        both = jnp.concatenate([packed[2 * pair, 0:width, :], packed[2 * pair + 1, 0:width, :]], axis=1)
        z = jnp.dot(x, both, preferred_element_type=F32)
        even, odd = z[:, 0:128], z[:, 128:256]
        gate = jnp.where(low, even, pltpu.roll(odd, 64, 1))
        up = jnp.where(low, pltpu.roll(even, 64, 1), odd)
        hidden.append((jax.nn.silu(gate) * up).astype(BF16))
    hid = jnp.concatenate(hidden, axis=1)
    for c in range(width // 256):
        cols = []
        for half in range(2):
            at = width + (2 * c + half) * 64
            cols.append(jnp.concatenate([packed[p, at : at + 64, :] for p in range(4)], axis=0))
        acc[:, c * 256 : (c + 1) * 256] += jnp.dot(
            hid, jnp.concatenate(cols, axis=1), preferred_element_type=F32
        )

    @pl.when(k == pl.num_programs(0) - 1)
    def _():
        out[...] = acc[...].astype(BF16)


def combine_kernel(values, stream, gain, routes, weights, out):
    rows = stream.shape[0]
    slots = values.shape[0]
    experts = 16
    capacity = slots // experts
    first, second = routes[:, 0:1], routes[:, 1:2]
    ids = lax.broadcasted_iota(jnp.int32, (rows, experts), 1)
    hit0 = (ids == first).astype(F32)
    hit1 = (ids == second).astype(F32)
    r = lax.broadcasted_iota(jnp.int32, (rows, rows), 0)
    c = lax.broadcasted_iota(jnp.int32, (rows, rows), 1)
    earlier = jnp.dot((c < r).astype(BF16), (hit0 + hit1).astype(BF16), preferred_element_type=F32)
    slot0 = first * capacity + jnp.sum(hit0 * earlier, axis=1, keepdims=True).astype(jnp.int32)
    slot1 = second * capacity + jnp.sum(hit1 * earlier, axis=1, keepdims=True).astype(jnp.int32)
    places = lax.broadcasted_iota(jnp.int32, (rows, slots), 1)
    table = jnp.where(places == slot0, weights[:, 0:1], 0.0) + jnp.where(
        places == slot1, weights[:, 1:2], 0.0
    )
    high = table.astype(BF16)
    rest = table - high.astype(F32)
    mid = rest.astype(BF16)
    low = (rest - mid.astype(F32)).astype(BF16)
    parts = jnp.dot(jnp.concatenate([high, mid, low], axis=0), values[...], preferred_element_type=F32)
    mixture = parts[0:rows] + (parts[rows : 2 * rows] + parts[2 * rows : 3 * rows])
    mixture = mixture.astype(BF16).astype(F32)
    out[...] = (stream[...].astype(F32) + scaled(mixture, gain[2:3, :])).astype(BF16)


def shape(dims, dtype):
    return jax.ShapeDtypeStruct(dims, dtype)


def on_device(
    mix_in,
    gate_in,
    conv_w,
    conv_b,
    decay_param,
    recur_gate,
    recur_bias,
    input_gate,
    input_bias,
    residual,
    out_proj,
    norm_gain,
    routes,
    route_wt,
    exp_gate,
    exp_up,
    exp_down,
):
    length, channels = mix_in.shape
    rows, width = residual.shape
    sp = lax.axis_size("sp")
    tp = lax.axis_size("tp")
    ff_own = exp_down.shape[1]
    packed_rows = width + ff_own * width // 128
    packed = pl.pallas_call(
        pack_kernel,
        out_shape=shape((packed_rows, 128), BF16),
        in_specs=[whole()] * 3,
        out_specs=whole(),
        compiler_params=params(8),
        name="pack",
    )(exp_gate, exp_up, exp_down)
    gathered = lax.all_gather(packed, "tp", axis=0, tiled=False)

    ends = sp - 1
    before = lax.ppermute(mix_in[length - 2 :], "sp", [(i, i + 1) for i in range(ends)])
    after = lax.ppermute(mix_in[:2], "sp", [(i + 1, i) for i in range(ends)])
    step = length // SEGS
    lines = SEGS * (step + 8)
    state = shape((length, channels), F32)
    h_f, p_f, h_b, p_b, seg, total = pl.pallas_call(
        scan_kernel,
        out_shape=(state, state, state, state, shape((32, 128), F32), shape((sp, 8, 128), F32)),
        in_specs=[whole()] * 10,
        out_specs=(whole(),) * 6,
        scratch_shapes=[
            pltpu.VMEM((length + 16, 128), F32),
            pltpu.VMEM((length, 128), F32),
            pltpu.VMEM((length, 256), BF16),
            pltpu.VMEM((256, 512), BF16),
            pltpu.VMEM((128, 512), BF16),
            pltpu.VMEM((length, 512), F32),
            pltpu.VMEM((lines, 128), F32),
            pltpu.VMEM((lines, 128), F32),
            pltpu.VMEM((lines, 128), F32),
            pltpu.VMEM((lines, 128), F32),
        ],
        compiler_params=params(20),
        name="scan",
    )(mix_in, before, after, conv_w, conv_b[None], decay_param, recur_gate, recur_bias, input_gate, input_bias)
    totals = lax.all_to_all(total, "sp", split_axis=0, concat_axis=0, tiled=True)
    mixed = pl.pallas_call(
        mix_kernel,
        out_shape=shape((length, channels), BF16),
        in_specs=[whole()] * 7,
        out_specs=whole(),
        scratch_shapes=[pltpu.VMEM((lines, 128), F32)],
        compiler_params=params(12),
        name="mix",
    )(h_f, p_f, h_b, p_b, seg, totals, gate_in)
    token_rows = lax.all_to_all(
        mixed.reshape(tp, rows, channels), "tp", split_axis=0, concat_axis=0, tiled=True
    )
    own = lax.axis_index("tp") * rows
    own_routes = lax.dynamic_slice_in_dim(routes, own, rows, 0)
    own_weights = lax.dynamic_slice_in_dim(route_wt, own, rows, 0)
    slots = 2 * rows * routes.shape[1]
    block = 256
    fixed = lambda *dims: pl.BlockSpec(dims, lambda k: (0,) * len(dims))
    stream, outgoing = pl.pallas_call(
        proj_kernel,
        grid=(width // block,),
        out_shape=(shape((rows, width), BF16), shape((slots, width), BF16)),
        in_specs=[
            pl.BlockSpec((block // channels, rows, channels), lambda k: (k, 0, 0)),
            pl.BlockSpec((block, width), lambda k: (k, 0)),
            fixed(rows, width),
            fixed(*norm_gain.shape),
            fixed(routes.shape[1], rows),
        ],
        out_specs=(fixed(rows, width), fixed(slots, width)),
        scratch_shapes=[pltpu.VMEM((rows, width), F32)],
        compiler_params=params(16),
        name="proj",
    )(token_rows, out_proj, residual, norm_gain, own_routes.T)
    arrived = lax.all_to_all(
        outgoing.reshape(sp, slots // sp, width), "sp", split_axis=0, concat_axis=0, tiled=True
    )
    done = pl.pallas_call(
        expert_kernel,
        grid=(tp // 4,),
        out_shape=shape((slots, width), BF16),
        in_specs=[
            fixed(slots, width),
            pl.BlockSpec((4, packed_rows, 128), lambda k: (k, 0, 0)),
        ],
        out_specs=fixed(slots, width),
        scratch_shapes=[pltpu.VMEM((slots, width), F32)],
        compiler_params=params(32),
        name="experts",
    )(arrived.reshape(slots, width), gathered)
    returned = lax.all_to_all(
        done.reshape(sp, slots // sp, width), "sp", split_axis=0, concat_axis=0, tiled=True
    )
    return pl.pallas_call(
        combine_kernel,
        out_shape=shape((rows, width), BF16),
        in_specs=[whole()] * 5,
        out_specs=whole(),
        compiler_params=params(16),
        name="combine",
    )(returned.reshape(slots, width), stream, norm_gain, own_routes, own_weights)


def solution(mesh):
    return jax.shard_map(
        on_device,
        mesh=mesh,
        in_specs=(
            P("sp", "tp"),
            P("sp", "tp"),
            P(None, "tp"),
            P("tp"),
            P(None, "tp"),
            P(None, "tp", None, None),
            P(None, "tp"),
            P(None, "tp", None, None),
            P(None, "tp"),
            P(("sp", "tp"), None),
            P(),
            P(),
            P("sp", None),
            P("sp", None),
            P("sp", None, "tp"),
            P("sp", None, "tp"),
            P("sp", "tp", None),
        ),
        out_specs=P(("sp", "tp"), None),
        check_vma=False,
    )
```

```python
import jax
import jax.numpy as jnp
from jax import lax
from jax.experimental import pallas as pl
from jax.experimental.pallas import tpu as pltpu
from jax.sharding import PartitionSpec as P

EPSILON = 1e-06
F32 = jnp.float32
BF16 = jnp.bfloat16
SEGS = 8
VMEM = pltpu.MemorySpace.VMEM


def whole():
    return pl.BlockSpec(memory_space=VMEM)


def params(mib):
    return pltpu.CompilerParams(vmem_limit_bytes=mib * 1024 * 1024)


def anywhere():
    return pl.BlockSpec(memory_space=pl.ANY)


def fetched(sources, buffers, sems, first=0):
    copies = [pltpu.make_async_copy(src, dst, sems.at[first + k]) for k, (src, dst) in enumerate(zip(sources, buffers))]
    for copy in copies:
        copy.start()
    return copies


def one_minus_square(log_decay, decay):
    y = 2.0 * log_decay
    series = 1.0 + y * (1.0 / 7.0)
    for k in (6.0, 5.0, 4.0, 3.0, 2.0):
        series = 1.0 + y * (1.0 / k) * series
    return jnp.where(y > -0.5, -y * series, 1.0 - decay * decay)


def softplus_of(x):
    u = jnp.exp(-jnp.abs(x))
    z = u / (2.0 + u)
    z2 = z * z
    series = jnp.full_like(z, 1.0 / 17.0)
    for k in (15.0, 13.0, 11.0, 9.0, 7.0, 5.0, 3.0, 1.0):
        series = 1.0 / k + z2 * series
    return jnp.maximum(x, 0.0) + 2.0 * z * series


def scan_kernel(
    mix_h, before, after, conv_w_h, conv_b_h, decay_param_h, recur_gate_h, recur_bias_h, input_gate_h, input_bias_h,
    h_f, p_f, h_b, p_b, seg, total,
    padded, conv, split, wide, wlow, pre, a_f, b_f, a_b, b_b,
    mix, conv_w, conv_b, decay_param, recur_gate, recur_bias, input_gate, input_bias, sems,
):
    for copy in fetched(
        (mix_h, conv_w_h, conv_b_h, decay_param_h, recur_gate_h, recur_bias_h, input_gate_h, input_bias_h),
        (mix, conv_w, conv_b, decay_param, recur_gate, recur_bias, input_gate, input_bias),
        sems,
    ):
        copy.wait()
    length = mix.shape[0]
    step = length // SEGS
    stride = step + 8
    padded[0:8, :] = jnp.zeros((8, 128), F32)
    padded[6:8, :] = before[...].astype(F32)
    padded[8 : 8 + length, :] = mix[...].astype(F32)
    padded[8 + length : 16 + length, :] = jnp.zeros((8, 128), F32)
    padded[8 + length : 10 + length, :] = after[...].astype(F32)
    zero = jnp.zeros((64, 64), F32)
    columns = []
    for sense in range(2):
        for gate in (recur_gate, input_gate):
            columns.append(
                jnp.concatenate(
                    [
                        jnp.concatenate([gate[sense, 0], zero], axis=1),
                        jnp.concatenate([zero, gate[sense, 1]], axis=1),
                    ],
                    axis=0,
                )
            )
    maps = jnp.concatenate(columns, axis=1)
    high = maps.astype(BF16)
    wide[0:128, :] = high
    wide[128:256, :] = high
    wlow[...] = (maps - high.astype(F32)).astype(BF16)

    rows = 64

    def convolve(k, carry):
        at = pl.multiple_of(k * rows, rows)
        out = conv_b[...] + padded[pl.ds(at + 6, rows), :] * conv_w[0:1, :]
        for tap in range(1, 4):
            out = out + padded[pl.ds(at + 6 + tap, rows), :] * conv_w[tap : tap + 1, :]
        conv[pl.ds(at, rows), :] = out
        top = out.astype(BF16)
        split[pl.ds(at, rows), 0:128] = top
        split[pl.ds(at, rows), 128:256] = (out - top.astype(F32)).astype(BF16)
        return carry

    lax.fori_loop(0, length // rows, convolve, 0)
    pre[...] = jnp.dot(split[...], wide[...], preferred_element_type=F32) + jnp.dot(
        split[:, 0:128], wlow[...], preferred_element_type=F32
    )
    rate = -8.0 * softplus_of(-decay_param[...])

    per = step // rows

    def gates(k, carry):
        at = pl.multiple_of(k * rows, rows)
        to = pl.multiple_of((k // per) * stride + (k % per) * rows, 8)
        signal = conv[pl.ds(at, rows), :]
        for sense, (a_ref, b_ref) in enumerate(((a_f, b_f), (a_b, b_b))):
            base = sense * 256
            recur = jax.nn.sigmoid(pre[pl.ds(at, rows), base : base + 128] + recur_bias[sense : sense + 1, :])
            inner = jax.nn.sigmoid(pre[pl.ds(at, rows), base + 128 : base + 256] + input_bias[sense : sense + 1, :])
            log_decay = recur * rate[sense : sense + 1, :]
            decay = jnp.exp(log_decay)
            a_ref[pl.ds(to, rows), :] = decay
            b_ref[pl.ds(to, rows), :] = jnp.sqrt(one_minus_square(log_decay, decay)) * (inner * signal)
        return carry

    lax.fori_loop(0, length // rows, gates, 0)

    def advance(t, carry):
        hf, pf, hb, pb = carry
        back = step - 1 - t
        af = a_f[pl.ds(t, SEGS, stride=stride), :]
        bf = b_f[pl.ds(t, SEGS, stride=stride), :]
        ab = a_b[pl.ds(back, SEGS, stride=stride), :]
        bb = b_b[pl.ds(back, SEGS, stride=stride), :]
        hf = af * hf + bf
        pf = pf * af
        hb = ab * hb + bb
        pb = pb * ab
        here = pl.multiple_of(t * SEGS, SEGS)
        there = pl.multiple_of(back * SEGS, SEGS)
        h_f[pl.ds(here, SEGS), :] = hf
        p_f[pl.ds(here, SEGS), :] = pf
        h_b[pl.ds(there, SEGS), :] = hb
        p_b[pl.ds(there, SEGS), :] = pb
        return hf, pf, hb, pb

    none = jnp.zeros((SEGS, 128), F32)
    ones = jnp.ones((SEGS, 128), F32)
    hf, pf, hb, pb = lax.fori_loop(0, step, advance, (none, ones, none, ones), unroll=8)

    sums = []
    for base, h, p, order in ((0, hf, pf, range(SEGS)), (16, hb, pb, reversed(range(SEGS)))):
        enter = jnp.zeros((1, 128), F32)
        factor = jnp.ones((1, 128), F32)
        for s in order:
            seg[base + s : base + s + 1, :] = enter
            seg[base + 8 + s : base + 9 + s, :] = factor
            enter = p[s : s + 1, :] * enter + h[s : s + 1, :]
            factor = p[s : s + 1, :] * factor
        sums += [factor, enter]
    both = jnp.concatenate(sums + [jnp.zeros((4, 128), F32)], axis=0)
    total[...] = jnp.broadcast_to(both[None], total.shape)


def mix_kernel(h_f, p_f, h_b, p_b, seg, totals, gate_h, out, natural, gate_in, sems):
    (copy,) = fetched((gate_h,), (gate_in,), sems)
    length = out.shape[0]
    step = length // SEGS
    stride = step + 8
    count = totals.shape[0]
    here = lax.axis_index("sp")
    enter_f = jnp.zeros((1, 128), F32)
    enter_b = jnp.zeros((1, 128), F32)
    for j in range(count):
        enter_f = jnp.where(j < here, totals[j, 0:1, :] * enter_f + totals[j, 1:2, :], enter_f)
        k = count - 1 - j
        enter_b = jnp.where(k > here, totals[k, 2:3, :] * enter_b + totals[k, 3:4, :], enter_b)
    into_f = seg[0:8, :] + seg[8:16, :] * enter_f
    into_b = seg[16:24, :] + seg[24:32, :] * enter_b

    def place(t, carry):
        at = pl.multiple_of(t * SEGS, SEGS)
        rows = pl.ds(at, SEGS)
        natural[pl.ds(t, SEGS, stride=stride), :] = (
            h_f[rows, :] + p_f[rows, :] * into_f + (h_b[rows, :] + p_b[rows, :] * into_b)
        )
        return carry

    lax.fori_loop(0, step, place, 0, unroll=8)
    copy.wait()
    for s in range(SEGS):
        gate = gate_in[s * step : (s + 1) * step, :].astype(F32)
        out[s * step : (s + 1) * step, :] = (
            natural[s * stride : s * stride + step, :] * jax.nn.gelu(gate)
        ).astype(BF16)


def scaled(values, gain):
    return values * lax.rsqrt(jnp.mean(values * values, axis=-1, keepdims=True) + EPSILON) * gain


def proj_kernel(mixed, weights_h, residual_h, gain_h, routes, stream_out, outgoing, weights, residual, gain, sems):
    width = weights.shape[0]
    blocks = 8
    block = width // blocks
    parts = [(weights_h.at[pl.ds(k * block, block)], weights.at[pl.ds(k * block, block)]) for k in range(blocks)]
    loads = fetched(*zip(*parts), sems)
    others = fetched((residual_h, gain_h), (residual, gain), sems, blocks)
    acc = jnp.zeros(residual.shape, F32)
    per = mixed.shape[0] // blocks
    for k in range(blocks):
        lanes = jnp.concatenate([mixed[k * per + j] for j in range(per)], axis=1)
        loads[k].wait()
        acc = acc + jnp.dot(lanes, weights[k * block : (k + 1) * block, :], preferred_element_type=F32)
    for copy in others:
        copy.wait()
    if True:
        proj = acc.astype(BF16).astype(F32)
        stream = (residual[...].astype(F32) + scaled(proj, gain[0:1, :])).astype(BF16)
        stream_out[...] = stream
        normed = scaled(stream.astype(F32), gain[1:2, :]).astype(BF16)
        rows = normed.shape[0]
        slots = outgoing.shape[0]
        experts = 16
        capacity = slots // experts
        first, second = routes[0:1, :], routes[1:2, :]
        ids = lax.broadcasted_iota(jnp.int32, (experts, rows), 0)
        hit0 = (ids == first).astype(F32)
        hit1 = (ids == second).astype(F32)
        r = lax.broadcasted_iota(jnp.int32, (rows, rows), 0)
        c = lax.broadcasted_iota(jnp.int32, (rows, rows), 1)
        earlier = jnp.dot((hit0 + hit1).astype(BF16), (r < c).astype(BF16), preferred_element_type=F32)
        slot0 = first * capacity + jnp.sum(hit0 * earlier, axis=0, keepdims=True).astype(jnp.int32)
        slot1 = second * capacity + jnp.sum(hit1 * earlier, axis=0, keepdims=True).astype(jnp.int32)
        places = lax.broadcasted_iota(jnp.int32, (slots, rows), 0)
        pick = jnp.where(jnp.logical_or(places == slot0, places == slot1), 1.0, 0.0).astype(BF16)
        outgoing[...] = jnp.dot(pick, normed, preferred_element_type=F32).astype(BF16)


def pack_kernel(*refs):
    own, other, out, sems = refs[0:3], refs[3:6], refs[6], refs[7]
    ff = own[0].shape[0]
    core = lax.rem(lax.axis_index("tp"), 2)
    copies = []
    for side, group in enumerate((own, other)):
        first = (core if side == 0 else 1 - core) * 3 * ff
        for j, ref in enumerate(group):
            copy = pltpu.make_async_copy(ref, out.at[pl.ds(first + j * ff, ff)], sems.at[3 * side + j])
            copy.start()
            copies.append(copy)
    for copy in copies:
        copy.wait()


def expert_kernel(*refs):
    tokens, shares, (out, gate_w, up_w, down_w, sems) = refs[0], refs[1:-5], refs[-5:]
    ff = 64
    copies = []
    at = 0
    for share in shares:
        for piece in range(share.shape[0] // (3 * ff)):
            copies.append(
                fetched(
                    [share.at[pl.ds((3 * piece + j) * ff, ff)] for j in range(3)],
                    [w.at[pl.ds(at * ff, ff)] for w in (gate_w, up_w, down_w)],
                    sems,
                    3 * at,
                )
            )
            at += 1
    x = tokens[...]
    acc = jnp.zeros(out.shape, F32)
    block = 256
    last = (((1,), (1,)), ((), ()))
    for k in range(at * ff // block):
        for piece in range(k * block // ff, (k + 1) * block // ff):
            for copy in copies[piece]:
                copy.wait()
        rows = slice(k * block, (k + 1) * block)
        gate = lax.dot_general(x, gate_w[rows, :], last, preferred_element_type=F32)
        up = lax.dot_general(x, up_w[rows, :], last, preferred_element_type=F32)
        hidden = (jax.nn.silu(gate) * up).astype(BF16)
        acc = acc + jnp.dot(hidden, down_w[rows, :], preferred_element_type=F32)
    out[...] = acc.astype(BF16)


def combine_kernel(values, stream, gain, routes, weights, out):
    rows = stream.shape[0]
    slots = values.shape[0]
    experts = 16
    capacity = slots // experts
    first, second = routes[:, 0:1], routes[:, 1:2]
    ids = lax.broadcasted_iota(jnp.int32, (rows, experts), 1)
    hit0 = (ids == first).astype(F32)
    hit1 = (ids == second).astype(F32)
    r = lax.broadcasted_iota(jnp.int32, (rows, rows), 0)
    c = lax.broadcasted_iota(jnp.int32, (rows, rows), 1)
    earlier = jnp.dot((c < r).astype(BF16), (hit0 + hit1).astype(BF16), preferred_element_type=F32)
    slot0 = first * capacity + jnp.sum(hit0 * earlier, axis=1, keepdims=True).astype(jnp.int32)
    slot1 = second * capacity + jnp.sum(hit1 * earlier, axis=1, keepdims=True).astype(jnp.int32)
    places = lax.broadcasted_iota(jnp.int32, (rows, slots), 1)
    table = jnp.where(places == slot0, weights[:, 0:1], 0.0) + jnp.where(
        places == slot1, weights[:, 1:2], 0.0
    )
    high = table.astype(BF16)
    rest = table - high.astype(F32)
    mid = rest.astype(BF16)
    low = (rest - mid.astype(F32)).astype(BF16)
    parts = jnp.dot(jnp.concatenate([high, mid, low], axis=0), values[...], preferred_element_type=F32)
    mixture = parts[0:rows] + (parts[rows : 2 * rows] + parts[2 * rows : 3 * rows])
    mixture = mixture.astype(BF16).astype(F32)
    out[...] = (stream[...].astype(F32) + scaled(mixture, gain[2:3, :])).astype(BF16)


def shape(dims, dtype):
    return jax.ShapeDtypeStruct(dims, dtype)


def on_device(
    mix_in,
    gate_in,
    conv_w,
    conv_b,
    decay_param,
    recur_gate,
    recur_bias,
    input_gate,
    input_bias,
    residual,
    out_proj,
    norm_gain,
    routes,
    route_wt,
    exp_gate,
    exp_up,
    exp_down,
):
    length, channels = mix_in.shape
    rows, width = residual.shape
    sp = lax.axis_size("sp")
    tp = lax.axis_size("tp")
    own_share = (jnp.swapaxes(exp_gate, 1, 2)[0], jnp.swapaxes(exp_up, 1, 2)[0], exp_down[0])
    partner = [(i, i ^ 1) for i in range(tp)]
    around = [(i, (i + 2) % tp if i % 2 == 0 else (i - 2) % tp) for i in range(tp)]
    other_share = [lax.ppermute(part, "tp", partner) for part in own_share]
    ff_own = exp_down.shape[1]
    share0 = pl.pallas_call(
        pack_kernel,
        out_shape=shape((6 * ff_own, width), BF16),
        in_specs=[anywhere()] * 6,
        out_specs=anywhere(),
        scratch_shapes=[pltpu.SemaphoreType.DMA((6,))],
        name="pack",
    )(*own_share, *other_share)
    share1 = lax.ppermute(share0, "tp", around)

    ends = sp - 1
    before = lax.ppermute(mix_in[length - 2 :], "sp", [(i, i + 1) for i in range(ends)])
    after = lax.ppermute(mix_in[:2], "sp", [(i + 1, i) for i in range(ends)])
    step = length // SEGS
    lines = SEGS * (step + 8)
    state = shape((length, channels), F32)
    h_f, p_f, h_b, p_b, seg, total = pl.pallas_call(
        scan_kernel,
        out_shape=(state, state, state, state, shape((32, 128), F32), shape((sp, 8, 128), F32)),
        in_specs=[anywhere(), whole(), whole()] + [anywhere()] * 7,
        out_specs=(whole(),) * 6,
        scratch_shapes=[
            pltpu.VMEM((length + 16, 128), F32),
            pltpu.VMEM((length, 128), F32),
            pltpu.VMEM((length, 256), BF16),
            pltpu.VMEM((256, 512), BF16),
            pltpu.VMEM((128, 512), BF16),
            pltpu.VMEM((length, 512), F32),
            pltpu.VMEM((lines, 128), F32),
            pltpu.VMEM((lines, 128), F32),
            pltpu.VMEM((lines, 128), F32),
            pltpu.VMEM((lines, 128), F32),
            pltpu.VMEM(mix_in.shape, BF16),
            pltpu.VMEM(conv_w.shape, F32),
            pltpu.VMEM((1, 128), F32),
            pltpu.VMEM(decay_param.shape, F32),
            pltpu.VMEM(recur_gate.shape, F32),
            pltpu.VMEM(recur_bias.shape, F32),
            pltpu.VMEM(input_gate.shape, F32),
            pltpu.VMEM(input_bias.shape, F32),
            pltpu.SemaphoreType.DMA((8,)),
        ],
        compiler_params=params(20),
        name="scan",
    )(mix_in, before, after, conv_w, conv_b[None], decay_param, recur_gate, recur_bias, input_gate, input_bias)
    totals = lax.all_to_all(total, "sp", split_axis=0, concat_axis=0, tiled=True)
    totals, share1 = lax.optimization_barrier((totals, share1))
    share2 = lax.ppermute(share1, "tp", around)
    other1 = lax.ppermute(share1, "tp", partner)
    mixed = pl.pallas_call(
        mix_kernel,
        out_shape=shape((length, channels), BF16),
        in_specs=[whole()] * 6 + [anywhere()],
        out_specs=whole(),
        scratch_shapes=[
            pltpu.VMEM((lines, 128), F32),
            pltpu.VMEM((length, channels), BF16),
            pltpu.SemaphoreType.DMA((1,)),
        ],
        compiler_params=params(12),
        name="mix",
    )(h_f, p_f, h_b, p_b, seg, totals, gate_in)
    token_rows = lax.all_to_all(
        mixed.reshape(tp, rows, channels), "tp", split_axis=0, concat_axis=0, tiled=True
    )
    token_rows, share2 = lax.optimization_barrier((token_rows, share2))
    share3 = lax.ppermute(share2, "tp", around)
    other2 = lax.ppermute(share2, "tp", partner)
    own = lax.axis_index("tp") * rows
    own_routes = lax.dynamic_slice_in_dim(routes, own, rows, 0)
    own_weights = lax.dynamic_slice_in_dim(route_wt, own, rows, 0)
    slots = 2 * rows * routes.shape[1]
    stream, outgoing = pl.pallas_call(
        proj_kernel,
        out_shape=(shape((rows, width), BF16), shape((slots, width), BF16)),
        in_specs=[whole(), anywhere(), anywhere(), anywhere(), whole()],
        out_specs=(whole(), whole()),
        scratch_shapes=[
            pltpu.VMEM(out_proj.shape, BF16),
            pltpu.VMEM(residual.shape, BF16),
            pltpu.VMEM(norm_gain.shape, F32),
            pltpu.SemaphoreType.DMA((10,)),
        ],
        compiler_params=params(16),
        name="proj",
    )(token_rows, out_proj, residual, norm_gain, own_routes.T)
    arrived = lax.all_to_all(
        outgoing.reshape(sp, slots // sp, width), "sp", split_axis=0, concat_axis=0, tiled=True
    )
    arrived, share3 = lax.optimization_barrier((arrived, share3))
    half = 3 * ff_own
    core = lax.rem(lax.axis_index("tp"), 2)
    share4 = lax.ppermute(lax.dynamic_slice_in_dim(share3, core * half, half, 0), "tp", around)
    other3 = lax.ppermute(share3, "tp", partner)
    other4 = lax.ppermute(share4, "tp", partner)
    shares = (share0, share1, other1, share2, other2, share3, other3, share4, other4)
    hidden_units = tp * ff_own
    done = pl.pallas_call(
        expert_kernel,
        out_shape=shape((slots, width), BF16),
        in_specs=[whole()] + [anywhere()] * len(shares),
        out_specs=whole(),
        scratch_shapes=[pltpu.VMEM((hidden_units, width), BF16)] * 3 + [pltpu.SemaphoreType.DMA((3 * tp,))],
        compiler_params=params(32),
        name="experts",
    )(arrived.reshape(slots, width), *shares)
    returned = lax.all_to_all(
        done.reshape(sp, slots // sp, width), "sp", split_axis=0, concat_axis=0, tiled=True
    )
    return pl.pallas_call(
        combine_kernel,
        out_shape=shape((rows, width), BF16),
        in_specs=[whole()] * 5,
        out_specs=whole(),
        compiler_params=params(16),
        name="combine",
    )(returned.reshape(slots, width), stream, norm_gain, own_routes, own_weights)


def solution(mesh):
    return jax.shard_map(
        on_device,
        mesh=mesh,
        in_specs=(
            P("sp", "tp"),
            P("sp", "tp"),
            P(None, "tp"),
            P("tp"),
            P(None, "tp"),
            P(None, "tp", None, None),
            P(None, "tp"),
            P(None, "tp", None, None),
            P(None, "tp"),
            P(("sp", "tp"), None),
            P(),
            P(),
            P("sp", None),
            P("sp", None),
            P("sp", None, "tp"),
            P("sp", None, "tp"),
            P("sp", "tp", None),
        ),
        out_specs=P(("sp", "tp"), None),
        check_vma=False,
    )
```

```python
import functools

import jax
import jax.numpy as jnp
from jax import lax
from jax.experimental import pallas as pl
from jax.experimental.pallas import tpu as pltpu
from jax.sharding import PartitionSpec as P


EPSILON = 1e-06
F32 = jnp.float32
BF16 = jnp.bfloat16
SEGS = 8
VMEM = pltpu.MemorySpace.VMEM


def whole():
    return pl.BlockSpec(memory_space=VMEM)


def params(mib):
    return pltpu.CompilerParams(vmem_limit_bytes=mib * 1024 * 1024)


def anywhere():
    return pl.BlockSpec(memory_space=pl.ANY)


def in_hbm():
    return pl.BlockSpec(memory_space=pltpu.MemorySpace.HBM)


def fetched(sources, buffers, sems, first=0):
    copies = [pltpu.make_async_copy(src, dst, sems.at[first + k]) for k, (src, dst) in enumerate(zip(sources, buffers))]
    for copy in copies:
        copy.start()
    return copies


def one_minus_square(log_decay, decay):
    y = 2.0 * log_decay
    series = 1.0 + y * (1.0 / 7.0)
    for k in (6.0, 5.0, 4.0, 3.0, 2.0):
        series = 1.0 + y * (1.0 / k) * series
    return jnp.where(y > -0.5, -y * series, 1.0 - decay * decay)


def softplus_of(x):
    u = jnp.exp(-jnp.abs(x))
    z = u / (2.0 + u)
    z2 = z * z
    series = jnp.full_like(z, 1.0 / 17.0)
    for k in (15.0, 13.0, 11.0, 9.0, 7.0, 5.0, 3.0, 1.0):
        series = 1.0 / k + z2 * series
    return jnp.maximum(x, 0.0) + 2.0 * z * series


def scan_kernel(
    mix_h, before, after, conv_w_h, conv_b_h, decay_param_h, recur_gate_h, recur_bias_h, input_gate_h, input_bias_h,
    h_f, p_f, h_b, p_b, seg, total,
    padded, conv, split, wide, wlow, pre, a_f, b_f, a_b, b_b,
    mix, conv_w, conv_b, decay_param, recur_gate, recur_bias, input_gate, input_bias, sems,
):
    for copy in fetched(
        (mix_h, conv_w_h, conv_b_h, decay_param_h, recur_gate_h, recur_bias_h, input_gate_h, input_bias_h),
        (mix, conv_w, conv_b, decay_param, recur_gate, recur_bias, input_gate, input_bias),
        sems,
    ):
        copy.wait()
    length = mix.shape[0]
    step = length // SEGS
    stride = step + 8
    padded[0:8, :] = jnp.zeros((8, 128), F32)
    padded[6:8, :] = before[...].astype(F32)
    padded[8 : 8 + length, :] = mix[...].astype(F32)
    padded[8 + length : 16 + length, :] = jnp.zeros((8, 128), F32)
    padded[8 + length : 10 + length, :] = after[...].astype(F32)
    zero = jnp.zeros((64, 64), F32)
    columns = []
    for sense in range(2):
        for gate in (recur_gate, input_gate):
            columns.append(
                jnp.concatenate(
                    [
                        jnp.concatenate([gate[sense, 0], zero], axis=1),
                        jnp.concatenate([zero, gate[sense, 1]], axis=1),
                    ],
                    axis=0,
                )
            )
    maps = jnp.concatenate(columns, axis=1)
    high = maps.astype(BF16)
    wide[0:128, :] = high
    wide[128:256, :] = high
    wlow[...] = (maps - high.astype(F32)).astype(BF16)

    rows = 64

    def convolve(k, carry):
        at = pl.multiple_of(k * rows, rows)
        out = conv_b[...] + padded[pl.ds(at + 6, rows), :] * conv_w[0:1, :]
        for tap in range(1, 4):
            out = out + padded[pl.ds(at + 6 + tap, rows), :] * conv_w[tap : tap + 1, :]
        conv[pl.ds(at, rows), :] = out
        top = out.astype(BF16)
        split[pl.ds(at, rows), 0:128] = top
        split[pl.ds(at, rows), 128:256] = (out - top.astype(F32)).astype(BF16)
        return carry

    lax.fori_loop(0, length // rows, convolve, 0)
    pre[...] = jnp.dot(split[...], wide[...], preferred_element_type=F32) + jnp.dot(
        split[:, 0:128], wlow[...], preferred_element_type=F32
    )
    rate = -8.0 * softplus_of(-decay_param[...])

    per = step // rows

    def gates(k, carry):
        at = pl.multiple_of(k * rows, rows)
        to = pl.multiple_of((k // per) * stride + (k % per) * rows, 8)
        signal = conv[pl.ds(at, rows), :]
        for sense, (a_ref, b_ref) in enumerate(((a_f, b_f), (a_b, b_b))):
            base = sense * 256
            recur = jax.nn.sigmoid(pre[pl.ds(at, rows), base : base + 128] + recur_bias[sense : sense + 1, :])
            inner = jax.nn.sigmoid(pre[pl.ds(at, rows), base + 128 : base + 256] + input_bias[sense : sense + 1, :])
            log_decay = recur * rate[sense : sense + 1, :]
            decay = jnp.exp(log_decay)
            a_ref[pl.ds(to, rows), :] = decay
            b_ref[pl.ds(to, rows), :] = jnp.sqrt(one_minus_square(log_decay, decay)) * (inner * signal)
        return carry

    lax.fori_loop(0, length // rows, gates, 0)

    def advance(t, carry):
        hf, pf, hb, pb = carry
        back = step - 1 - t
        af = a_f[pl.ds(t, SEGS, stride=stride), :]
        bf = b_f[pl.ds(t, SEGS, stride=stride), :]
        ab = a_b[pl.ds(back, SEGS, stride=stride), :]
        bb = b_b[pl.ds(back, SEGS, stride=stride), :]
        hf = af * hf + bf
        pf = pf * af
        hb = ab * hb + bb
        pb = pb * ab
        here = pl.multiple_of(t * SEGS, SEGS)
        there = pl.multiple_of(back * SEGS, SEGS)
        h_f[pl.ds(here, SEGS), :] = hf
        p_f[pl.ds(here, SEGS), :] = pf
        h_b[pl.ds(there, SEGS), :] = hb
        p_b[pl.ds(there, SEGS), :] = pb
        return hf, pf, hb, pb

    none = jnp.zeros((SEGS, 128), F32)
    ones = jnp.ones((SEGS, 128), F32)
    hf, pf, hb, pb = lax.fori_loop(0, step, advance, (none, ones, none, ones), unroll=8)

    sums = []
    for base, h, p, order in ((0, hf, pf, range(SEGS)), (16, hb, pb, reversed(range(SEGS)))):
        enter = jnp.zeros((1, 128), F32)
        factor = jnp.ones((1, 128), F32)
        for s in order:
            seg[base + s : base + s + 1, :] = enter
            seg[base + 8 + s : base + 9 + s, :] = factor
            enter = p[s : s + 1, :] * enter + h[s : s + 1, :]
            factor = p[s : s + 1, :] * factor
        sums += [factor, enter]
    both = jnp.concatenate(sums + [jnp.zeros((4, 128), F32)], axis=0)
    total[...] = jnp.broadcast_to(both[None], total.shape)


def mix_kernel(h_f, p_f, h_b, p_b, seg, totals, gate_h, out, natural, gate_in, sems):
    (copy,) = fetched((gate_h,), (gate_in,), sems)
    length = out.shape[0]
    step = length // SEGS
    stride = step + 8
    count = totals.shape[0]
    here = lax.axis_index("sp")
    enter_f = jnp.zeros((1, 128), F32)
    enter_b = jnp.zeros((1, 128), F32)
    for j in range(count):
        enter_f = jnp.where(j < here, totals[j, 0:1, :] * enter_f + totals[j, 1:2, :], enter_f)
        k = count - 1 - j
        enter_b = jnp.where(k > here, totals[k, 2:3, :] * enter_b + totals[k, 3:4, :], enter_b)
    into_f = seg[0:8, :] + seg[8:16, :] * enter_f
    into_b = seg[16:24, :] + seg[24:32, :] * enter_b

    def place(t, carry):
        at = pl.multiple_of(t * SEGS, SEGS)
        rows = pl.ds(at, SEGS)
        natural[pl.ds(t, SEGS, stride=stride), :] = (
            h_f[rows, :] + p_f[rows, :] * into_f + (h_b[rows, :] + p_b[rows, :] * into_b)
        )
        return carry

    lax.fori_loop(0, step, place, 0, unroll=8)
    copy.wait()
    for s in range(SEGS):
        gate = gate_in[s * step : (s + 1) * step, :].astype(F32)
        out[s * step : (s + 1) * step, :] = (
            natural[s * stride : s * stride + step, :] * jax.nn.gelu(gate)
        ).astype(BF16)


def scaled(values, gain):
    return values * lax.rsqrt(jnp.mean(values * values, axis=-1, keepdims=True) + EPSILON) * gain


def proj_kernel(mixed, weights_h, residual_h, gain_h, routes, stream_out, outgoing_h, weights, residual, gain, outgoing, sems):
    width = weights.shape[0]
    blocks = 8
    block = width // blocks
    parts = [(weights_h.at[pl.ds(k * block, block)], weights.at[pl.ds(k * block, block)]) for k in range(blocks)]
    loads = fetched(*zip(*parts), sems)
    others = fetched((residual_h, gain_h), (residual, gain), sems, blocks)
    acc = jnp.zeros(residual.shape, F32)
    per = mixed.shape[0] // blocks
    for k in range(blocks):
        lanes = jnp.concatenate([mixed[k * per + j] for j in range(per)], axis=1)
        loads[k].wait()
        acc = acc + jnp.dot(lanes, weights[k * block : (k + 1) * block, :], preferred_element_type=F32)
    for copy in others:
        copy.wait()
    proj = acc.astype(BF16).astype(F32)
    stream = (residual[...].astype(F32) + scaled(proj, gain[0:1, :])).astype(BF16)
    stream_out[...] = stream
    normed = scaled(stream.astype(F32), gain[1:2, :]).astype(BF16)
    rows = normed.shape[0]
    slots = outgoing.shape[0]
    experts = 16
    capacity = slots // experts
    first, second = routes[0:1, :], routes[1:2, :]
    ids = lax.broadcasted_iota(jnp.int32, (experts, rows), 0)
    hit0 = (ids == first).astype(F32)
    hit1 = (ids == second).astype(F32)
    r = lax.broadcasted_iota(jnp.int32, (rows, rows), 0)
    c = lax.broadcasted_iota(jnp.int32, (rows, rows), 1)
    earlier = jnp.dot((hit0 + hit1).astype(BF16), (r < c).astype(BF16), preferred_element_type=F32)
    slot0 = first * capacity + jnp.sum(hit0 * earlier, axis=0, keepdims=True).astype(jnp.int32)
    slot1 = second * capacity + jnp.sum(hit1 * earlier, axis=0, keepdims=True).astype(jnp.int32)
    places = lax.broadcasted_iota(jnp.int32, (slots, rows), 0)
    pick = jnp.where(jnp.logical_or(places == slot0, places == slot1), 1.0, 0.0).astype(BF16)
    sent = []
    for k in range(4):
        part = slice(k * 512, (k + 1) * 512)
        outgoing[:, part] = jnp.dot(pick, normed[:, part], preferred_element_type=F32).astype(BF16)
        sent += fetched([outgoing.at[:, part]], [outgoing_h.at[:, part]], sems, 10 + k)
    for copy in sent:
        copy.wait()


def pack_kernel(gate, up, down, out, buffer, sems):
    ff = gate.shape[0]
    refs = (gate, up, down)
    parts = [pl.ds(j * ff, ff) for j in range(3)]
    inward = fetched(refs, [buffer.at[part] for part in parts], sems)
    outward = []
    for copy, part in zip(inward, parts):
        copy.wait()
        outward += fetched([buffer.at[part]], [out.at[part]], sems, 3 + len(outward))
    for copy in outward:
        copy.wait()


def expert_kernel(*refs, pieces, head, tail):
    tokens, shares = refs[0], refs[1 : 1 + pieces]
    rest = refs[1 + pieces :]
    if not head:
        before, rest = rest[0], rest[1:]
    out, gate_w, up_w, down_w, sems = rest[:5]
    ff = shares[0].shape[0] // 3
    copies = [
        fetched(
            [share.at[pl.ds(j * ff, ff)] for j in range(3)],
            [w.at[pl.ds(at * ff, ff)] for w in (gate_w, up_w, down_w)],
            sems,
            3 * at,
        )
        for at, share in enumerate(shares)
    ]
    x = tokens[...]
    acc = jnp.zeros(x.shape, F32) if head else before[...]
    block = 256
    last = (((1,), (1,)), ((), ()))
    for k in range(pieces * ff // block):
        for piece in range(k * block // ff, (k + 1) * block // ff):
            for copy in copies[piece]:
                copy.wait()
        rows = slice(k * block, (k + 1) * block)
        gate = lax.dot_general(x, gate_w[rows, :], last, preferred_element_type=F32)
        up = lax.dot_general(x, up_w[rows, :], last, preferred_element_type=F32)
        hidden = (jax.nn.silu(gate) * up).astype(BF16)
        acc = acc + jnp.dot(hidden, down_w[rows, :], preferred_element_type=F32)
    if tail:
        result, done = rest[5:]
        result[...] = acc.astype(BF16)
        copy = pltpu.make_async_copy(result, out, done.at[0])
        copy.start()
        copy.wait()
    else:
        out[...] = acc


def combine_kernel(values, stream, gain, routes, weights, out):
    rows = stream.shape[0]
    slots = values.shape[0]
    experts = 16
    capacity = slots // experts
    first, second = routes[:, 0:1], routes[:, 1:2]
    ids = lax.broadcasted_iota(jnp.int32, (rows, experts), 1)
    hit0 = (ids == first).astype(F32)
    hit1 = (ids == second).astype(F32)
    r = lax.broadcasted_iota(jnp.int32, (rows, rows), 0)
    c = lax.broadcasted_iota(jnp.int32, (rows, rows), 1)
    earlier = jnp.dot((c < r).astype(BF16), (hit0 + hit1).astype(BF16), preferred_element_type=F32)
    slot0 = first * capacity + jnp.sum(hit0 * earlier, axis=1, keepdims=True).astype(jnp.int32)
    slot1 = second * capacity + jnp.sum(hit1 * earlier, axis=1, keepdims=True).astype(jnp.int32)
    places = lax.broadcasted_iota(jnp.int32, (rows, slots), 1)
    table = jnp.where(places == slot0, weights[:, 0:1], 0.0) + jnp.where(
        places == slot1, weights[:, 1:2], 0.0
    )
    high = table.astype(BF16)
    rest = table - high.astype(F32)
    mid = rest.astype(BF16)
    low = (rest - mid.astype(F32)).astype(BF16)
    parts = jnp.dot(jnp.concatenate([high, mid, low], axis=0), values[...], preferred_element_type=F32)
    mixture = parts[0:rows] + (parts[rows : 2 * rows] + parts[2 * rows : 3 * rows])
    mixture = mixture.astype(BF16).astype(F32)
    out[...] = (stream[...].astype(F32) + scaled(mixture, gain[2:3, :])).astype(BF16)


def shape(dims, dtype):
    return jax.ShapeDtypeStruct(dims, dtype)


def layer(
    mix_in,
    gate_in,
    conv_w,
    conv_b,
    decay_param,
    recur_gate,
    recur_bias,
    input_gate,
    input_bias,
    residual,
    out_proj,
    norm_gain,
    routes,
    route_wt,
    exp_gate,
    exp_up,
    exp_down,
):
    length, channels = mix_in.shape
    rows, width = residual.shape
    sp = lax.axis_size("sp")
    tp = lax.axis_size("tp")
    ends = sp - 1
    before = lax.ppermute(mix_in[length - 2 :], "sp", [(i, i + 1) for i in range(ends)])
    after = lax.ppermute(mix_in[:2], "sp", [(i + 1, i) for i in range(ends)])
    ff_own = exp_down.shape[1]
    piece = shape((3 * ff_own, width), BF16)
    own = pl.pallas_call(
        pack_kernel,
        out_shape=piece,
        in_specs=[in_hbm()] * 3,
        out_specs=in_hbm(),
        scratch_shapes=[pltpu.VMEM(piece.shape, BF16), pltpu.SemaphoreType.DMA((6,))],
        name="pack",
    )(jnp.swapaxes(exp_gate, 1, 2)[0], jnp.swapaxes(exp_up, 1, 2)[0], exp_down[0])

    def around(part):
        return lax.ppermute(part, "tp", [(i, (i + 2 - 4 * (i % 2)) % tp) for i in range(tp)])

    def across(part):
        return lax.ppermute(part, "tp", [(i, i ^ 1) for i in range(tp)])

    other = across(own)
    r1a = around(own)
    r1b = around(other)
    step = length // SEGS
    lines = SEGS * (step + 8)
    state = shape((length, channels), F32)
    h_f, p_f, h_b, p_b, seg, total = pl.pallas_call(
        scan_kernel,
        out_shape=(state, state, state, state, shape((32, 128), F32), shape((sp, 8, 128), F32)),
        in_specs=[anywhere(), whole(), whole()] + [anywhere()] * 7,
        out_specs=(whole(),) * 6,
        scratch_shapes=[
            pltpu.VMEM((length + 16, 128), F32),
            pltpu.VMEM((length, 128), F32),
            pltpu.VMEM((length, 256), BF16),
            pltpu.VMEM((256, 512), BF16),
            pltpu.VMEM((128, 512), BF16),
            pltpu.VMEM((length, 512), F32),
            pltpu.VMEM((lines, 128), F32),
            pltpu.VMEM((lines, 128), F32),
            pltpu.VMEM((lines, 128), F32),
            pltpu.VMEM((lines, 128), F32),
            pltpu.VMEM(mix_in.shape, BF16),
            pltpu.VMEM(conv_w.shape, F32),
            pltpu.VMEM((1, 128), F32),
            pltpu.VMEM(decay_param.shape, F32),
            pltpu.VMEM(recur_gate.shape, F32),
            pltpu.VMEM(recur_bias.shape, F32),
            pltpu.VMEM(input_gate.shape, F32),
            pltpu.VMEM(input_bias.shape, F32),
            pltpu.SemaphoreType.DMA((8,)),
        ],
        compiler_params=params(20),
        name="scan",
    )(mix_in, before, after, conv_w, conv_b[None], decay_param, recur_gate, recur_bias, input_gate, input_bias)
    total, r1a = lax.optimization_barrier((total, r1a))
    r2a, e1a = around(r1a), across(r1a)
    totals = lax.all_to_all(total, "sp", split_axis=0, concat_axis=0, tiled=True)
    totals, r1b = lax.optimization_barrier((totals, r1b))
    r2b, e1b = around(r1b), across(r1b)
    mixed = pl.pallas_call(
        mix_kernel,
        out_shape=shape((length, channels), BF16),
        in_specs=[whole()] * 6 + [anywhere()],
        out_specs=whole(),
        scratch_shapes=[
            pltpu.VMEM((lines, 128), F32),
            pltpu.VMEM((length, channels), BF16),
            pltpu.SemaphoreType.DMA((1,)),
        ],
        compiler_params=params(12),
        name="mix",
    )(h_f, p_f, h_b, p_b, seg, totals, gate_in)
    token_rows = lax.all_to_all(
        mixed.reshape(tp, rows, channels), "tp", split_axis=0, concat_axis=0, tiled=True
    )
    r3a, e2a = around(r2a), across(r2a)
    first_row = lax.axis_index("tp") * rows
    own_routes = lax.dynamic_slice_in_dim(routes, first_row, rows, 0)
    own_weights = lax.dynamic_slice_in_dim(route_wt, first_row, rows, 0)
    slots = 2 * rows * routes.shape[1]
    project = pl.pallas_call(
        proj_kernel,
        out_shape=(shape((rows, width), BF16), shape((slots, width), BF16)),
        in_specs=[whole(), in_hbm(), anywhere(), anywhere(), whole()],
        out_specs=(whole(), in_hbm()),
        scratch_shapes=[
            pltpu.VMEM(out_proj.shape, BF16),
            pltpu.VMEM(residual.shape, BF16),
            pltpu.VMEM(norm_gain.shape, F32),
            pltpu.VMEM((slots, width), BF16),
            pltpu.SemaphoreType.DMA((14,)),
        ],
        compiler_params=params(16),
        name="proj",
    )
    stream, outgoing = project(token_rows, out_proj, residual, norm_gain, own_routes.T)
    r3b, e2b = around(r2b), across(r2b)
    r4, e3a = around(r3a), across(r3a)
    e3b, e4 = across(r3b), across(r4)
    arrived = lax.all_to_all(outgoing.reshape(sp, slots // sp, width), "sp", split_axis=0, concat_axis=0, tiled=True)
    arrived = arrived.reshape(slots, width)

    def experts(shares, before, tail):
        count = len(shares)
        tall = count * ff_own
        scratch = [pltpu.VMEM((tall, width), BF16)] * 3 + [pltpu.SemaphoreType.DMA((3 * count,))]
        if tail:
            scratch += [pltpu.VMEM((slots, width), BF16), pltpu.SemaphoreType.DMA((1,))]
        head = before is None
        return pl.pallas_call(
            functools.partial(expert_kernel, pieces=count, head=head, tail=tail),
            out_shape=shape((slots, width), BF16 if tail else F32),
            in_specs=[whole()] + [in_hbm()] * count + [whole()] * (not head),
            out_specs=in_hbm() if tail else whole(),
            scratch_shapes=scratch,
            compiler_params=params(24),
            name="experts_tail" if tail else "experts_head",
        )(arrived, *shares, *([] if head else [before]))

    first = experts((own, other, r1a, e1a, r1b, e1b, r2a, e2a, r2b, e2b, r3a, e3a), None, False)
    done = experts((r3b, e3b, r4, e4), first, True)
    returned = lax.all_to_all(
        done.reshape(sp, slots // sp, width), "sp", split_axis=0, concat_axis=0, tiled=True
    )
    return pl.pallas_call(
        combine_kernel,
        out_shape=shape((rows, width), BF16),
        in_specs=[whole()] * 5,
        out_specs=whole(),
        compiler_params=params(16),
        name="combine",
    )(returned.reshape(slots, width), stream, norm_gain, own_routes, own_weights)


def solution(mesh):
    return jax.shard_map(
        layer,
        mesh=mesh,
        in_specs=(
            P("sp", "tp"),
            P("sp", "tp"),
            P(None, "tp"),
            P("tp"),
            P(None, "tp"),
            P(None, "tp", None, None),
            P(None, "tp"),
            P(None, "tp", None, None),
            P(None, "tp"),
            P(("sp", "tp"), None),
            P(),
            P(),
            P("sp", None),
            P("sp", None),
            P("sp", None, "tp"),
            P("sp", None, "tp"),
            P("sp", "tp", None),
        ),
        out_specs=P(("sp", "tp"), None),
        check_vma=False,
    )
```

```python
import functools

import jax
import jax.numpy as jnp
from jax import lax
from jax.experimental import pallas as pl
from jax.experimental.pallas import tpu as pltpu
from jax.sharding import PartitionSpec as P


EPSILON = 1e-06
F32 = jnp.float32
BF16 = jnp.bfloat16
SEGS = 8


FULL = pltpu.CompilerParams(vmem_limit_bytes=67043328)


def anywhere():
    return pl.BlockSpec(memory_space=pl.ANY)


def in_hbm():
    return pl.BlockSpec(memory_space=pltpu.MemorySpace.HBM)


def fetched(sources, buffers, sems, first=0):
    copies = [pltpu.make_async_copy(src, dst, sems.at[first + k]) for k, (src, dst) in enumerate(zip(sources, buffers))]
    for copy in copies:
        copy.start()
    return copies


def one_minus_square(log_decay, decay):
    y = 2.0 * log_decay
    series = 1.0 + y * (1.0 / 7.0)
    for k in (6.0, 5.0, 4.0, 3.0, 2.0):
        series = 1.0 + y * (1.0 / k) * series
    return jnp.where(y > -0.5, -y * series, 1.0 - decay * decay)


def softplus_of(x):
    u = jnp.exp(-jnp.abs(x))
    z = u / (2.0 + u)
    z2 = z * z
    series = jnp.full_like(z, 1.0 / 17.0)
    for k in (15.0, 13.0, 11.0, 9.0, 7.0, 5.0, 3.0, 1.0):
        series = 1.0 / k + z2 * series
    return jnp.maximum(x, 0.0) + 2.0 * z * series


def scan_kernel(
    mix_h, before_h, after_h, conv_w_h, conv_b_h, decay_param_h, recur_gate_h, recur_bias_h, input_gate_h, input_bias_h,
    h_f_h, p_f_h, h_b_h, p_b_h, seg_h, total_h,
    padded, conv, split, wide, wlow, pre, a_f, b_f, a_b, b_b,
    mix, before, after, conv_w, conv_b, decay_param, recur_gate, recur_bias, input_gate, input_bias,
    h_f, p_f, h_b, p_b, seg, total, sems,
):
    for copy in fetched(
        (
            mix_h, before_h, after_h, conv_w_h, conv_b_h, decay_param_h,
            recur_gate_h, recur_bias_h, input_gate_h, input_bias_h,
        ),
        (mix, before, after, conv_w, conv_b, decay_param, recur_gate, recur_bias, input_gate, input_bias),
        sems,
    ):
        copy.wait()
    length = mix.shape[0]
    step = length // SEGS
    stride = step + 8
    padded[0:8, :] = jnp.zeros((8, 128), F32)
    padded[6:8, :] = before[...].astype(F32)
    padded[8 : 8 + length, :] = mix[...].astype(F32)
    padded[8 + length : 16 + length, :] = jnp.zeros((8, 128), F32)
    padded[8 + length : 10 + length, :] = after[...].astype(F32)
    zero = jnp.zeros((64, 64), F32)
    columns = []
    for sense in range(2):
        for gate in (recur_gate, input_gate):
            columns.append(
                jnp.concatenate(
                    [
                        jnp.concatenate([gate[sense, 0], zero], axis=1),
                        jnp.concatenate([zero, gate[sense, 1]], axis=1),
                    ],
                    axis=0,
                )
            )
    maps = jnp.concatenate(columns, axis=1)
    high = maps.astype(BF16)
    wide[0:128, :] = high
    wide[128:256, :] = high
    wlow[...] = (maps - high.astype(F32)).astype(BF16)

    rows = 64

    def convolve(k, carry):
        at = pl.multiple_of(k * rows, rows)
        out = conv_b[...] + padded[pl.ds(at + 6, rows), :] * conv_w[0:1, :]
        for tap in range(1, 4):
            out = out + padded[pl.ds(at + 6 + tap, rows), :] * conv_w[tap : tap + 1, :]
        conv[pl.ds(at, rows), :] = out
        top = out.astype(BF16)
        split[pl.ds(at, rows), 0:128] = top
        split[pl.ds(at, rows), 128:256] = (out - top.astype(F32)).astype(BF16)
        return carry

    lax.fori_loop(0, length // rows, convolve, 0)
    pre[...] = jnp.dot(split[...], wide[...], preferred_element_type=F32) + jnp.dot(
        split[:, 0:128], wlow[...], preferred_element_type=F32
    )
    rate = -8.0 * softplus_of(-decay_param[...])

    per = step // rows

    def gates(k, carry):
        at = pl.multiple_of(k * rows, rows)
        to = pl.multiple_of((k // per) * stride + (k % per) * rows, 8)
        signal = conv[pl.ds(at, rows), :]
        for sense, (a_ref, b_ref) in enumerate(((a_f, b_f), (a_b, b_b))):
            base = sense * 256
            recur = jax.nn.sigmoid(pre[pl.ds(at, rows), base : base + 128] + recur_bias[sense : sense + 1, :])
            inner = jax.nn.sigmoid(pre[pl.ds(at, rows), base + 128 : base + 256] + input_bias[sense : sense + 1, :])
            log_decay = recur * rate[sense : sense + 1, :]
            decay = jnp.exp(log_decay)
            a_ref[pl.ds(to, rows), :] = decay
            b_ref[pl.ds(to, rows), :] = jnp.sqrt(one_minus_square(log_decay, decay)) * (inner * signal)
        return carry

    lax.fori_loop(0, length // rows, gates, 0)

    def advance(t, carry):
        hf, pf, hb, pb = carry
        back = step - 1 - t
        af = a_f[pl.ds(t, SEGS, stride=stride), :]
        bf = b_f[pl.ds(t, SEGS, stride=stride), :]
        ab = a_b[pl.ds(back, SEGS, stride=stride), :]
        bb = b_b[pl.ds(back, SEGS, stride=stride), :]
        hf = af * hf + bf
        pf = pf * af
        hb = ab * hb + bb
        pb = pb * ab
        here = pl.multiple_of(t * SEGS, SEGS)
        there = pl.multiple_of(back * SEGS, SEGS)
        h_f[pl.ds(here, SEGS), :] = hf
        p_f[pl.ds(here, SEGS), :] = pf
        h_b[pl.ds(there, SEGS), :] = hb
        p_b[pl.ds(there, SEGS), :] = pb
        return hf, pf, hb, pb

    none = jnp.zeros((SEGS, 128), F32)
    ones = jnp.ones((SEGS, 128), F32)
    hf, pf, hb, pb = lax.fori_loop(0, step, advance, (none, ones, none, ones), unroll=8)

    sums = []
    for base, h, p, order in ((0, hf, pf, range(SEGS)), (16, hb, pb, reversed(range(SEGS)))):
        enter = jnp.zeros((1, 128), F32)
        factor = jnp.ones((1, 128), F32)
        for s in order:
            seg[base + s : base + s + 1, :] = enter
            seg[base + 8 + s : base + 9 + s, :] = factor
            enter = p[s : s + 1, :] * enter + h[s : s + 1, :]
            factor = p[s : s + 1, :] * factor
        sums += [factor, enter]
    both = jnp.concatenate(sums + [jnp.zeros((4, 128), F32)], axis=0)
    total[...] = jnp.broadcast_to(both[None], total.shape)
    for copy in fetched((h_f, p_f, h_b, p_b, seg, total), (h_f_h, p_f_h, h_b_h, p_b_h, seg_h, total_h), sems, 10):
        copy.wait()


def mix_kernel(*refs):
    sources, out_h, natural, buffers, out, sems = refs[:7], refs[7], refs[8], refs[9:16], refs[16], refs[17]
    h_f, p_f, h_b, p_b, seg, totals, gate_in = buffers
    for copy in fetched(sources, buffers, sems):
        copy.wait()
    length = out.shape[0]
    step = length // SEGS
    stride = step + 8
    count = totals.shape[0]
    here = lax.axis_index("sp")
    enter_f = jnp.zeros((1, 128), F32)
    enter_b = jnp.zeros((1, 128), F32)
    for j in range(count):
        enter_f = jnp.where(j < here, totals[j, 0:1, :] * enter_f + totals[j, 1:2, :], enter_f)
        k = count - 1 - j
        enter_b = jnp.where(k > here, totals[k, 2:3, :] * enter_b + totals[k, 3:4, :], enter_b)
    into_f = seg[0:8, :] + seg[8:16, :] * enter_f
    into_b = seg[16:24, :] + seg[24:32, :] * enter_b

    def place(t, carry):
        at = pl.multiple_of(t * SEGS, SEGS)
        rows = pl.ds(at, SEGS)
        natural[pl.ds(t, SEGS, stride=stride), :] = (
            h_f[rows, :] + p_f[rows, :] * into_f + (h_b[rows, :] + p_b[rows, :] * into_b)
        )
        return carry

    lax.fori_loop(0, step, place, 0, unroll=8)
    for s in range(SEGS):
        gate = gate_in[s * step : (s + 1) * step, :].astype(F32)
        out[s * step : (s + 1) * step, :] = (
            natural[s * stride : s * stride + step, :] * jax.nn.gelu(gate)
        ).astype(BF16)
    (copy,) = fetched((out,), (out_h,), sems, 7)
    copy.wait()


def scaled(values, gain):
    return values * lax.rsqrt(jnp.mean(values * values, axis=-1, keepdims=True) + EPSILON) * gain


def proj_kernel(
    mixed_h, weights_h, residual_h, gain_h, routes_h, stream_h, outgoing_h,
    mixed, weights, residual, gain, routes, stream_out, outgoing, sems,
):
    (mixed_copy,) = fetched((mixed_h,), (mixed,), sems, 15)
    width = weights.shape[0]
    blocks = 8
    block = width // blocks
    parts = [(weights_h.at[pl.ds(k * block, block)], weights.at[pl.ds(k * block, block)]) for k in range(blocks)]
    loads = fetched(*zip(*parts), sems)
    others = fetched((residual_h, gain_h, routes_h), (residual, gain, routes), sems, blocks)
    mixed_copy.wait()
    acc = jnp.zeros(residual.shape, F32)
    per = mixed.shape[0] // blocks
    for k in range(blocks):
        lanes = jnp.concatenate([mixed[k * per + j] for j in range(per)], axis=1)
        loads[k].wait()
        acc = acc + jnp.dot(lanes, weights[k * block : (k + 1) * block, :], preferred_element_type=F32)
    for copy in others:
        copy.wait()
    proj = acc.astype(BF16).astype(F32)
    stream = (residual[...].astype(F32) + scaled(proj, gain[0:1, :])).astype(BF16)
    stream_out[...] = stream
    sent = fetched((stream_out,), (stream_h,), sems, 16)
    normed = scaled(stream.astype(F32), gain[1:2, :]).astype(BF16)
    rows = normed.shape[0]
    slots = outgoing.shape[0]
    experts = 16
    capacity = slots // experts
    first, second = routes[0:1, :], routes[1:2, :]
    ids = lax.broadcasted_iota(jnp.int32, (experts, rows), 0)
    hit0 = (ids == first).astype(F32)
    hit1 = (ids == second).astype(F32)
    r = lax.broadcasted_iota(jnp.int32, (rows, rows), 0)
    c = lax.broadcasted_iota(jnp.int32, (rows, rows), 1)
    earlier = jnp.dot((hit0 + hit1).astype(BF16), (r < c).astype(BF16), preferred_element_type=F32)
    slot0 = first * capacity + jnp.sum(hit0 * earlier, axis=0, keepdims=True).astype(jnp.int32)
    slot1 = second * capacity + jnp.sum(hit1 * earlier, axis=0, keepdims=True).astype(jnp.int32)
    places = lax.broadcasted_iota(jnp.int32, (slots, rows), 0)
    pick = jnp.where(jnp.logical_or(places == slot0, places == slot1), 1.0, 0.0).astype(BF16)
    for k in range(4):
        part = slice(k * 512, (k + 1) * 512)
        outgoing[:, part] = jnp.dot(pick, normed[:, part], preferred_element_type=F32).astype(BF16)
        sent += fetched([outgoing.at[:, part]], [outgoing_h.at[:, part]], sems, 11 + k)
    for copy in sent:
        copy.wait()


def pack_kernel(gate, up, down, out, buffer, sems):
    ff = gate.shape[0]
    refs = (gate, up, down)
    parts = [pl.ds(j * ff, ff) for j in range(3)]
    inward = fetched(refs, [buffer.at[part] for part in parts], sems)
    outward = []
    for copy, part in zip(inward, parts):
        copy.wait()
        outward += fetched([buffer.at[part]], [out.at[part]], sems, 3 + len(outward))
    for copy in outward:
        copy.wait()


def expert_kernel(*refs, pieces, head, tail):
    tokens, shares = refs[0], refs[1 : 1 + pieces]
    rest = refs[1 + pieces :]
    if not head:
        before, rest = rest[0], rest[1:]
    out, gate_w, up_w, down_w, held, acc_held, sems, extra = rest
    starts = fetched((tokens,), (held,), extra) + ([] if head else fetched((before,), (acc_held,), extra, 1))
    ff = shares[0].shape[0] // 3
    copies = [
        fetched(
            [share.at[pl.ds(j * ff, ff)] for j in range(3)],
            [w.at[pl.ds(at * ff, ff)] for w in (gate_w, up_w, down_w)],
            sems,
            3 * at,
        )
        for at, share in enumerate(shares)
    ]
    for copy in starts:
        copy.wait()
    x = held[...]
    acc = jnp.zeros(x.shape, F32) if head else acc_held[...]
    block = 256
    last = (((1,), (1,)), ((), ()))
    for k in range(pieces * ff // block):
        for piece in range(k * block // ff, (k + 1) * block // ff):
            for copy in copies[piece]:
                copy.wait()
        rows = slice(k * block, (k + 1) * block)
        gate = lax.dot_general(x, gate_w[rows, :], last, preferred_element_type=F32)
        up = lax.dot_general(x, up_w[rows, :], last, preferred_element_type=F32)
        hidden = (jax.nn.silu(gate) * up).astype(BF16)
        acc = acc + jnp.dot(hidden, down_w[rows, :], preferred_element_type=F32)
    result = held if tail else acc_held
    result[...] = acc.astype(result.dtype)
    (copy,) = fetched((result,), (out,), extra, 2)
    copy.wait()


def combine_kernel(*refs):
    sources, out_h, buffers, out, sems = refs[:5], refs[5], refs[6:11], refs[11], refs[12]
    values, stream, gain, routes, weights = buffers
    for copy in fetched(sources, buffers, sems):
        copy.wait()
    rows = stream.shape[0]
    slots = values.shape[0]
    experts = 16
    capacity = slots // experts
    first, second = routes[:, 0:1], routes[:, 1:2]
    ids = lax.broadcasted_iota(jnp.int32, (rows, experts), 1)
    hit0 = (ids == first).astype(F32)
    hit1 = (ids == second).astype(F32)
    r = lax.broadcasted_iota(jnp.int32, (rows, rows), 0)
    c = lax.broadcasted_iota(jnp.int32, (rows, rows), 1)
    earlier = jnp.dot((c < r).astype(BF16), (hit0 + hit1).astype(BF16), preferred_element_type=F32)
    slot0 = first * capacity + jnp.sum(hit0 * earlier, axis=1, keepdims=True).astype(jnp.int32)
    slot1 = second * capacity + jnp.sum(hit1 * earlier, axis=1, keepdims=True).astype(jnp.int32)
    places = lax.broadcasted_iota(jnp.int32, (rows, slots), 1)
    table = jnp.where(places == slot0, weights[:, 0:1], 0.0) + jnp.where(
        places == slot1, weights[:, 1:2], 0.0
    )
    high = table.astype(BF16)
    rest = table - high.astype(F32)
    mid = rest.astype(BF16)
    low = (rest - mid.astype(F32)).astype(BF16)
    parts = jnp.dot(jnp.concatenate([high, mid, low], axis=0), values[...], preferred_element_type=F32)
    mixture = parts[0:rows] + (parts[rows : 2 * rows] + parts[2 * rows : 3 * rows])
    mixture = mixture.astype(BF16).astype(F32)
    out[...] = (stream[...].astype(F32) + scaled(mixture, gain[2:3, :])).astype(BF16)
    (copy,) = fetched((out,), (out_h,), sems, 5)
    copy.wait()


def shape(dims, dtype):
    return jax.ShapeDtypeStruct(dims, dtype)


def layer(
    mix_in,
    gate_in,
    conv_w,
    conv_b,
    decay_param,
    recur_gate,
    recur_bias,
    input_gate,
    input_bias,
    residual,
    out_proj,
    norm_gain,
    routes,
    route_wt,
    exp_gate,
    exp_up,
    exp_down,
):
    length, channels = mix_in.shape
    rows, width = residual.shape
    sp = lax.axis_size("sp")
    tp = lax.axis_size("tp")
    ends = sp - 1
    before = lax.ppermute(mix_in[length - 2 :], "sp", [(i, i + 1) for i in range(ends)])
    after = lax.ppermute(mix_in[:2], "sp", [(i + 1, i) for i in range(ends)])
    ff_own = exp_down.shape[1]
    piece = shape((3 * ff_own, width), BF16)
    own = pl.pallas_call(
        pack_kernel,
        out_shape=piece,
        in_specs=[in_hbm()] * 3,
        out_specs=in_hbm(),
        scratch_shapes=[pltpu.VMEM(piece.shape, BF16), pltpu.SemaphoreType.DMA((6,))],
        compiler_params=FULL,
        name="pack",
    )(jnp.swapaxes(exp_gate, 1, 2)[0], jnp.swapaxes(exp_up, 1, 2)[0], exp_down[0])

    def around(part):
        return lax.ppermute(part, "tp", [(i, (i + 2 - 4 * (i % 2)) % tp) for i in range(tp)])

    def across(part):
        return lax.ppermute(part, "tp", [(i, i ^ 1) for i in range(tp)])

    other = across(own)
    r1a = around(own)
    r1b = around(other)
    step = length // SEGS
    lines = SEGS * (step + 8)
    state = shape((length, channels), F32)
    h_f, p_f, h_b, p_b, seg, total = pl.pallas_call(
        scan_kernel,
        out_shape=(state, state, state, state, shape((32, 128), F32), shape((sp, 8, 128), F32)),
        in_specs=[anywhere()] * 10,
        out_specs=(anywhere(),) * 6,
        scratch_shapes=[
            pltpu.VMEM((length + 16, 128), F32),
            pltpu.VMEM((length, 128), F32),
            pltpu.VMEM((length, 256), BF16),
            pltpu.VMEM((256, 512), BF16),
            pltpu.VMEM((128, 512), BF16),
            pltpu.VMEM((length, 512), F32),
            pltpu.VMEM((lines, 128), F32),
            pltpu.VMEM((lines, 128), F32),
            pltpu.VMEM((lines, 128), F32),
            pltpu.VMEM((lines, 128), F32),
            pltpu.VMEM(mix_in.shape, BF16),
            pltpu.VMEM(before.shape, BF16),
            pltpu.VMEM(after.shape, BF16),
            pltpu.VMEM(conv_w.shape, F32),
            pltpu.VMEM((1, 128), F32),
            pltpu.VMEM(decay_param.shape, F32),
            pltpu.VMEM(recur_gate.shape, F32),
            pltpu.VMEM(recur_bias.shape, F32),
            pltpu.VMEM(input_gate.shape, F32),
            pltpu.VMEM(input_bias.shape, F32),
            pltpu.VMEM(state.shape, F32),
            pltpu.VMEM(state.shape, F32),
            pltpu.VMEM(state.shape, F32),
            pltpu.VMEM(state.shape, F32),
            pltpu.VMEM((32, 128), F32),
            pltpu.VMEM((sp, 8, 128), F32),
            pltpu.SemaphoreType.DMA((16,)),
        ],
        compiler_params=FULL,
        name="scan",
    )(mix_in, before, after, conv_w, conv_b[None], decay_param, recur_gate, recur_bias, input_gate, input_bias)
    total, r1a = lax.optimization_barrier((total, r1a))
    r2a, e1a = around(r1a), across(r1a)
    totals = lax.all_to_all(total, "sp", split_axis=0, concat_axis=0, tiled=True)
    totals, r1b = lax.optimization_barrier((totals, r1b))
    r2b, e1b = around(r1b), across(r1b)
    mixed = pl.pallas_call(
        mix_kernel,
        out_shape=shape((length, channels), BF16),
        in_specs=[anywhere()] * 7,
        out_specs=anywhere(),
        scratch_shapes=[pltpu.VMEM((lines, 128), F32)]
        + [pltpu.VMEM(state.shape, F32)] * 4
        + [
            pltpu.VMEM((32, 128), F32),
            pltpu.VMEM((sp, 8, 128), F32),
            pltpu.VMEM((length, channels), BF16),
            pltpu.VMEM((length, channels), BF16),
            pltpu.SemaphoreType.DMA((8,)),
        ],
        compiler_params=FULL,
        name="mix",
    )(h_f, p_f, h_b, p_b, seg, totals, gate_in)
    token_rows = lax.all_to_all(
        mixed.reshape(tp, rows, channels), "tp", split_axis=0, concat_axis=0, tiled=True
    )
    r3a, e2a = around(r2a), across(r2a)
    first_row = lax.axis_index("tp") * rows
    own_routes = lax.dynamic_slice_in_dim(routes, first_row, rows, 0)
    own_weights = lax.dynamic_slice_in_dim(route_wt, first_row, rows, 0)
    slots = 2 * rows * routes.shape[1]
    project = pl.pallas_call(
        proj_kernel,
        out_shape=(shape((rows, width), BF16), shape((slots, width), BF16)),
        in_specs=[anywhere()] * 5,
        out_specs=(anywhere(), anywhere()),
        scratch_shapes=[
            pltpu.VMEM(token_rows.shape, BF16),
            pltpu.VMEM(out_proj.shape, BF16),
            pltpu.VMEM(residual.shape, BF16),
            pltpu.VMEM(norm_gain.shape, F32),
            pltpu.VMEM((routes.shape[1], rows), jnp.int32),
            pltpu.VMEM(residual.shape, BF16),
            pltpu.VMEM((slots, width), BF16),
            pltpu.SemaphoreType.DMA((17,)),
        ],
        compiler_params=FULL,
        name="proj",
    )
    stream, outgoing = project(token_rows, out_proj, residual, norm_gain, own_routes.T)
    r3b, e2b = around(r2b), across(r2b)
    r4, e3a = around(r3a), across(r3a)
    e3b, e4 = across(r3b), across(r4)
    arrived = lax.all_to_all(outgoing.reshape(sp, slots // sp, width), "sp", split_axis=0, concat_axis=0, tiled=True)
    arrived = arrived.reshape(slots, width)

    def experts(shares, before, tail):
        count = len(shares)
        tall = count * ff_own
        scratch = [pltpu.VMEM((tall, width), BF16)] * 3 + [
            pltpu.VMEM((slots, width), BF16),
            pltpu.VMEM((slots, width), F32),
            pltpu.SemaphoreType.DMA((3 * count,)),
            pltpu.SemaphoreType.DMA((3,)),
        ]
        head = before is None
        return pl.pallas_call(
            functools.partial(expert_kernel, pieces=count, head=head, tail=tail),
            out_shape=shape((slots, width), BF16 if tail else F32),
            in_specs=[anywhere()] * (1 + count + (not head)),
            out_specs=anywhere(),
            scratch_shapes=scratch,
            compiler_params=FULL,
            name="experts_tail" if tail else "experts_head",
        )(arrived, *shares, *([] if head else [before]))

    first = experts((own, other, r1a, e1a, r1b, e1b, r2a, e2a, r2b, e2b, r3a, e3a), None, False)
    done = experts((r3b, e3b, r4, e4), first, True)
    returned = lax.all_to_all(
        done.reshape(sp, slots // sp, width), "sp", split_axis=0, concat_axis=0, tiled=True
    )
    return pl.pallas_call(
        combine_kernel,
        out_shape=shape((rows, width), BF16),
        in_specs=[anywhere()] * 5,
        out_specs=anywhere(),
        scratch_shapes=[
            pltpu.VMEM((slots, width), BF16),
            pltpu.VMEM((rows, width), BF16),
            pltpu.VMEM(norm_gain.shape, F32),
            pltpu.VMEM(own_routes.shape, jnp.int32),
            pltpu.VMEM(own_weights.shape, F32),
            pltpu.VMEM((rows, width), BF16),
            pltpu.SemaphoreType.DMA((6,)),
        ],
        compiler_params=FULL,
        name="combine",
    )(returned.reshape(slots, width), stream, norm_gain, own_routes, own_weights)


def solution(mesh):
    return jax.shard_map(
        layer,
        mesh=mesh,
        in_specs=(
            P("sp", "tp"),
            P("sp", "tp"),
            P(None, "tp"),
            P("tp"),
            P(None, "tp"),
            P(None, "tp", None, None),
            P(None, "tp"),
            P(None, "tp", None, None),
            P(None, "tp"),
            P(("sp", "tp"), None),
            P(),
            P(),
            P("sp", None),
            P("sp", None),
            P("sp", None, "tp"),
            P("sp", None, "tp"),
            P("sp", "tp", None),
        ),
        out_specs=P(("sp", "tp"), None),
        check_vma=False,
    )
```

```python
import functools

import jax
import jax.numpy as jnp
from jax import lax
from jax.experimental import pallas as pl
from jax.experimental.pallas import tpu as pltpu
from jax.sharding import PartitionSpec as P


EPSILON = 1e-06
F32 = jnp.float32
BF16 = jnp.bfloat16
SEGS = 8


FULL = pltpu.CompilerParams(vmem_limit_bytes=67043328)
ROOMY = pltpu.CompilerParams(vmem_limit_bytes=30 * 1024 * 1024)


def anywhere():
    return pl.BlockSpec(memory_space=pl.ANY)


def in_hbm():
    return pl.BlockSpec(memory_space=pltpu.MemorySpace.HBM)


def fetched(sources, buffers, sems, first=0):
    copies = [pltpu.make_async_copy(src, dst, sems.at[first + k]) for k, (src, dst) in enumerate(zip(sources, buffers))]
    for copy in copies:
        copy.start()
    return copies


def one_minus_square(log_decay, decay):
    y = 2.0 * log_decay
    series = 1.0 + y * (1.0 / 7.0)
    for k in (6.0, 5.0, 4.0, 3.0, 2.0):
        series = 1.0 + y * (1.0 / k) * series
    return jnp.where(y > -0.5, -y * series, 1.0 - decay * decay)


def softplus_of(x):
    u = jnp.exp(-jnp.abs(x))
    z = u / (2.0 + u)
    z2 = z * z
    series = jnp.full_like(z, 1.0 / 17.0)
    for k in (15.0, 13.0, 11.0, 9.0, 7.0, 5.0, 3.0, 1.0):
        series = 1.0 / k + z2 * series
    return jnp.maximum(x, 0.0) + 2.0 * z * series


def scan_kernel(
    mix_h, before_h, after_h, conv_w_h, conv_b_h, decay_param_h, recur_gate_h, recur_bias_h, input_gate_h, input_bias_h,
    h_h, p_f_h, p_b_h, seg_h, total_h,
    padded, conv, split, wide, wlow, pre, a_f, b_f, a_b, b_b,
    mix, before, after, conv_w, conv_b, decay_param, recur_gate, recur_bias, input_gate, input_bias,
    h, p_f, p_b, seg, total, sems,
):
    for copy in fetched(
        (
            mix_h, before_h, after_h, conv_w_h, conv_b_h, decay_param_h,
            recur_gate_h, recur_bias_h, input_gate_h, input_bias_h,
        ),
        (mix, before, after, conv_w, conv_b, decay_param, recur_gate, recur_bias, input_gate, input_bias),
        sems,
    ):
        copy.wait()
    length = mix.shape[0]
    step = length // SEGS
    stride = step + 8
    padded[0:8, :] = jnp.zeros((8, 128), F32)
    padded[6:8, :] = before[...].astype(F32)
    padded[8 : 8 + length, :] = mix[...].astype(F32)
    padded[8 + length : 16 + length, :] = jnp.zeros((8, 128), F32)
    padded[8 + length : 10 + length, :] = after[...].astype(F32)
    zero = jnp.zeros((64, 64), F32)
    columns = []
    for sense in range(2):
        for gate in (recur_gate, input_gate):
            columns.append(
                jnp.concatenate(
                    [
                        jnp.concatenate([gate[sense, 0], zero], axis=1),
                        jnp.concatenate([zero, gate[sense, 1]], axis=1),
                    ],
                    axis=0,
                )
            )
    maps = jnp.concatenate(columns, axis=1)
    high = maps.astype(BF16)
    wide[0:128, :] = high
    wide[128:256, :] = high
    wlow[...] = (maps - high.astype(F32)).astype(BF16)

    rows = 64

    def convolve(k, carry):
        at = pl.multiple_of(k * rows, rows)
        out = conv_b[...] + padded[pl.ds(at + 6, rows), :] * conv_w[0:1, :]
        for tap in range(1, 4):
            out = out + padded[pl.ds(at + 6 + tap, rows), :] * conv_w[tap : tap + 1, :]
        conv[pl.ds(at, rows), :] = out
        top = out.astype(BF16)
        split[pl.ds(at, rows), 0:128] = top
        split[pl.ds(at, rows), 128:256] = (out - top.astype(F32)).astype(BF16)
        return carry

    lax.fori_loop(0, length // rows, convolve, 0)
    pre[...] = jnp.dot(split[...], wide[...], preferred_element_type=F32) + jnp.dot(
        split[:, 0:128], wlow[...], preferred_element_type=F32
    )
    rate = -8.0 * softplus_of(-decay_param[...])

    per = step // rows

    def gates(k, carry):
        at = pl.multiple_of(k * rows, rows)
        to = pl.multiple_of((k // per) * stride + (k % per) * rows, 8)
        signal = conv[pl.ds(at, rows), :]
        for sense, (a_ref, b_ref) in enumerate(((a_f, b_f), (a_b, b_b))):
            base = sense * 256
            recur = jax.nn.sigmoid(pre[pl.ds(at, rows), base : base + 128] + recur_bias[sense : sense + 1, :])
            inner = jax.nn.sigmoid(pre[pl.ds(at, rows), base + 128 : base + 256] + input_bias[sense : sense + 1, :])
            log_decay = recur * rate[sense : sense + 1, :]
            decay = jnp.exp(log_decay)
            a_ref[pl.ds(to, rows), :] = decay
            b_ref[pl.ds(to, rows), :] = jnp.sqrt(one_minus_square(log_decay, decay)) * (inner * signal)
        return carry

    lax.fori_loop(0, length // rows, gates, 0)

    def advance(t, carry, meet):
        hf, pf, hb, pb = carry
        back = step - 1 - t
        af = a_f[pl.ds(t, SEGS, stride=stride), :]
        bf = b_f[pl.ds(t, SEGS, stride=stride), :]
        ab = a_b[pl.ds(back, SEGS, stride=stride), :]
        bb = b_b[pl.ds(back, SEGS, stride=stride), :]
        hf = af * hf + bf
        pf = pf * af
        hb = ab * hb + bb
        pb = pb * ab
        here = pl.ds(pl.multiple_of(t * SEGS, SEGS), SEGS)
        there = pl.ds(pl.multiple_of(back * SEGS, SEGS), SEGS)
        h[here, :] = hf + h[here, :] if meet else hf
        h[there, :] = hb + h[there, :] if meet else hb
        p_f[here, :] = pf
        p_b[there, :] = pb
        return hf, pf, hb, pb

    none = jnp.zeros((SEGS, 128), F32)
    ones = jnp.ones((SEGS, 128), F32)
    half = step // 2
    state = (none, ones, none, ones)
    state = lax.fori_loop(0, half, functools.partial(advance, meet=False), state, unroll=8)
    low, high = pl.ds(0, length // 2), pl.ds(length // 2, length // 2)
    sent = fetched((p_f.at[low], p_b.at[high]), (p_f_h.at[low], p_b_h.at[high]), sems, 10)
    hf, pf, hb, pb = lax.fori_loop(half, step, functools.partial(advance, meet=True), state, unroll=8)
    sent += fetched((h, p_f.at[high], p_b.at[low]), (h_h, p_f_h.at[high], p_b_h.at[low]), sems, 12)

    sums = []
    for base, last, p, order in ((0, hf, pf, range(SEGS)), (16, hb, pb, reversed(range(SEGS)))):
        enter = jnp.zeros((1, 128), F32)
        factor = jnp.ones((1, 128), F32)
        for s in order:
            seg[base + s : base + s + 1, :] = enter
            seg[base + 8 + s : base + 9 + s, :] = factor
            enter = p[s : s + 1, :] * enter + last[s : s + 1, :]
            factor = p[s : s + 1, :] * factor
        sums += [factor, enter]
    both = jnp.concatenate(sums + [jnp.zeros((4, 128), F32)], axis=0)
    total[...] = jnp.broadcast_to(both[None], total.shape)
    sent += fetched((seg, total), (seg_h, total_h), sems, 15)
    for copy in sent:
        copy.wait()


def mix_kernel(*refs):
    sources, out_h, natural, buffers, out, sems = refs[:6], refs[6], refs[7], refs[8:14], refs[14], refs[15]
    h, p_f, p_b, seg, totals, gate_in = buffers
    for copy in fetched(sources, buffers, sems):
        copy.wait()
    length = out.shape[0]
    step = length // SEGS
    stride = step + 8
    count = totals.shape[0]
    here = lax.axis_index("sp")
    enter_f = jnp.zeros((1, 128), F32)
    enter_b = jnp.zeros((1, 128), F32)
    for j in range(count):
        enter_f = jnp.where(j < here, totals[j, 0:1, :] * enter_f + totals[j, 1:2, :], enter_f)
        k = count - 1 - j
        enter_b = jnp.where(k > here, totals[k, 2:3, :] * enter_b + totals[k, 3:4, :], enter_b)
    into_f = seg[0:8, :] + seg[8:16, :] * enter_f
    into_b = seg[16:24, :] + seg[24:32, :] * enter_b

    def place(t, carry):
        at = pl.multiple_of(t * SEGS, SEGS)
        rows = pl.ds(at, SEGS)
        natural[pl.ds(t, SEGS, stride=stride), :] = (
            h[rows, :] + p_f[rows, :] * into_f + p_b[rows, :] * into_b
        )
        return carry

    lax.fori_loop(0, step, place, 0, unroll=8)
    for s in range(SEGS):
        gate = gate_in[s * step : (s + 1) * step, :].astype(F32)
        out[s * step : (s + 1) * step, :] = (
            natural[s * stride : s * stride + step, :] * jax.nn.gelu(gate)
        ).astype(BF16)
    (copy,) = fetched((out,), (out_h,), sems, 6)
    copy.wait()


def scaled(values, gain):
    return values * lax.rsqrt(jnp.mean(values * values, axis=-1, keepdims=True) + EPSILON) * gain


def proj_kernel(
    mixed_h, weights_h, residual_h, gain_h, routes_h, stream_h, outgoing_h,
    mixed, weights, residual, gain, routes, stream_out, outgoing, sems,
):
    (mixed_copy,) = fetched((mixed_h,), (mixed,), sems, 15)
    width = weights.shape[0]
    blocks = 8
    block = width // blocks
    parts = [(weights_h.at[pl.ds(k * block, block)], weights.at[pl.ds(k * block, block)]) for k in range(blocks)]
    loads = fetched(*zip(*parts), sems)
    others = fetched((residual_h, gain_h, routes_h), (residual, gain, routes), sems, blocks)
    mixed_copy.wait()
    acc = jnp.zeros(residual.shape, F32)
    per = mixed.shape[0] // blocks
    for k in range(blocks):
        lanes = jnp.concatenate([mixed[k * per + j] for j in range(per)], axis=1)
        loads[k].wait()
        acc = acc + jnp.dot(lanes, weights[k * block : (k + 1) * block, :], preferred_element_type=F32)
    for copy in others:
        copy.wait()
    proj = acc.astype(BF16).astype(F32)
    stream = (residual[...].astype(F32) + scaled(proj, gain[0:1, :])).astype(BF16)
    stream_out[...] = stream
    sent = fetched((stream_out,), (stream_h,), sems, 16)
    normed = scaled(stream.astype(F32), gain[1:2, :]).astype(BF16)
    rows = normed.shape[0]
    slots = outgoing.shape[0]
    experts = 16
    capacity = slots // experts
    first, second = routes[0:1, :], routes[1:2, :]
    ids = lax.broadcasted_iota(jnp.int32, (experts, rows), 0)
    hit0 = (ids == first).astype(F32)
    hit1 = (ids == second).astype(F32)
    r = lax.broadcasted_iota(jnp.int32, (rows, rows), 0)
    c = lax.broadcasted_iota(jnp.int32, (rows, rows), 1)
    earlier = jnp.dot((hit0 + hit1).astype(BF16), (r < c).astype(BF16), preferred_element_type=F32)
    slot0 = first * capacity + jnp.sum(hit0 * earlier, axis=0, keepdims=True).astype(jnp.int32)
    slot1 = second * capacity + jnp.sum(hit1 * earlier, axis=0, keepdims=True).astype(jnp.int32)
    places = lax.broadcasted_iota(jnp.int32, (slots, rows), 0)
    pick = jnp.where(jnp.logical_or(places == slot0, places == slot1), 1.0, 0.0).astype(BF16)
    for k in range(4):
        part = slice(k * 512, (k + 1) * 512)
        outgoing[:, part] = jnp.dot(pick, normed[:, part], preferred_element_type=F32).astype(BF16)
        sent += fetched([outgoing.at[:, part]], [outgoing_h.at[:, part]], sems, 11 + k)
    for copy in sent:
        copy.wait()


def pack_kernel(gate, up, down, out, buffer, sems):
    ff = gate.shape[0]
    refs = (gate, up, down)
    parts = [pl.ds(j * ff, ff) for j in range(3)]
    inward = fetched(refs, [buffer.at[part] for part in parts], sems)
    outward = []
    for copy, part in zip(inward, parts):
        copy.wait()
        outward += fetched([buffer.at[part]], [out.at[part]], sems, 3 + len(outward))
    for copy in outward:
        copy.wait()


def expert_kernel(*refs):
    tokens, shares = refs[0], refs[1:-7]
    out, gate_w, up_w, down_w, held, sems, extra = refs[-7:]
    (tokens_copy,) = fetched((tokens,), (held,), extra)
    ff = shares[0].shape[0] // 3
    copies = [
        fetched(
            [share.at[pl.ds(j * ff, ff)] for j in range(3)],
            [w.at[pl.ds(at * ff, ff)] for w in (gate_w, up_w, down_w)],
            sems,
            3 * at,
        )
        for at, share in enumerate(shares)
    ]
    tokens_copy.wait()
    x = held[...]
    acc = jnp.zeros(x.shape, F32)
    block = 256
    last = (((1,), (1,)), ((), ()))
    for k in range(len(shares) * ff // block):
        for piece in range(k * block // ff, (k + 1) * block // ff):
            for copy in copies[piece]:
                copy.wait()
        rows = slice(k * block, (k + 1) * block)
        gate = lax.dot_general(x, gate_w[rows, :], last, preferred_element_type=F32)
        up = lax.dot_general(x, up_w[rows, :], last, preferred_element_type=F32)
        hidden = (jax.nn.silu(gate) * up).astype(BF16)
        acc = acc + jnp.dot(hidden, down_w[rows, :], preferred_element_type=F32)
    held[...] = acc.astype(BF16)
    (copy,) = fetched((held,), (out,), extra, 1)
    copy.wait()


def combine_kernel(*refs):
    sources, out_h, buffers, out, sems = refs[:5], refs[5], refs[6:11], refs[11], refs[12]
    values, stream, gain, routes, weights = buffers
    for copy in fetched(sources, buffers, sems):
        copy.wait()
    rows = stream.shape[0]
    slots = values.shape[0]
    experts = 16
    capacity = slots // experts
    first, second = routes[:, 0:1], routes[:, 1:2]
    ids = lax.broadcasted_iota(jnp.int32, (rows, experts), 1)
    hit0 = (ids == first).astype(F32)
    hit1 = (ids == second).astype(F32)
    r = lax.broadcasted_iota(jnp.int32, (rows, rows), 0)
    c = lax.broadcasted_iota(jnp.int32, (rows, rows), 1)
    earlier = jnp.dot((c < r).astype(BF16), (hit0 + hit1).astype(BF16), preferred_element_type=F32)
    slot0 = first * capacity + jnp.sum(hit0 * earlier, axis=1, keepdims=True).astype(jnp.int32)
    slot1 = second * capacity + jnp.sum(hit1 * earlier, axis=1, keepdims=True).astype(jnp.int32)
    places = lax.broadcasted_iota(jnp.int32, (rows, slots), 1)
    table = jnp.where(places == slot0, weights[:, 0:1], 0.0) + jnp.where(
        places == slot1, weights[:, 1:2], 0.0
    )
    high = table.astype(BF16)
    rest = table - high.astype(F32)
    mid = rest.astype(BF16)
    low = (rest - mid.astype(F32)).astype(BF16)
    parts = jnp.dot(jnp.concatenate([high, mid, low], axis=0), values[...], preferred_element_type=F32)
    mixture = parts[0:rows] + (parts[rows : 2 * rows] + parts[2 * rows : 3 * rows])
    mixture = mixture.astype(BF16).astype(F32)
    out[...] = (stream[...].astype(F32) + scaled(mixture, gain[2:3, :])).astype(BF16)
    (copy,) = fetched((out,), (out_h,), sems, 5)
    copy.wait()


def shape(dims, dtype):
    return jax.ShapeDtypeStruct(dims, dtype)


def layer(
    mix_in,
    gate_in,
    conv_w,
    conv_b,
    decay_param,
    recur_gate,
    recur_bias,
    input_gate,
    input_bias,
    residual,
    out_proj,
    norm_gain,
    routes,
    route_wt,
    exp_gate,
    exp_up,
    exp_down,
):
    length, channels = mix_in.shape
    rows, width = residual.shape
    sp = lax.axis_size("sp")
    tp = lax.axis_size("tp")
    ends = sp - 1
    before = lax.ppermute(mix_in[length - 2 :], "sp", [(i, i + 1) for i in range(ends)])
    after = lax.ppermute(mix_in[:2], "sp", [(i + 1, i) for i in range(ends)])
    ff_own = exp_down.shape[1]
    piece = shape((3 * ff_own, width), BF16)
    own = pl.pallas_call(
        pack_kernel,
        out_shape=piece,
        in_specs=[in_hbm()] * 3,
        out_specs=in_hbm(),
        scratch_shapes=[pltpu.VMEM(piece.shape, BF16), pltpu.SemaphoreType.DMA((6,))],
        compiler_params=FULL,
        name="pack",
    )(jnp.swapaxes(exp_gate, 1, 2)[0], jnp.swapaxes(exp_up, 1, 2)[0], exp_down[0])

    def around(part):
        return lax.ppermute(part, "tp", [(i, (i + 2 - 4 * (i % 2)) % tp) for i in range(tp)])

    def across(part):
        return lax.ppermute(part, "tp", [(i, i ^ 1) for i in range(tp)])

    other = across(own)
    r1a = around(own)
    r1b = around(other)
    step = length // SEGS
    lines = SEGS * (step + 8)
    state = shape((length, channels), F32)
    h, p_f, p_b, seg, total = pl.pallas_call(
        scan_kernel,
        out_shape=(state, state, state, shape((32, 128), F32), shape((sp, 8, 128), F32)),
        in_specs=[anywhere()] * 10,
        out_specs=(anywhere(),) * 5,
        scratch_shapes=[
            pltpu.VMEM((length + 16, 128), F32),
            pltpu.VMEM((length, 128), F32),
            pltpu.VMEM((length, 256), BF16),
            pltpu.VMEM((256, 512), BF16),
            pltpu.VMEM((128, 512), BF16),
            pltpu.VMEM((length, 512), F32),
            pltpu.VMEM((lines, 128), F32),
            pltpu.VMEM((lines, 128), F32),
            pltpu.VMEM((lines, 128), F32),
            pltpu.VMEM((lines, 128), F32),
            pltpu.VMEM(mix_in.shape, BF16),
            pltpu.VMEM(before.shape, BF16),
            pltpu.VMEM(after.shape, BF16),
            pltpu.VMEM(conv_w.shape, F32),
            pltpu.VMEM((1, 128), F32),
            pltpu.VMEM(decay_param.shape, F32),
            pltpu.VMEM(recur_gate.shape, F32),
            pltpu.VMEM(recur_bias.shape, F32),
            pltpu.VMEM(input_gate.shape, F32),
            pltpu.VMEM(input_bias.shape, F32),
            pltpu.VMEM(state.shape, F32),
            pltpu.VMEM(state.shape, F32),
            pltpu.VMEM(state.shape, F32),
            pltpu.VMEM((32, 128), F32),
            pltpu.VMEM((sp, 8, 128), F32),
            pltpu.SemaphoreType.DMA((17,)),
        ],
        compiler_params=FULL,
        name="scan",
    )(mix_in, before, after, conv_w, conv_b[None], decay_param, recur_gate, recur_bias, input_gate, input_bias)
    total, r1a, r1b = lax.optimization_barrier((total, r1a, r1b))
    r2a, e1a = around(r1a), across(r1a)
    r2b, e1b = around(r1b), across(r1b)
    totals = lax.all_to_all(total, "sp", split_axis=0, concat_axis=0, tiled=True)
    mixed = pl.pallas_call(
        mix_kernel,
        out_shape=shape((length, channels), BF16),
        in_specs=[anywhere()] * 6,
        out_specs=anywhere(),
        scratch_shapes=[pltpu.VMEM((lines, 128), F32)]
        + [pltpu.VMEM(state.shape, F32)] * 3
        + [
            pltpu.VMEM((32, 128), F32),
            pltpu.VMEM((sp, 8, 128), F32),
            pltpu.VMEM((length, channels), BF16),
            pltpu.VMEM((length, channels), BF16),
            pltpu.SemaphoreType.DMA((8,)),
        ],
        compiler_params=FULL,
        name="mix",
    )(h, p_f, p_b, seg, totals, gate_in)
    token_rows = lax.all_to_all(
        mixed.reshape(tp, rows, channels), "tp", split_axis=0, concat_axis=0, tiled=True
    )
    r3a, e2a = around(r2a), across(r2a)
    r3b, e2b = around(r2b), across(r2b)
    first_row = lax.axis_index("tp") * rows
    own_routes = lax.dynamic_slice_in_dim(routes, first_row, rows, 0)
    own_weights = lax.dynamic_slice_in_dim(route_wt, first_row, rows, 0)
    slots = 2 * rows * routes.shape[1]
    project = pl.pallas_call(
        proj_kernel,
        out_shape=(shape((rows, width), BF16), shape((slots, width), BF16)),
        in_specs=[anywhere()] * 5,
        out_specs=(anywhere(), anywhere()),
        scratch_shapes=[
            pltpu.VMEM(token_rows.shape, BF16),
            pltpu.VMEM(out_proj.shape, BF16),
            pltpu.VMEM(residual.shape, BF16),
            pltpu.VMEM(norm_gain.shape, F32),
            pltpu.VMEM((routes.shape[1], rows), jnp.int32),
            pltpu.VMEM(residual.shape, BF16),
            pltpu.VMEM((slots, width), BF16),
            pltpu.SemaphoreType.DMA((17,)),
        ],
        compiler_params=FULL,
        name="proj",
    )
    stream, outgoing = project(token_rows, out_proj, residual, norm_gain, own_routes.T)
    r4, e3a = around(r3a), across(r3a)
    e3b, e4 = across(r3b), across(r4)
    arrived = lax.all_to_all(outgoing.reshape(sp, slots // sp, width), "sp", split_axis=0, concat_axis=0, tiled=True)
    arrived = arrived.reshape(slots, width)

    shares = (own, other, r1a, e1a, r1b, e1b, r2a, e2a, r2b, e2b, r3a, e3a, r3b, e3b, r4, e4)
    experts = pl.pallas_call(
        expert_kernel,
        out_shape=shape((slots, width), BF16),
        in_specs=[anywhere()] * (1 + len(shares)),
        out_specs=anywhere(),
        scratch_shapes=[pltpu.VMEM((len(shares) * ff_own, width), BF16)] * 3
        + [
            pltpu.VMEM((slots, width), BF16),
            pltpu.SemaphoreType.DMA((3 * len(shares),)),
            pltpu.SemaphoreType.DMA((2,)),
        ],
        compiler_params=ROOMY,
        name="experts",
    )
    done = experts(arrived, *shares)
    returned = lax.all_to_all(
        done.reshape(sp, slots // sp, width), "sp", split_axis=0, concat_axis=0, tiled=True
    )
    return pl.pallas_call(
        combine_kernel,
        out_shape=shape((rows, width), BF16),
        in_specs=[anywhere()] * 5,
        out_specs=anywhere(),
        scratch_shapes=[
            pltpu.VMEM((slots, width), BF16),
            pltpu.VMEM((rows, width), BF16),
            pltpu.VMEM(norm_gain.shape, F32),
            pltpu.VMEM(own_routes.shape, jnp.int32),
            pltpu.VMEM(own_weights.shape, F32),
            pltpu.VMEM((rows, width), BF16),
            pltpu.SemaphoreType.DMA((6,)),
        ],
        compiler_params=FULL,
        name="combine",
    )(returned.reshape(slots, width), stream, norm_gain, own_routes, own_weights)


def solution(mesh):
    return jax.shard_map(
        layer,
        mesh=mesh,
        in_specs=(
            P("sp", "tp"),
            P("sp", "tp"),
            P(None, "tp"),
            P("tp"),
            P(None, "tp"),
            P(None, "tp", None, None),
            P(None, "tp"),
            P(None, "tp", None, None),
            P(None, "tp"),
            P(("sp", "tp"), None),
            P(),
            P(),
            P("sp", None),
            P("sp", None),
            P("sp", None, "tp"),
            P("sp", None, "tp"),
            P("sp", "tp", None),
        ),
        out_specs=P(("sp", "tp"), None),
        check_vma=False,
    )
```

```python
import functools

import jax
import jax.numpy as jnp
from jax import lax
from jax.experimental import pallas as pl
from jax.experimental.pallas import tpu as pltpu
from jax.sharding import PartitionSpec as P


EPSILON = 1e-06
F32 = jnp.float32
BF16 = jnp.bfloat16
SEGS = 8
VMEM = pltpu.MemorySpace.VMEM


def whole():
    return pl.BlockSpec(memory_space=VMEM)


FULL = pltpu.CompilerParams(vmem_limit_bytes=67043328)
SMALL = pltpu.CompilerParams(vmem_limit_bytes=8 * 1024 * 1024)
PROJ = pltpu.CompilerParams(vmem_limit_bytes=67043328 - (8 * 1024 + 448) * 1024)
ROOMY = pltpu.CompilerParams(vmem_limit_bytes=48 * 1024 * 1024)


def anywhere():
    return pl.BlockSpec(memory_space=pl.ANY)


def in_hbm():
    return pl.BlockSpec(memory_space=pltpu.MemorySpace.HBM)


def fetched(sources, buffers, sems, first=0):
    copies = [pltpu.make_async_copy(src, dst, sems.at[first + k]) for k, (src, dst) in enumerate(zip(sources, buffers))]
    for copy in copies:
        copy.start()
    return copies


def one_minus_square(log_decay, decay):
    y = 2.0 * log_decay
    series = 1.0 + y * (1.0 / 7.0)
    for k in (6.0, 5.0, 4.0, 3.0, 2.0):
        series = 1.0 + y * (1.0 / k) * series
    return jnp.where(y > -0.5, -y * series, 1.0 - decay * decay)


def softplus_of(x):
    u = jnp.exp(-jnp.abs(x))
    z = u / (2.0 + u)
    z2 = z * z
    series = jnp.full_like(z, 1.0 / 17.0)
    for k in (15.0, 13.0, 11.0, 9.0, 7.0, 5.0, 3.0, 1.0):
        series = 1.0 / k + z2 * series
    return jnp.maximum(x, 0.0) + 2.0 * z * series


def scan_kernel(
    mix_h, before_h, after_h, conv_w_h, conv_b_h, decay_param_h, recur_gate_h, recur_bias_h, input_gate_h, input_bias_h,
    h_h, p_f_h, p_b_h, seg_h, total_h,
    padded, conv, split, wide, wlow, pre, a_f, b_f, a_b, b_b,
    mix, before, after, conv_w, conv_b, decay_param, recur_gate, recur_bias, input_gate, input_bias,
    h, p_f, p_b, seg, total, sems,
):
    for copy in fetched(
        (
            mix_h, before_h, after_h, conv_w_h, conv_b_h, decay_param_h,
            recur_gate_h, recur_bias_h, input_gate_h, input_bias_h,
        ),
        (mix, before, after, conv_w, conv_b, decay_param, recur_gate, recur_bias, input_gate, input_bias),
        sems,
    ):
        copy.wait()
    length = mix.shape[0]
    step = length // SEGS
    stride = step + 8
    padded[0:8, :] = jnp.zeros((8, 128), F32)
    padded[6:8, :] = before[...].astype(F32)
    padded[8 : 8 + length, :] = mix[...].astype(F32)
    padded[8 + length : 16 + length, :] = jnp.zeros((8, 128), F32)
    padded[8 + length : 10 + length, :] = after[...].astype(F32)
    zero = jnp.zeros((64, 64), F32)
    columns = []
    for sense in range(2):
        for gate in (recur_gate, input_gate):
            columns.append(
                jnp.concatenate(
                    [
                        jnp.concatenate([gate[sense, 0], zero], axis=1),
                        jnp.concatenate([zero, gate[sense, 1]], axis=1),
                    ],
                    axis=0,
                )
            )
    maps = jnp.concatenate(columns, axis=1)
    high = maps.astype(BF16)
    wide[0:128, :] = high
    wide[128:256, :] = high
    wlow[...] = (maps - high.astype(F32)).astype(BF16)

    rows = 64

    def convolve(k, carry):
        at = pl.multiple_of(k * rows, rows)
        out = conv_b[...] + padded[pl.ds(at + 6, rows), :] * conv_w[0:1, :]
        for tap in range(1, 4):
            out = out + padded[pl.ds(at + 6 + tap, rows), :] * conv_w[tap : tap + 1, :]
        conv[pl.ds(at, rows), :] = out
        top = out.astype(BF16)
        split[pl.ds(at, rows), 0:128] = top
        split[pl.ds(at, rows), 128:256] = (out - top.astype(F32)).astype(BF16)
        return carry

    lax.fori_loop(0, length // rows, convolve, 0)
    pre[...] = jnp.dot(split[...], wide[...], preferred_element_type=F32) + jnp.dot(
        split[:, 0:128], wlow[...], preferred_element_type=F32
    )
    rate = -8.0 * softplus_of(-decay_param[...])

    per = step // rows

    def gates(k, carry):
        at = pl.multiple_of(k * rows, rows)
        to = pl.multiple_of((k // per) * stride + (k % per) * rows, 8)
        signal = conv[pl.ds(at, rows), :]
        for sense, (a_ref, b_ref) in enumerate(((a_f, b_f), (a_b, b_b))):
            base = sense * 256
            recur = jax.nn.sigmoid(pre[pl.ds(at, rows), base : base + 128] + recur_bias[sense : sense + 1, :])
            inner = jax.nn.sigmoid(pre[pl.ds(at, rows), base + 128 : base + 256] + input_bias[sense : sense + 1, :])
            log_decay = recur * rate[sense : sense + 1, :]
            decay = jnp.exp(log_decay)
            a_ref[pl.ds(to, rows), :] = decay
            b_ref[pl.ds(to, rows), :] = jnp.sqrt(one_minus_square(log_decay, decay)) * (inner * signal)
        return carry

    lax.fori_loop(0, length // rows, gates, 0)

    def advance(t, carry, meet):
        hf, pf, hb, pb = carry
        back = step - 1 - t
        af = a_f[pl.ds(t, SEGS, stride=stride), :]
        bf = b_f[pl.ds(t, SEGS, stride=stride), :]
        ab = a_b[pl.ds(back, SEGS, stride=stride), :]
        bb = b_b[pl.ds(back, SEGS, stride=stride), :]
        hf = af * hf + bf
        pf = pf * af
        hb = ab * hb + bb
        pb = pb * ab
        here = pl.ds(pl.multiple_of(t * SEGS, SEGS), SEGS)
        there = pl.ds(pl.multiple_of(back * SEGS, SEGS), SEGS)
        h[here, :] = hf + h[here, :] if meet else hf
        h[there, :] = hb + h[there, :] if meet else hb
        p_f[here, :] = pf
        p_b[there, :] = pb
        return hf, pf, hb, pb

    none = jnp.zeros((SEGS, 128), F32)
    ones = jnp.ones((SEGS, 128), F32)
    half = step // 2
    state = (none, ones, none, ones)
    state = lax.fori_loop(0, half, functools.partial(advance, meet=False), state, unroll=8)
    low, high = pl.ds(0, length // 2), pl.ds(length // 2, length // 2)
    sent = fetched((p_f.at[low], p_b.at[high]), (p_f_h.at[low], p_b_h.at[high]), sems, 10)
    hf, pf, hb, pb = lax.fori_loop(half, step, functools.partial(advance, meet=True), state, unroll=8)
    sent += fetched((h, p_f.at[high], p_b.at[low]), (h_h, p_f_h.at[high], p_b_h.at[low]), sems, 12)

    sums = []
    for base, last, p, order in ((0, hf, pf, range(SEGS)), (16, hb, pb, reversed(range(SEGS)))):
        enter = jnp.zeros((1, 128), F32)
        factor = jnp.ones((1, 128), F32)
        for s in order:
            seg[base + s : base + s + 1, :] = enter
            seg[base + 8 + s : base + 9 + s, :] = factor
            enter = p[s : s + 1, :] * enter + last[s : s + 1, :]
            factor = p[s : s + 1, :] * factor
        sums += [factor, enter]
    both = jnp.concatenate(sums + [jnp.zeros((4, 128), F32)], axis=0)
    total[...] = jnp.broadcast_to(both[None], total.shape)
    sent += fetched((seg, total), (seg_h, total_h), sems, 15)
    for copy in sent:
        copy.wait()


def mix_kernel(*refs):
    sources, out_h, natural, buffers, out, sems = refs[:6], refs[6], refs[7], refs[8:14], refs[14], refs[15]
    h, p_f, p_b, seg, totals, gate_in = buffers
    for copy in fetched(sources, buffers, sems):
        copy.wait()
    length = out.shape[0]
    step = length // SEGS
    stride = step + 8
    count = totals.shape[0]
    here = lax.axis_index("sp")
    enter_f = jnp.zeros((1, 128), F32)
    enter_b = jnp.zeros((1, 128), F32)
    for j in range(count):
        enter_f = jnp.where(j < here, totals[j, 0:1, :] * enter_f + totals[j, 1:2, :], enter_f)
        k = count - 1 - j
        enter_b = jnp.where(k > here, totals[k, 2:3, :] * enter_b + totals[k, 3:4, :], enter_b)
    into_f = seg[0:8, :] + seg[8:16, :] * enter_f
    into_b = seg[16:24, :] + seg[24:32, :] * enter_b

    def place(t, carry):
        at = pl.multiple_of(t * SEGS, SEGS)
        rows = pl.ds(at, SEGS)
        natural[pl.ds(t, SEGS, stride=stride), :] = (
            h[rows, :] + p_f[rows, :] * into_f + p_b[rows, :] * into_b
        )
        return carry

    lax.fori_loop(0, step, place, 0, unroll=8)
    for s in range(SEGS):
        gate = gate_in[s * step : (s + 1) * step, :].astype(F32)
        out[s * step : (s + 1) * step, :] = (
            natural[s * stride : s * stride + step, :] * jax.nn.gelu(gate)
        ).astype(BF16)
    (copy,) = fetched((out,), (out_h,), sems, 6)
    copy.wait()


def scaled(values, gain):
    return values * lax.rsqrt(jnp.mean(values * values, axis=-1, keepdims=True) + EPSILON) * gain


def preload_kernel(source, target, sem):
    (copy,) = fetched((source,), (target,), sem)
    copy.wait()


def slots_of(first, second, axis, capacity, experts):
    rows = first.size
    ids = lax.broadcasted_iota(jnp.int32, (experts, rows) if axis == 0 else (rows, experts), axis)
    hit0 = (ids == first).astype(F32)
    hit1 = (ids == second).astype(F32)
    r = lax.broadcasted_iota(jnp.int32, (rows, rows), 0)
    c = lax.broadcasted_iota(jnp.int32, (rows, rows), 1)
    both = (hit0 + hit1).astype(BF16)
    if axis == 0:
        earlier = jnp.dot(both, (r < c).astype(BF16), preferred_element_type=F32)
    else:
        earlier = jnp.dot((c < r).astype(BF16), both, preferred_element_type=F32)
    return tuple(
        ids0 * capacity + jnp.sum(hit * earlier, axis=axis, keepdims=True).astype(jnp.int32)
        for ids0, hit in ((first, hit0), (second, hit1))
    )


def proj_kernel(
    weights, mixed, residual_h, gain_h, routes_h, columns_h, route_wt_h, stream_h, outgoing_h, table_h,
    residual, gain, routes, columns, route_wt, stream_out, outgoing, table_out, sems,
):
    small = fetched((routes_h, columns_h, route_wt_h), (routes, columns, route_wt), sems)
    small += fetched((residual_h, gain_h), (residual, gain), sems, 9)
    width = weights.shape[0]
    rows = residual.shape[0]
    slots = outgoing.shape[0]
    experts = 16
    capacity = slots // experts
    lanes = jnp.concatenate([mixed[j] for j in range(mixed.shape[0])], axis=1)
    acc = jnp.dot(lanes, weights[...], preferred_element_type=F32)
    for copy in small:
        copy.wait()
    slot0, slot1 = slots_of(columns[:, 0:1], columns[:, 1:2], 1, capacity, experts)
    places = lax.broadcasted_iota(jnp.int32, (rows, slots), 1)
    table = jnp.where(places == slot0, route_wt[:, 0:1], 0.0) + jnp.where(
        places == slot1, route_wt[:, 1:2], 0.0
    )
    high = table.astype(BF16)
    rest = table - high.astype(F32)
    mid = rest.astype(BF16)
    table_out[0:rows, :] = high
    table_out[rows : 2 * rows, :] = mid
    table_out[2 * rows : 3 * rows, :] = (rest - mid.astype(F32)).astype(BF16)
    sent = fetched((table_out,), (table_h,), sems, 3)
    slot0, slot1 = slots_of(routes[0:1, :], routes[1:2, :], 0, capacity, experts)
    places = lax.broadcasted_iota(jnp.int32, (slots, rows), 0)
    pick = jnp.where(jnp.logical_or(places == slot0, places == slot1), 1.0, 0.0).astype(BF16)
    proj = acc.astype(BF16).astype(F32)
    stream = (residual[...].astype(F32) + scaled(proj, gain[0:1, :])).astype(BF16)
    stream_out[...] = stream
    sent += fetched((stream_out,), (stream_h,), sems, 4)
    normed = scaled(stream.astype(F32), gain[1:2, :]).astype(BF16)
    for k in range(4):
        part = slice(k * width // 4, (k + 1) * width // 4)
        outgoing[:, part] = jnp.dot(pick, normed[:, part], preferred_element_type=F32).astype(BF16)
        sent += fetched([outgoing.at[:, part]], [outgoing_h.at[:, part]], sems, 5 + k)
    for copy in sent:
        copy.wait()


def pack_kernel(gate, up, down, out, buffer, sems):
    ff = gate.shape[0]
    refs = (gate, up, down)
    parts = [pl.ds(j * ff, ff) for j in range(3)]
    inward = fetched(refs, [buffer.at[part] for part in parts], sems)
    outward = []
    for copy, part in zip(inward, parts):
        copy.wait()
        outward += fetched([buffer.at[part]], [out.at[part]], sems, 3 + len(outward))
    for copy in outward:
        copy.wait()


def expert_kernel(*refs):
    tokens, shares = refs[0], refs[1:-7]
    out, gate_w, up_w, down_w, held, sems, extra = refs[-7:]
    (tokens_copy,) = fetched((tokens,), (held,), extra)
    ff = shares[0].shape[0] // 3
    copies = [
        fetched(
            [share.at[pl.ds(j * ff, ff)] for j in range(3)],
            [w.at[pl.ds(at * ff, ff)] for w in (gate_w, up_w, down_w)],
            sems,
            3 * at,
        )
        for at, share in enumerate(shares)
    ]
    tokens_copy.wait()
    x = held[...]
    acc = jnp.zeros(x.shape, F32)
    block = 256
    last = (((1,), (1,)), ((), ()))
    for k in range(len(shares) * ff // block):
        for piece in range(k * block // ff, (k + 1) * block // ff):
            for copy in copies[piece]:
                copy.wait()
        rows = slice(k * block, (k + 1) * block)
        gate = lax.dot_general(x, gate_w[rows, :], last, preferred_element_type=F32)
        up = lax.dot_general(x, up_w[rows, :], last, preferred_element_type=F32)
        hidden = (jax.nn.silu(gate) * up).astype(BF16)
        acc = acc + jnp.dot(hidden, down_w[rows, :], preferred_element_type=F32)
    held[...] = acc.astype(BF16)
    (copy,) = fetched((held,), (out,), extra, 1)
    copy.wait()


def combine_kernel(*refs):
    sources, out_h, buffers, out, sems = refs[:4], refs[4], refs[5:9], refs[9], refs[10]
    values, stream, gain, table = buffers
    for copy in fetched(sources, buffers, sems):
        copy.wait()
    rows = stream.shape[0]
    parts = jnp.dot(table[...], values[...], preferred_element_type=F32)
    mixture = parts[0:rows] + (parts[rows : 2 * rows] + parts[2 * rows : 3 * rows])
    mixture = mixture.astype(BF16).astype(F32)
    out[...] = (stream[...].astype(F32) + scaled(mixture, gain[2:3, :])).astype(BF16)
    (copy,) = fetched((out,), (out_h,), sems, 4)
    copy.wait()


def shape(dims, dtype):
    return jax.ShapeDtypeStruct(dims, dtype)


def layer(
    mix_in,
    gate_in,
    conv_w,
    conv_b,
    decay_param,
    recur_gate,
    recur_bias,
    input_gate,
    input_bias,
    residual,
    out_proj,
    norm_gain,
    routes,
    route_wt,
    exp_gate,
    exp_up,
    exp_down,
):
    length, channels = mix_in.shape
    rows, width = residual.shape
    sp = lax.axis_size("sp")
    tp = lax.axis_size("tp")
    ends = sp - 1
    before = lax.ppermute(mix_in[length - 2 :], "sp", [(i, i + 1) for i in range(ends)])
    after = lax.ppermute(mix_in[:2], "sp", [(i + 1, i) for i in range(ends)])
    ff_own = exp_down.shape[1]
    piece = shape((3 * ff_own, width), BF16)
    own = pl.pallas_call(
        pack_kernel,
        out_shape=piece,
        in_specs=[in_hbm()] * 3,
        out_specs=in_hbm(),
        scratch_shapes=[pltpu.VMEM(piece.shape, BF16), pltpu.SemaphoreType.DMA((6,))],
        compiler_params=FULL,
        name="pack",
    )(jnp.swapaxes(exp_gate, 1, 2)[0], jnp.swapaxes(exp_up, 1, 2)[0], exp_down[0])

    def around(part):
        return lax.ppermute(part, "tp", [(i, (i + 2 - 4 * (i % 2)) % tp) for i in range(tp)])

    def across(part):
        return lax.ppermute(part, "tp", [(i, i ^ 1) for i in range(tp)])

    other = across(own)
    r1a = around(own)
    r1b = around(other)
    step = length // SEGS
    lines = SEGS * (step + 8)
    state = shape((length, channels), F32)
    h, p_f, p_b, seg, total = pl.pallas_call(
        scan_kernel,
        out_shape=(state, state, state, shape((32, 128), F32), shape((sp, 8, 128), F32)),
        in_specs=[anywhere()] * 10,
        out_specs=(anywhere(),) * 5,
        scratch_shapes=[
            pltpu.VMEM((length + 16, 128), F32),
            pltpu.VMEM((length, 128), F32),
            pltpu.VMEM((length, 256), BF16),
            pltpu.VMEM((256, 512), BF16),
            pltpu.VMEM((128, 512), BF16),
            pltpu.VMEM((length, 512), F32),
            pltpu.VMEM((lines, 128), F32),
            pltpu.VMEM((lines, 128), F32),
            pltpu.VMEM((lines, 128), F32),
            pltpu.VMEM((lines, 128), F32),
            pltpu.VMEM(mix_in.shape, BF16),
            pltpu.VMEM(before.shape, BF16),
            pltpu.VMEM(after.shape, BF16),
            pltpu.VMEM(conv_w.shape, F32),
            pltpu.VMEM((1, 128), F32),
            pltpu.VMEM(decay_param.shape, F32),
            pltpu.VMEM(recur_gate.shape, F32),
            pltpu.VMEM(recur_bias.shape, F32),
            pltpu.VMEM(input_gate.shape, F32),
            pltpu.VMEM(input_bias.shape, F32),
            pltpu.VMEM(state.shape, F32),
            pltpu.VMEM(state.shape, F32),
            pltpu.VMEM(state.shape, F32),
            pltpu.VMEM((32, 128), F32),
            pltpu.VMEM((sp, 8, 128), F32),
            pltpu.SemaphoreType.DMA((17,)),
        ],
        compiler_params=FULL,
        name="scan",
    )(mix_in, before, after, conv_w, conv_b[None], decay_param, recur_gate, recur_bias, input_gate, input_bias)
    total, r1a, r1b = lax.optimization_barrier((total, r1a, r1b))
    r2a, e1a = around(r1a), across(r1a)
    r2b, e1b = around(r1b), across(r1b)
    totals = lax.all_to_all(total, "sp", split_axis=0, concat_axis=0, tiled=True)
    mixed = pl.pallas_call(
        mix_kernel,
        out_shape=shape((length, channels), BF16),
        in_specs=[anywhere()] * 6,
        out_specs=anywhere(),
        scratch_shapes=[pltpu.VMEM((lines, 128), F32)]
        + [pltpu.VMEM(state.shape, F32)] * 3
        + [
            pltpu.VMEM((32, 128), F32),
            pltpu.VMEM((sp, 8, 128), F32),
            pltpu.VMEM((length, channels), BF16),
            pltpu.VMEM((length, channels), BF16),
            pltpu.SemaphoreType.DMA((8,)),
        ],
        compiler_params=FULL,
        name="mix",
    )(h, p_f, p_b, seg, totals, gate_in)
    token_rows = lax.all_to_all(
        mixed.reshape(tp, rows, channels), "tp", split_axis=0, concat_axis=0, tiled=True
    )
    r3a, e2a = around(r2a), across(r2a)
    r3b, e2b = around(r2b), across(r2b)
    first_row = lax.axis_index("tp") * rows
    own_routes = lax.dynamic_slice_in_dim(routes, first_row, rows, 0)
    own_weights = lax.dynamic_slice_in_dim(route_wt, first_row, rows, 0)
    slots = 2 * rows * routes.shape[1]
    preload = pl.pallas_call(
        preload_kernel,
        out_shape=shape(out_proj.shape, BF16),
        in_specs=[anywhere()],
        out_specs=whole(),
        scratch_shapes=[pltpu.SemaphoreType.DMA((1,))],
        compiler_params=PROJ,
        name="preload",
    )
    weights_v = preload(out_proj)
    project = pl.pallas_call(
        proj_kernel,
        out_shape=(
            shape((rows, width), BF16),
            shape((slots, width), BF16),
            shape((3 * rows, slots), BF16),
        ),
        in_specs=[whole()] * 2 + [anywhere()] * 5,
        out_specs=(anywhere(),) * 3,
        scratch_shapes=[
            pltpu.VMEM(residual.shape, BF16),
            pltpu.VMEM(norm_gain.shape, F32),
            pltpu.VMEM((routes.shape[1], rows), jnp.int32),
            pltpu.VMEM(own_routes.shape, jnp.int32),
            pltpu.VMEM(own_weights.shape, F32),
            pltpu.VMEM(residual.shape, BF16),
            pltpu.VMEM((slots, width), BF16),
            pltpu.VMEM((3 * rows, slots), BF16),
            pltpu.SemaphoreType.DMA((11,)),
        ],
        compiler_params=PROJ,
        name="proj",
    )
    stream, outgoing, table = project(
        weights_v, token_rows, residual, norm_gain, own_routes.T, own_routes, own_weights
    )
    r4, e3a = around(r3a), across(r3a)
    e3b, e4 = across(r3b), across(r4)
    arrived = lax.all_to_all(
        outgoing.reshape(sp, slots // sp, width), "sp", split_axis=0, concat_axis=0, tiled=True
    )
    arrived = arrived.reshape(slots, width)

    shares = (own, other, r1a, e1a, r1b, e1b, r2a, e2a, r2b, e2b, r3a, e3a, r3b, e3b, r4, e4)
    experts = pl.pallas_call(
        expert_kernel,
        out_shape=shape((slots, width), BF16),
        in_specs=[anywhere()] * (1 + len(shares)),
        out_specs=anywhere(),
        scratch_shapes=[pltpu.VMEM((len(shares) * ff_own, width), BF16)] * 3
        + [
            pltpu.VMEM((slots, width), BF16),
            pltpu.SemaphoreType.DMA((3 * len(shares),)),
            pltpu.SemaphoreType.DMA((2,)),
        ],
        compiler_params=ROOMY,
        name="experts",
    )
    done = experts(arrived, *shares)
    returned = lax.all_to_all(
        done.reshape(sp, slots // sp, width), "sp", split_axis=0, concat_axis=0, tiled=True
    )
    return pl.pallas_call(
        combine_kernel,
        out_shape=shape((rows, width), BF16),
        in_specs=[anywhere()] * 4,
        out_specs=anywhere(),
        scratch_shapes=[
            pltpu.VMEM((slots, width), BF16),
            pltpu.VMEM((rows, width), BF16),
            pltpu.VMEM(norm_gain.shape, F32),
            pltpu.VMEM((3 * rows, slots), BF16),
            pltpu.VMEM((rows, width), BF16),
            pltpu.SemaphoreType.DMA((5,)),
        ],
        compiler_params=FULL,
        name="combine",
    )(returned.reshape(slots, width), stream, norm_gain, table)


def solution(mesh):
    return jax.shard_map(
        layer,
        mesh=mesh,
        in_specs=(
            P("sp", "tp"),
            P("sp", "tp"),
            P(None, "tp"),
            P("tp"),
            P(None, "tp"),
            P(None, "tp", None, None),
            P(None, "tp"),
            P(None, "tp", None, None),
            P(None, "tp"),
            P(("sp", "tp"), None),
            P(),
            P(),
            P("sp", None),
            P("sp", None),
            P("sp", None, "tp"),
            P("sp", None, "tp"),
            P("sp", "tp", None),
        ),
        out_specs=P(("sp", "tp"), None),
        check_vma=False,
    )
```

```python
import functools

import jax
import jax.numpy as jnp
from jax import lax
from jax.experimental import pallas as pl
from jax.experimental.pallas import tpu as pltpu
from jax.sharding import PartitionSpec as P


EPSILON = 1e-06
F32 = jnp.float32
BF16 = jnp.bfloat16
SEGS = 8


FULL = pltpu.CompilerParams(vmem_limit_bytes=67043328)
ROOMY = pltpu.CompilerParams(vmem_limit_bytes=30 * 1024 * 1024)


def anywhere():
    return pl.BlockSpec(memory_space=pl.ANY)


def in_hbm():
    return pl.BlockSpec(memory_space=pltpu.MemorySpace.HBM)


def fetched(sources, buffers, sems, first=0):
    copies = [pltpu.make_async_copy(src, dst, sems.at[first + k]) for k, (src, dst) in enumerate(zip(sources, buffers))]
    for copy in copies:
        copy.start()
    return copies


def one_minus_square(log_decay, decay):
    y = 2.0 * log_decay
    series = 1.0 + y * (1.0 / 7.0)
    for k in (6.0, 5.0, 4.0, 3.0, 2.0):
        series = 1.0 + y * (1.0 / k) * series
    return jnp.where(y > -0.5, -y * series, 1.0 - decay * decay)


def softplus_of(x):
    u = jnp.exp(-jnp.abs(x))
    z = u / (2.0 + u)
    z2 = z * z
    series = jnp.full_like(z, 1.0 / 17.0)
    for k in (15.0, 13.0, 11.0, 9.0, 7.0, 5.0, 3.0, 1.0):
        series = 1.0 / k + z2 * series
    return jnp.maximum(x, 0.0) + 2.0 * z * series


def scan_kernel(
    mix_h, before_h, after_h, conv_w_h, conv_b_h, decay_param_h, recur_gate_h, recur_bias_h, input_gate_h, input_bias_h,
    h_h, p_f_h, p_b_h, seg_h, total_h,
    padded, conv, split, wide, wlow, pre, a_f, b_f, a_b, b_b,
    mix, before, after, conv_w, conv_b, decay_param, recur_gate, recur_bias, input_gate, input_bias,
    h, p_f, p_b, seg, total, sems,
):
    for copy in fetched(
        (
            mix_h, before_h, after_h, conv_w_h, conv_b_h, decay_param_h,
            recur_gate_h, recur_bias_h, input_gate_h, input_bias_h,
        ),
        (mix, before, after, conv_w, conv_b, decay_param, recur_gate, recur_bias, input_gate, input_bias),
        sems,
    ):
        copy.wait()
    length = mix.shape[0]
    step = length // SEGS
    stride = step + 8
    padded[0:8, :] = jnp.zeros((8, 128), F32)
    padded[6:8, :] = before[...].astype(F32)
    padded[8 : 8 + length, :] = mix[...].astype(F32)
    padded[8 + length : 16 + length, :] = jnp.zeros((8, 128), F32)
    padded[8 + length : 10 + length, :] = after[...].astype(F32)
    zero = jnp.zeros((64, 64), F32)
    columns = []
    for sense in range(2):
        for gate in (recur_gate, input_gate):
            columns.append(
                jnp.concatenate(
                    [
                        jnp.concatenate([gate[sense, 0], zero], axis=1),
                        jnp.concatenate([zero, gate[sense, 1]], axis=1),
                    ],
                    axis=0,
                )
            )
    maps = jnp.concatenate(columns, axis=1)
    high = maps.astype(BF16)
    wide[0:128, :] = high
    wide[128:256, :] = high
    wlow[...] = (maps - high.astype(F32)).astype(BF16)

    rows = 64

    def convolve(k, carry):
        at = pl.multiple_of(k * rows, rows)
        out = conv_b[...] + padded[pl.ds(at + 6, rows), :] * conv_w[0:1, :]
        for tap in range(1, 4):
            out = out + padded[pl.ds(at + 6 + tap, rows), :] * conv_w[tap : tap + 1, :]
        conv[pl.ds(at, rows), :] = out
        top = out.astype(BF16)
        split[pl.ds(at, rows), 0:128] = top
        split[pl.ds(at, rows), 128:256] = (out - top.astype(F32)).astype(BF16)
        return carry

    lax.fori_loop(0, length // rows, convolve, 0)
    pre[...] = jnp.dot(split[...], wide[...], preferred_element_type=F32) + jnp.dot(
        split[:, 0:128], wlow[...], preferred_element_type=F32
    )
    rate = -8.0 * softplus_of(-decay_param[...])

    per = step // rows

    def gates(k, carry):
        at = pl.multiple_of(k * rows, rows)
        to = pl.multiple_of((k // per) * stride + (k % per) * rows, 8)
        signal = conv[pl.ds(at, rows), :]
        for sense, (a_ref, b_ref) in enumerate(((a_f, b_f), (a_b, b_b))):
            base = sense * 256
            recur = jax.nn.sigmoid(pre[pl.ds(at, rows), base : base + 128] + recur_bias[sense : sense + 1, :])
            inner = jax.nn.sigmoid(pre[pl.ds(at, rows), base + 128 : base + 256] + input_bias[sense : sense + 1, :])
            log_decay = recur * rate[sense : sense + 1, :]
            decay = jnp.exp(log_decay)
            a_ref[pl.ds(to, rows), :] = decay
            b_ref[pl.ds(to, rows), :] = jnp.sqrt(one_minus_square(log_decay, decay)) * (inner * signal)
        return carry

    lax.fori_loop(0, length // rows, gates, 0)

    def advance(t, carry, meet):
        hf, pf, hb, pb = carry
        back = step - 1 - t
        af = a_f[pl.ds(t, SEGS, stride=stride), :]
        bf = b_f[pl.ds(t, SEGS, stride=stride), :]
        ab = a_b[pl.ds(back, SEGS, stride=stride), :]
        bb = b_b[pl.ds(back, SEGS, stride=stride), :]
        hf = af * hf + bf
        pf = pf * af
        hb = ab * hb + bb
        pb = pb * ab
        here = pl.ds(pl.multiple_of(t * SEGS, SEGS), SEGS)
        there = pl.ds(pl.multiple_of(back * SEGS, SEGS), SEGS)
        h[here, :] = hf + h[here, :] if meet else hf
        h[there, :] = hb + h[there, :] if meet else hb
        p_f[here, :] = pf
        p_b[there, :] = pb
        return hf, pf, hb, pb

    none = jnp.zeros((SEGS, 128), F32)
    ones = jnp.ones((SEGS, 128), F32)
    half = step // 2
    state = (none, ones, none, ones)
    state = lax.fori_loop(0, half, functools.partial(advance, meet=False), state, unroll=8)
    low, high = pl.ds(0, length // 2), pl.ds(length // 2, length // 2)
    sent = fetched((p_f.at[low], p_b.at[high]), (p_f_h.at[low], p_b_h.at[high]), sems, 10)
    hf, pf, hb, pb = lax.fori_loop(half, step, functools.partial(advance, meet=True), state, unroll=8)
    sent += fetched((h, p_f.at[high], p_b.at[low]), (h_h, p_f_h.at[high], p_b_h.at[low]), sems, 12)

    sums = []
    for base, last, p, order in ((0, hf, pf, range(SEGS)), (16, hb, pb, reversed(range(SEGS)))):
        enter = jnp.zeros((1, 128), F32)
        factor = jnp.ones((1, 128), F32)
        for s in order:
            seg[base + s : base + s + 1, :] = enter
            seg[base + 8 + s : base + 9 + s, :] = factor
            enter = p[s : s + 1, :] * enter + last[s : s + 1, :]
            factor = p[s : s + 1, :] * factor
        sums += [factor, enter]
    both = jnp.concatenate(sums + [jnp.zeros((4, 128), F32)], axis=0)
    total[...] = jnp.broadcast_to(both[None], total.shape)
    sent += fetched((seg, total), (seg_h, total_h), sems, 15)
    for copy in sent:
        copy.wait()


def mix_kernel(*refs):
    sources, out_h, natural, buffers, out, sems = refs[:6], refs[6], refs[7], refs[8:14], refs[14], refs[15]
    h, p_f, p_b, seg, totals, gate_in = buffers
    for copy in fetched(sources, buffers, sems):
        copy.wait()
    length = out.shape[0]
    step = length // SEGS
    stride = step + 8
    count = totals.shape[0]
    here = lax.axis_index("sp")
    enter_f = jnp.zeros((1, 128), F32)
    enter_b = jnp.zeros((1, 128), F32)
    for j in range(count):
        enter_f = jnp.where(j < here, totals[j, 0:1, :] * enter_f + totals[j, 1:2, :], enter_f)
        k = count - 1 - j
        enter_b = jnp.where(k > here, totals[k, 2:3, :] * enter_b + totals[k, 3:4, :], enter_b)
    into_f = seg[0:8, :] + seg[8:16, :] * enter_f
    into_b = seg[16:24, :] + seg[24:32, :] * enter_b

    def place(t, carry):
        at = pl.multiple_of(t * SEGS, SEGS)
        rows = pl.ds(at, SEGS)
        natural[pl.ds(t, SEGS, stride=stride), :] = (
            h[rows, :] + p_f[rows, :] * into_f + p_b[rows, :] * into_b
        )
        return carry

    lax.fori_loop(0, step, place, 0, unroll=8)
    for s in range(SEGS):
        gate = gate_in[s * step : (s + 1) * step, :].astype(F32)
        out[s * step : (s + 1) * step, :] = (
            natural[s * stride : s * stride + step, :] * jax.nn.gelu(gate)
        ).astype(BF16)
    (copy,) = fetched((out,), (out_h,), sems, 6)
    copy.wait()


def scaled(values, gain):
    return values * lax.rsqrt(jnp.mean(values * values, axis=-1, keepdims=True) + EPSILON) * gain


def slots_of(first, second, axis, capacity, experts):
    rows = first.size
    ids = lax.broadcasted_iota(jnp.int32, (experts, rows) if axis == 0 else (rows, experts), axis)
    hit0 = (ids == first).astype(F32)
    hit1 = (ids == second).astype(F32)
    r = lax.broadcasted_iota(jnp.int32, (rows, rows), 0)
    c = lax.broadcasted_iota(jnp.int32, (rows, rows), 1)
    both = (hit0 + hit1).astype(BF16)
    if axis == 0:
        earlier = jnp.dot(both, (r < c).astype(BF16), preferred_element_type=F32)
    else:
        earlier = jnp.dot((c < r).astype(BF16), both, preferred_element_type=F32)
    return tuple(
        ids0 * capacity + jnp.sum(hit * earlier, axis=axis, keepdims=True).astype(jnp.int32)
        for ids0, hit in ((first, hit0), (second, hit1))
    )


def proj_kernel(
    mixed_h, weights_h, residual_h, gain_h, routes_h, columns_h, route_wt_h, stream_h, outgoing_h, table_h,
    mixed, weights, residual, gain, routes, columns, route_wt, stream_out, outgoing, table_out, sems,
):
    small = fetched((routes_h, columns_h, route_wt_h), (routes, columns, route_wt), sems)
    (mixed_copy,) = fetched((mixed_h,), (mixed,), sems, 9)
    width = weights.shape[0]
    blocks = 8
    block = width // blocks
    parts = [(weights_h.at[pl.ds(k * block, block)], weights.at[pl.ds(k * block, block)]) for k in range(blocks)]
    loads = fetched(*zip(*parts), sems, 12)
    others = fetched((residual_h, gain_h), (residual, gain), sems, 10)
    rows = residual.shape[0]
    slots = outgoing.shape[0]
    experts = 16
    capacity = slots // experts
    for copy in small:
        copy.wait()
    slot0, slot1 = slots_of(columns[:, 0:1], columns[:, 1:2], 1, capacity, experts)
    places = lax.broadcasted_iota(jnp.int32, (rows, slots), 1)
    table = jnp.where(places == slot0, route_wt[:, 0:1], 0.0) + jnp.where(
        places == slot1, route_wt[:, 1:2], 0.0
    )
    high = table.astype(BF16)
    rest = table - high.astype(F32)
    mid = rest.astype(BF16)
    table_out[0:rows, :] = high
    table_out[rows : 2 * rows, :] = mid
    table_out[2 * rows : 3 * rows, :] = (rest - mid.astype(F32)).astype(BF16)
    sent = fetched((table_out,), (table_h,), sems, 3)
    slot0, slot1 = slots_of(routes[0:1, :], routes[1:2, :], 0, capacity, experts)
    places = lax.broadcasted_iota(jnp.int32, (slots, rows), 0)
    pick = jnp.where(jnp.logical_or(places == slot0, places == slot1), 1.0, 0.0).astype(BF16)
    mixed_copy.wait()
    acc = jnp.zeros(residual.shape, F32)
    per = mixed.shape[0] // blocks
    for k in range(blocks):
        lanes = jnp.concatenate([mixed[k * per + j] for j in range(per)], axis=1)
        loads[k].wait()
        acc = acc + jnp.dot(lanes, weights[k * block : (k + 1) * block, :], preferred_element_type=F32)
    for copy in others:
        copy.wait()
    proj = acc.astype(BF16).astype(F32)
    stream = (residual[...].astype(F32) + scaled(proj, gain[0:1, :])).astype(BF16)
    stream_out[...] = stream
    sent += fetched((stream_out,), (stream_h,), sems, 4)
    normed = scaled(stream.astype(F32), gain[1:2, :]).astype(BF16)
    for k in range(4):
        part = slice(k * width // 4, (k + 1) * width // 4)
        outgoing[:, part] = jnp.dot(pick, normed[:, part], preferred_element_type=F32).astype(BF16)
        sent += fetched([outgoing.at[:, part]], [outgoing_h.at[:, part]], sems, 5 + k)
    for copy in sent:
        copy.wait()


def pack_kernel(gate, up, down, out, buffer, sems):
    ff = gate.shape[0]
    refs = (gate, up, down)
    parts = [pl.ds(j * ff, ff) for j in range(3)]
    inward = fetched(refs, [buffer.at[part] for part in parts], sems)
    outward = []
    for copy, part in zip(inward, parts):
        copy.wait()
        outward += fetched([buffer.at[part]], [out.at[part]], sems, 3 + len(outward))
    for copy in outward:
        copy.wait()


def expert_kernel(*refs):
    tokens, shares = refs[0], refs[1:-7]
    out, gate_w, up_w, down_w, held, sems, extra = refs[-7:]
    (tokens_copy,) = fetched((tokens,), (held,), extra)
    ff = shares[0].shape[0] // 3
    copies = [
        fetched(
            [share.at[pl.ds(j * ff, ff)] for j in range(3)],
            [w.at[pl.ds(at * ff, ff)] for w in (gate_w, up_w, down_w)],
            sems,
            3 * at,
        )
        for at, share in enumerate(shares)
    ]
    tokens_copy.wait()
    x = held[...]
    acc = jnp.zeros(x.shape, F32)
    block = 256
    last = (((1,), (1,)), ((), ()))
    for k in range(len(shares) * ff // block):
        for piece in range(k * block // ff, (k + 1) * block // ff):
            for copy in copies[piece]:
                copy.wait()
        rows = slice(k * block, (k + 1) * block)
        gate = lax.dot_general(x, gate_w[rows, :], last, preferred_element_type=F32)
        up = lax.dot_general(x, up_w[rows, :], last, preferred_element_type=F32)
        hidden = (jax.nn.silu(gate) * up).astype(BF16)
        acc = acc + jnp.dot(hidden, down_w[rows, :], preferred_element_type=F32)
    held[...] = acc.astype(BF16)
    (copy,) = fetched((held,), (out,), extra, 1)
    copy.wait()


def combine_kernel(*refs):
    sources, out_h, buffers, out, sems = refs[:4], refs[4], refs[5:9], refs[9], refs[10]
    values, stream, gain, table = buffers
    for copy in fetched(sources, buffers, sems):
        copy.wait()
    rows = stream.shape[0]
    parts = jnp.dot(table[...], values[...], preferred_element_type=F32)
    mixture = parts[0:rows] + (parts[rows : 2 * rows] + parts[2 * rows : 3 * rows])
    mixture = mixture.astype(BF16).astype(F32)
    out[...] = (stream[...].astype(F32) + scaled(mixture, gain[2:3, :])).astype(BF16)
    (copy,) = fetched((out,), (out_h,), sems, 4)
    copy.wait()


def shape(dims, dtype):
    return jax.ShapeDtypeStruct(dims, dtype)


def layer(
    mix_in,
    gate_in,
    conv_w,
    conv_b,
    decay_param,
    recur_gate,
    recur_bias,
    input_gate,
    input_bias,
    residual,
    out_proj,
    norm_gain,
    routes,
    route_wt,
    exp_gate,
    exp_up,
    exp_down,
):
    length, channels = mix_in.shape
    rows, width = residual.shape
    sp = lax.axis_size("sp")
    tp = lax.axis_size("tp")
    ends = sp - 1
    before = lax.ppermute(mix_in[length - 2 :], "sp", [(i, i + 1) for i in range(ends)])
    after = lax.ppermute(mix_in[:2], "sp", [(i + 1, i) for i in range(ends)])
    ff_own = exp_down.shape[1]
    piece = shape((3 * ff_own, width), BF16)
    own = pl.pallas_call(
        pack_kernel,
        out_shape=piece,
        in_specs=[in_hbm()] * 3,
        out_specs=in_hbm(),
        scratch_shapes=[pltpu.VMEM(piece.shape, BF16), pltpu.SemaphoreType.DMA((6,))],
        compiler_params=FULL,
        name="pack",
    )(jnp.swapaxes(exp_gate, 1, 2)[0], jnp.swapaxes(exp_up, 1, 2)[0], exp_down[0])

    def around(part):
        return lax.ppermute(part, "tp", [(i, (i + 2 - 4 * (i % 2)) % tp) for i in range(tp)])

    def across(part):
        return lax.ppermute(part, "tp", [(i, i ^ 1) for i in range(tp)])

    other = across(own)
    r1a = around(own)
    r1b = around(other)
    step = length // SEGS
    lines = SEGS * (step + 8)
    state = shape((length, channels), F32)
    h, p_f, p_b, seg, total = pl.pallas_call(
        scan_kernel,
        out_shape=(state, state, state, shape((32, 128), F32), shape((sp, 8, 128), F32)),
        in_specs=[anywhere()] * 10,
        out_specs=(anywhere(),) * 5,
        scratch_shapes=[
            pltpu.VMEM((length + 16, 128), F32),
            pltpu.VMEM((length, 128), F32),
            pltpu.VMEM((length, 256), BF16),
            pltpu.VMEM((256, 512), BF16),
            pltpu.VMEM((128, 512), BF16),
            pltpu.VMEM((length, 512), F32),
            pltpu.VMEM((lines, 128), F32),
            pltpu.VMEM((lines, 128), F32),
            pltpu.VMEM((lines, 128), F32),
            pltpu.VMEM((lines, 128), F32),
            pltpu.VMEM(mix_in.shape, BF16),
            pltpu.VMEM(before.shape, BF16),
            pltpu.VMEM(after.shape, BF16),
            pltpu.VMEM(conv_w.shape, F32),
            pltpu.VMEM((1, 128), F32),
            pltpu.VMEM(decay_param.shape, F32),
            pltpu.VMEM(recur_gate.shape, F32),
            pltpu.VMEM(recur_bias.shape, F32),
            pltpu.VMEM(input_gate.shape, F32),
            pltpu.VMEM(input_bias.shape, F32),
            pltpu.VMEM(state.shape, F32),
            pltpu.VMEM(state.shape, F32),
            pltpu.VMEM(state.shape, F32),
            pltpu.VMEM((32, 128), F32),
            pltpu.VMEM((sp, 8, 128), F32),
            pltpu.SemaphoreType.DMA((17,)),
        ],
        compiler_params=FULL,
        name="scan",
    )(mix_in, before, after, conv_w, conv_b[None], decay_param, recur_gate, recur_bias, input_gate, input_bias)
    total, r1a = lax.optimization_barrier((total, r1a))
    r2a, e1a = around(r1a), across(r1a)
    totals = lax.all_to_all(total, "sp", split_axis=0, concat_axis=0, tiled=True)
    totals, r1b = lax.optimization_barrier((totals, r1b))
    r2b, e1b = around(r1b), across(r1b)
    mix = pl.pallas_call(
        mix_kernel,
        out_shape=shape((length, channels), BF16),
        in_specs=[anywhere()] * 6,
        out_specs=anywhere(),
        scratch_shapes=[pltpu.VMEM((lines, 128), F32)]
        + [pltpu.VMEM(state.shape, F32)] * 3
        + [
            pltpu.VMEM((32, 128), F32),
            pltpu.VMEM((sp, 8, 128), F32),
            pltpu.VMEM((length, channels), BF16),
            pltpu.VMEM((length, channels), BF16),
            pltpu.SemaphoreType.DMA((8,)),
        ],
        compiler_params=FULL,
        name="mix",
    )
    mixed = mix(h, p_f, p_b, seg, totals, gate_in)
    token_rows = lax.all_to_all(
        mixed.reshape(tp, rows, channels), "tp", split_axis=0, concat_axis=0, tiled=True
    )
    r3a, e2a = around(r2a), across(r2a)
    r3b, e2b = around(r2b), across(r2b)
    first_row = lax.axis_index("tp") * rows
    own_routes = lax.dynamic_slice_in_dim(routes, first_row, rows, 0)
    own_weights = lax.dynamic_slice_in_dim(route_wt, first_row, rows, 0)
    slots = 2 * rows * routes.shape[1]
    project = pl.pallas_call(
        proj_kernel,
        out_shape=(
            shape((rows, width), BF16),
            shape((slots, width), BF16),
            shape((3 * rows, slots), BF16),
        ),
        in_specs=[anywhere()] * 7,
        out_specs=(anywhere(),) * 3,
        scratch_shapes=[
            pltpu.VMEM(token_rows.shape, BF16),
            pltpu.VMEM(out_proj.shape, BF16),
            pltpu.VMEM(residual.shape, BF16),
            pltpu.VMEM(norm_gain.shape, F32),
            pltpu.VMEM((routes.shape[1], rows), jnp.int32),
            pltpu.VMEM(own_routes.shape, jnp.int32),
            pltpu.VMEM(own_weights.shape, F32),
            pltpu.VMEM(residual.shape, BF16),
            pltpu.VMEM((slots, width), BF16),
            pltpu.VMEM((3 * rows, slots), BF16),
            pltpu.SemaphoreType.DMA((20,)),
        ],
        compiler_params=FULL,
        name="proj",
    )
    stream, outgoing, table = project(token_rows, out_proj, residual, norm_gain, own_routes.T, own_routes, own_weights)
    r4, e3a = around(r3a), across(r3a)
    e3b, e4 = across(r3b), across(r4)
    arrived = lax.all_to_all(outgoing.reshape(sp, slots // sp, width), "sp", split_axis=0, concat_axis=0, tiled=True)
    arrived = arrived.reshape(slots, width)

    shares = (own, other, r1a, e1a, r1b, e1b, r2a, e2a, r2b, e2b, r3a, e3a, r3b, e3b, r4, e4)
    experts = pl.pallas_call(
        expert_kernel,
        out_shape=shape((slots, width), BF16),
        in_specs=[anywhere()] * (1 + len(shares)),
        out_specs=anywhere(),
        scratch_shapes=[pltpu.VMEM((len(shares) * ff_own, width), BF16)] * 3
        + [
            pltpu.VMEM((slots, width), BF16),
            pltpu.SemaphoreType.DMA((3 * len(shares),)),
            pltpu.SemaphoreType.DMA((2,)),
        ],
        compiler_params=ROOMY,
        name="experts",
    )
    done = experts(arrived, *shares)
    returned = lax.all_to_all(
        done.reshape(sp, slots // sp, width), "sp", split_axis=0, concat_axis=0, tiled=True
    )
    return pl.pallas_call(
        combine_kernel,
        out_shape=shape((rows, width), BF16),
        in_specs=[anywhere()] * 4,
        out_specs=anywhere(),
        scratch_shapes=[
            pltpu.VMEM((slots, width), BF16),
            pltpu.VMEM((rows, width), BF16),
            pltpu.VMEM(norm_gain.shape, F32),
            pltpu.VMEM((3 * rows, slots), BF16),
            pltpu.VMEM((rows, width), BF16),
            pltpu.SemaphoreType.DMA((5,)),
        ],
        compiler_params=FULL,
        name="combine",
    )(returned.reshape(slots, width), stream, norm_gain, table)


def solution(mesh):
    return jax.shard_map(
        layer,
        mesh=mesh,
        in_specs=(
            P("sp", "tp"),
            P("sp", "tp"),
            P(None, "tp"),
            P("tp"),
            P(None, "tp"),
            P(None, "tp", None, None),
            P(None, "tp"),
            P(None, "tp", None, None),
            P(None, "tp"),
            P(("sp", "tp"), None),
            P(),
            P(),
            P("sp", None),
            P("sp", None),
            P("sp", None, "tp"),
            P("sp", None, "tp"),
            P("sp", "tp", None),
        ),
        out_specs=P(("sp", "tp"), None),
        check_vma=False,
    )
```

```python
import functools

import jax
import jax.numpy as jnp
from jax import lax
from jax.experimental import pallas as pl
from jax.experimental.pallas import tpu as pltpu
from jax.sharding import PartitionSpec as P


EPSILON = 1e-06
F32 = jnp.float32
BF16 = jnp.bfloat16
SEGS = 8
VMEM = pltpu.MemorySpace.VMEM


def whole():
    return pl.BlockSpec(memory_space=VMEM)


FULL = pltpu.CompilerParams(vmem_limit_bytes=67043328)
ROOMY = pltpu.CompilerParams(vmem_limit_bytes=30 * 1024 * 1024)


def anywhere():
    return pl.BlockSpec(memory_space=pl.ANY)


def in_hbm():
    return pl.BlockSpec(memory_space=pltpu.MemorySpace.HBM)


def fetched(sources, buffers, sems, first=0):
    copies = [pltpu.make_async_copy(src, dst, sems.at[first + k]) for k, (src, dst) in enumerate(zip(sources, buffers))]
    for copy in copies:
        copy.start()
    return copies


def one_minus_square(log_decay, decay):
    y = 2.0 * log_decay
    series = 1.0 + y * (1.0 / 7.0)
    for k in (6.0, 5.0, 4.0, 3.0, 2.0):
        series = 1.0 + y * (1.0 / k) * series
    return jnp.where(y > -0.5, -y * series, 1.0 - decay * decay)


def softplus_of(x):
    u = jnp.exp(-jnp.abs(x))
    z = u / (2.0 + u)
    z2 = z * z
    series = jnp.full_like(z, 1.0 / 17.0)
    for k in (15.0, 13.0, 11.0, 9.0, 7.0, 5.0, 3.0, 1.0):
        series = 1.0 / k + z2 * series
    return jnp.maximum(x, 0.0) + 2.0 * z * series


def scan_kernel(
    mix_h, before_h, after_h, conv_w_h, conv_b_h, decay_param_h, recur_gate_h, recur_bias_h, input_gate_h, input_bias_h,
    h_h, p_f_h, p_b_h, seg_h, total_h,
    padded, conv, split, wide, wlow, pre, a_f, b_f, a_b, b_b,
    mix, before, after, conv_w, conv_b, decay_param, recur_gate, recur_bias, input_gate, input_bias,
    h, p_f, p_b, seg, total, sems,
):
    for copy in fetched(
        (
            mix_h, before_h, after_h, conv_w_h, conv_b_h, decay_param_h,
            recur_gate_h, recur_bias_h, input_gate_h, input_bias_h,
        ),
        (mix, before, after, conv_w, conv_b, decay_param, recur_gate, recur_bias, input_gate, input_bias),
        sems,
    ):
        copy.wait()
    length = mix.shape[0]
    step = length // SEGS
    stride = step + 8
    padded[0:8, :] = jnp.zeros((8, 128), F32)
    padded[6:8, :] = before[...].astype(F32)
    padded[8 : 8 + length, :] = mix[...].astype(F32)
    padded[8 + length : 16 + length, :] = jnp.zeros((8, 128), F32)
    padded[8 + length : 10 + length, :] = after[...].astype(F32)
    zero = jnp.zeros((64, 64), F32)
    columns = []
    for sense in range(2):
        for gate in (recur_gate, input_gate):
            columns.append(
                jnp.concatenate(
                    [
                        jnp.concatenate([gate[sense, 0], zero], axis=1),
                        jnp.concatenate([zero, gate[sense, 1]], axis=1),
                    ],
                    axis=0,
                )
            )
    maps = jnp.concatenate(columns, axis=1)
    high = maps.astype(BF16)
    wide[0:128, :] = high
    wide[128:256, :] = high
    wlow[...] = (maps - high.astype(F32)).astype(BF16)

    rows = 64

    def convolve(k, carry):
        at = pl.multiple_of(k * rows, rows)
        out = conv_b[...] + padded[pl.ds(at + 6, rows), :] * conv_w[0:1, :]
        for tap in range(1, 4):
            out = out + padded[pl.ds(at + 6 + tap, rows), :] * conv_w[tap : tap + 1, :]
        conv[pl.ds(at, rows), :] = out
        top = out.astype(BF16)
        split[pl.ds(at, rows), 0:128] = top
        split[pl.ds(at, rows), 128:256] = (out - top.astype(F32)).astype(BF16)
        return carry

    lax.fori_loop(0, length // rows, convolve, 0)
    pre[...] = jnp.dot(split[...], wide[...], preferred_element_type=F32) + jnp.dot(
        split[:, 0:128], wlow[...], preferred_element_type=F32
    )
    rate = -8.0 * softplus_of(-decay_param[...])

    per = step // rows

    def gates(k, carry):
        at = pl.multiple_of(k * rows, rows)
        to = pl.multiple_of((k // per) * stride + (k % per) * rows, 8)
        signal = conv[pl.ds(at, rows), :]
        for sense, (a_ref, b_ref) in enumerate(((a_f, b_f), (a_b, b_b))):
            base = sense * 256
            recur = jax.nn.sigmoid(pre[pl.ds(at, rows), base : base + 128] + recur_bias[sense : sense + 1, :])
            inner = jax.nn.sigmoid(pre[pl.ds(at, rows), base + 128 : base + 256] + input_bias[sense : sense + 1, :])
            log_decay = recur * rate[sense : sense + 1, :]
            decay = jnp.exp(log_decay)
            a_ref[pl.ds(to, rows), :] = decay
            b_ref[pl.ds(to, rows), :] = jnp.sqrt(one_minus_square(log_decay, decay)) * (inner * signal)
        return carry

    lax.fori_loop(0, length // rows, gates, 0)

    def advance(t, carry, meet):
        hf, pf, hb, pb = carry
        back = step - 1 - t
        af = a_f[pl.ds(t, SEGS, stride=stride), :]
        bf = b_f[pl.ds(t, SEGS, stride=stride), :]
        ab = a_b[pl.ds(back, SEGS, stride=stride), :]
        bb = b_b[pl.ds(back, SEGS, stride=stride), :]
        hf = af * hf + bf
        pf = pf * af
        hb = ab * hb + bb
        pb = pb * ab
        here = pl.ds(pl.multiple_of(t * SEGS, SEGS), SEGS)
        there = pl.ds(pl.multiple_of(back * SEGS, SEGS), SEGS)
        h[here, :] = hf + h[here, :] if meet else hf
        h[there, :] = hb + h[there, :] if meet else hb
        p_f[here, :] = pf
        p_b[there, :] = pb
        return hf, pf, hb, pb

    none = jnp.zeros((SEGS, 128), F32)
    ones = jnp.ones((SEGS, 128), F32)
    half = step // 2
    state = (none, ones, none, ones)
    state = lax.fori_loop(0, half, functools.partial(advance, meet=False), state, unroll=8)
    low, high = pl.ds(0, length // 2), pl.ds(length // 2, length // 2)
    sent = fetched((p_f.at[low], p_b.at[high]), (p_f_h.at[low], p_b_h.at[high]), sems, 10)
    hf, pf, hb, pb = lax.fori_loop(half, step, functools.partial(advance, meet=True), state, unroll=8)
    sent += fetched((h, p_f.at[high], p_b.at[low]), (h_h, p_f_h.at[high], p_b_h.at[low]), sems, 12)

    sums = []
    for base, last, p, order in ((0, hf, pf, range(SEGS)), (16, hb, pb, reversed(range(SEGS)))):
        enter = jnp.zeros((1, 128), F32)
        factor = jnp.ones((1, 128), F32)
        for s in order:
            seg[base + s : base + s + 1, :] = enter
            seg[base + 8 + s : base + 9 + s, :] = factor
            enter = p[s : s + 1, :] * enter + last[s : s + 1, :]
            factor = p[s : s + 1, :] * factor
        sums += [factor, enter]
    both = jnp.concatenate(sums + [jnp.zeros((4, 128), F32)], axis=0)
    total[...] = jnp.broadcast_to(both[None], total.shape)
    sent += fetched((seg, total), (seg_h, total_h), sems, 15)
    for copy in sent:
        copy.wait()


def mix_kernel(*refs):
    sources, out_h, natural, buffers, out, sems = refs[:6], refs[6], refs[7], refs[8:14], refs[14], refs[15]
    h, p_f, p_b, seg, totals, gate_in = buffers
    for copy in fetched(sources, buffers, sems):
        copy.wait()
    length = out.shape[0]
    step = length // SEGS
    stride = step + 8
    count = totals.shape[0]
    here = lax.axis_index("sp")
    enter_f = jnp.zeros((1, 128), F32)
    enter_b = jnp.zeros((1, 128), F32)
    for j in range(count):
        enter_f = jnp.where(j < here, totals[j, 0:1, :] * enter_f + totals[j, 1:2, :], enter_f)
        k = count - 1 - j
        enter_b = jnp.where(k > here, totals[k, 2:3, :] * enter_b + totals[k, 3:4, :], enter_b)
    into_f = seg[0:8, :] + seg[8:16, :] * enter_f
    into_b = seg[16:24, :] + seg[24:32, :] * enter_b

    def place(t, carry):
        at = pl.multiple_of(t * SEGS, SEGS)
        rows = pl.ds(at, SEGS)
        natural[pl.ds(t, SEGS, stride=stride), :] = (
            h[rows, :] + p_f[rows, :] * into_f + p_b[rows, :] * into_b
        )
        return carry

    lax.fori_loop(0, step, place, 0, unroll=8)
    for s in range(SEGS):
        gate = gate_in[s * step : (s + 1) * step, :].astype(F32)
        out[s * step : (s + 1) * step, :] = (
            natural[s * stride : s * stride + step, :] * jax.nn.gelu(gate)
        ).astype(BF16)
    (copy,) = fetched((out,), (out_h,), sems, 6)
    copy.wait()


def scaled(values, gain):
    return values * lax.rsqrt(jnp.mean(values * values, axis=-1, keepdims=True) + EPSILON) * gain


def slots_of(first, second, axis, capacity, experts):
    rows = first.size
    ids = lax.broadcasted_iota(jnp.int32, (experts, rows) if axis == 0 else (rows, experts), axis)
    hit0 = (ids == first).astype(F32)
    hit1 = (ids == second).astype(F32)
    r = lax.broadcasted_iota(jnp.int32, (rows, rows), 0)
    c = lax.broadcasted_iota(jnp.int32, (rows, rows), 1)
    both = (hit0 + hit1).astype(BF16)
    if axis == 0:
        earlier = jnp.dot(both, (r < c).astype(BF16), preferred_element_type=F32)
    else:
        earlier = jnp.dot((c < r).astype(BF16), both, preferred_element_type=F32)
    return tuple(
        ids0 * capacity + jnp.sum(hit * earlier, axis=axis, keepdims=True).astype(jnp.int32)
        for ids0, hit in ((first, hit0), (second, hit1))
    )


def proj_kernel(
    mixed_h, weights_h, residual_h, gain_h, routes_h, columns_h, route_wt_h, stream_h, outgoing_h, table_h,
    mixed, weights, residual, gain, routes, columns, route_wt, stream_out, outgoing, table_out, sems,
):
    small = fetched((routes_h, columns_h, route_wt_h), (routes, columns, route_wt), sems)
    (mixed_copy,) = fetched((mixed_h,), (mixed,), sems, 9)
    width = weights.shape[0]
    blocks = 8
    block = width // blocks
    parts = [(weights_h.at[pl.ds(k * block, block)], weights.at[pl.ds(k * block, block)]) for k in range(blocks)]
    loads = fetched(*zip(*parts), sems, 12)
    others = fetched((residual_h, gain_h), (residual, gain), sems, 10)
    rows = residual.shape[0]
    slots = outgoing.shape[0]
    experts = 16
    capacity = slots // experts
    for copy in small:
        copy.wait()
    slot0, slot1 = slots_of(columns[:, 0:1], columns[:, 1:2], 1, capacity, experts)
    places = lax.broadcasted_iota(jnp.int32, (rows, slots), 1)
    table = jnp.where(places == slot0, route_wt[:, 0:1], 0.0) + jnp.where(
        places == slot1, route_wt[:, 1:2], 0.0
    )
    high = table.astype(BF16)
    rest = table - high.astype(F32)
    mid = rest.astype(BF16)
    table_out[0:rows, :] = high
    table_out[rows : 2 * rows, :] = mid
    table_out[2 * rows : 3 * rows, :] = (rest - mid.astype(F32)).astype(BF16)
    sent = fetched((table_out,), (table_h,), sems, 3)
    slot0, slot1 = slots_of(routes[0:1, :], routes[1:2, :], 0, capacity, experts)
    places = lax.broadcasted_iota(jnp.int32, (slots, rows), 0)
    pick = jnp.where(jnp.logical_or(places == slot0, places == slot1), 1.0, 0.0).astype(BF16)
    mixed_copy.wait()
    acc = jnp.zeros(residual.shape, F32)
    per = mixed.shape[0] // blocks
    for k in range(blocks):
        lanes = jnp.concatenate([mixed[k * per + j] for j in range(per)], axis=1)
        loads[k].wait()
        acc = acc + jnp.dot(lanes, weights[k * block : (k + 1) * block, :], preferred_element_type=F32)
    for copy in others:
        copy.wait()
    proj = acc.astype(BF16).astype(F32)
    stream = (residual[...].astype(F32) + scaled(proj, gain[0:1, :])).astype(BF16)
    stream_out[...] = stream
    sent += fetched((stream_out,), (stream_h,), sems, 4)
    normed = scaled(stream.astype(F32), gain[1:2, :]).astype(BF16)
    for k in range(4):
        part = slice(k * width // 4, (k + 1) * width // 4)
        outgoing[:, part] = jnp.dot(pick, normed[:, part], preferred_element_type=F32).astype(BF16)
        sent += fetched([outgoing.at[:, part]], [outgoing_h.at[:, part]], sems, 5 + k)
    for copy in sent:
        copy.wait()


def pack_kernel(gate, up, down, out, buffer, sems):
    ff = gate.shape[0]
    refs = (gate, up, down)
    parts = [pl.ds(j * ff, ff) for j in range(3)]
    inward = fetched(refs, [buffer.at[part] for part in parts], sems)
    outward = []
    for copy, part in zip(inward, parts):
        copy.wait()
        outward += fetched([buffer.at[part]], [out.at[part]], sems, 3 + len(outward))
    for copy in outward:
        copy.wait()


def expert_kernel(*refs):
    tokens, shares = refs[0], refs[1:-7]
    out, gate_w, up_w, down_w, held, sems, extra = refs[-7:]
    (tokens_copy,) = fetched((tokens,), (held,), extra)
    ff = shares[0].shape[0] // 3
    copies = [
        fetched(
            [share.at[pl.ds(j * ff, ff)] for j in range(3)],
            [w.at[pl.ds(at * ff, ff)] for w in (gate_w, up_w, down_w)],
            sems,
            3 * at,
        )
        for at, share in enumerate(shares)
    ]
    tokens_copy.wait()
    x = held[...]
    acc = jnp.zeros(x.shape, F32)
    block = 256
    last = (((1,), (1,)), ((), ()))
    for k in range(len(shares) * ff // block):
        for piece in range(k * block // ff, (k + 1) * block // ff):
            for copy in copies[piece]:
                copy.wait()
        rows = slice(k * block, (k + 1) * block)
        gate = lax.dot_general(x, gate_w[rows, :], last, preferred_element_type=F32)
        up = lax.dot_general(x, up_w[rows, :], last, preferred_element_type=F32)
        hidden = (jax.nn.silu(gate) * up).astype(BF16)
        acc = acc + jnp.dot(hidden, down_w[rows, :], preferred_element_type=F32)
    held[...] = acc.astype(BF16)
    (copy,) = fetched((held,), (out,), extra, 1)
    copy.wait()


def combine_kernel(values, stream, gain, table, out):
    rows = stream.shape[0]
    parts = jnp.dot(table[...], values[...], preferred_element_type=F32)
    mixture = parts[0:rows] + (parts[rows : 2 * rows] + parts[2 * rows : 3 * rows])
    mixture = mixture.astype(BF16).astype(F32)
    out[...] = (stream[...].astype(F32) + scaled(mixture, gain[2:3, :])).astype(BF16)


def shape(dims, dtype):
    return jax.ShapeDtypeStruct(dims, dtype)


def layer(
    mix_in,
    gate_in,
    conv_w,
    conv_b,
    decay_param,
    recur_gate,
    recur_bias,
    input_gate,
    input_bias,
    residual,
    out_proj,
    norm_gain,
    routes,
    route_wt,
    exp_gate,
    exp_up,
    exp_down,
):
    length, channels = mix_in.shape
    rows, width = residual.shape
    sp = lax.axis_size("sp")
    tp = lax.axis_size("tp")
    ends = sp - 1
    before = lax.ppermute(mix_in[length - 2 :], "sp", [(i, i + 1) for i in range(ends)])
    after = lax.ppermute(mix_in[:2], "sp", [(i + 1, i) for i in range(ends)])
    ff_own = exp_down.shape[1]
    piece = shape((3 * ff_own, width), BF16)
    own = pl.pallas_call(
        pack_kernel,
        out_shape=piece,
        in_specs=[in_hbm()] * 3,
        out_specs=in_hbm(),
        scratch_shapes=[pltpu.VMEM(piece.shape, BF16), pltpu.SemaphoreType.DMA((6,))],
        compiler_params=FULL,
        name="pack",
    )(jnp.swapaxes(exp_gate, 1, 2)[0], jnp.swapaxes(exp_up, 1, 2)[0], exp_down[0])

    def around(part):
        return lax.ppermute(part, "tp", [(i, (i + 2 - 4 * (i % 2)) % tp) for i in range(tp)])

    def across(part):
        return lax.ppermute(part, "tp", [(i, i ^ 1) for i in range(tp)])

    other = across(own)
    r1a = around(own)
    r1b = around(other)
    step = length // SEGS
    lines = SEGS * (step + 8)
    state = shape((length, channels), F32)
    h, p_f, p_b, seg, total = pl.pallas_call(
        scan_kernel,
        out_shape=(state, state, state, shape((32, 128), F32), shape((sp, 8, 128), F32)),
        in_specs=[anywhere()] * 10,
        out_specs=(anywhere(),) * 5,
        scratch_shapes=[
            pltpu.VMEM((length + 16, 128), F32),
            pltpu.VMEM((length, 128), F32),
            pltpu.VMEM((length, 256), BF16),
            pltpu.VMEM((256, 512), BF16),
            pltpu.VMEM((128, 512), BF16),
            pltpu.VMEM((length, 512), F32),
            pltpu.VMEM((lines, 128), F32),
            pltpu.VMEM((lines, 128), F32),
            pltpu.VMEM((lines, 128), F32),
            pltpu.VMEM((lines, 128), F32),
            pltpu.VMEM(mix_in.shape, BF16),
            pltpu.VMEM(before.shape, BF16),
            pltpu.VMEM(after.shape, BF16),
            pltpu.VMEM(conv_w.shape, F32),
            pltpu.VMEM((1, 128), F32),
            pltpu.VMEM(decay_param.shape, F32),
            pltpu.VMEM(recur_gate.shape, F32),
            pltpu.VMEM(recur_bias.shape, F32),
            pltpu.VMEM(input_gate.shape, F32),
            pltpu.VMEM(input_bias.shape, F32),
            pltpu.VMEM(state.shape, F32),
            pltpu.VMEM(state.shape, F32),
            pltpu.VMEM(state.shape, F32),
            pltpu.VMEM((32, 128), F32),
            pltpu.VMEM((sp, 8, 128), F32),
            pltpu.SemaphoreType.DMA((17,)),
        ],
        compiler_params=FULL,
        name="scan",
    )(mix_in, before, after, conv_w, conv_b[None], decay_param, recur_gate, recur_bias, input_gate, input_bias)
    total, r1a = lax.optimization_barrier((total, r1a))
    r2a, e1a = around(r1a), across(r1a)
    totals = lax.all_to_all(total, "sp", split_axis=0, concat_axis=0, tiled=True)
    totals, r1b = lax.optimization_barrier((totals, r1b))
    r2b, e1b = around(r1b), across(r1b)
    mix = pl.pallas_call(
        mix_kernel,
        out_shape=shape((length, channels), BF16),
        in_specs=[anywhere()] * 6,
        out_specs=anywhere(),
        scratch_shapes=[pltpu.VMEM((lines, 128), F32)]
        + [pltpu.VMEM(state.shape, F32)] * 3
        + [
            pltpu.VMEM((32, 128), F32),
            pltpu.VMEM((sp, 8, 128), F32),
            pltpu.VMEM((length, channels), BF16),
            pltpu.VMEM((length, channels), BF16),
            pltpu.SemaphoreType.DMA((8,)),
        ],
        compiler_params=FULL,
        name="mix",
    )
    mixed = mix(h, p_f, p_b, seg, totals, gate_in)
    token_rows = lax.all_to_all(
        mixed.reshape(tp, rows, channels), "tp", split_axis=0, concat_axis=0, tiled=True
    )
    r3a, e2a = around(r2a), across(r2a)
    r3b, e2b = around(r2b), across(r2b)
    first_row = lax.axis_index("tp") * rows
    own_routes = lax.dynamic_slice_in_dim(routes, first_row, rows, 0)
    own_weights = lax.dynamic_slice_in_dim(route_wt, first_row, rows, 0)
    slots = 2 * rows * routes.shape[1]
    project = pl.pallas_call(
        proj_kernel,
        out_shape=(
            shape((rows, width), BF16),
            shape((slots, width), BF16),
            shape((3 * rows, slots), BF16),
        ),
        in_specs=[anywhere()] * 7,
        out_specs=(anywhere(),) * 3,
        scratch_shapes=[
            pltpu.VMEM(token_rows.shape, BF16),
            pltpu.VMEM(out_proj.shape, BF16),
            pltpu.VMEM(residual.shape, BF16),
            pltpu.VMEM(norm_gain.shape, F32),
            pltpu.VMEM((routes.shape[1], rows), jnp.int32),
            pltpu.VMEM(own_routes.shape, jnp.int32),
            pltpu.VMEM(own_weights.shape, F32),
            pltpu.VMEM(residual.shape, BF16),
            pltpu.VMEM((slots, width), BF16),
            pltpu.VMEM((3 * rows, slots), BF16),
            pltpu.SemaphoreType.DMA((20,)),
        ],
        compiler_params=FULL,
        name="proj",
    )
    stream, outgoing, table = project(token_rows, out_proj, residual, norm_gain, own_routes.T, own_routes, own_weights)
    r4, e3a = around(r3a), across(r3a)
    e3b, e4 = across(r3b), across(r4)
    arrived = lax.all_to_all(outgoing.reshape(sp, slots // sp, width), "sp", split_axis=0, concat_axis=0, tiled=True)
    arrived = arrived.reshape(slots, width)

    shares = (own, other, r1a, e1a, r1b, e1b, r2a, e2a, r2b, e2b, r3a, e3a, r3b, e3b, r4, e4)
    experts = pl.pallas_call(
        expert_kernel,
        out_shape=shape((slots, width), BF16),
        in_specs=[anywhere()] * (1 + len(shares)),
        out_specs=anywhere(),
        scratch_shapes=[pltpu.VMEM((len(shares) * ff_own, width), BF16)] * 3
        + [
            pltpu.VMEM((slots, width), BF16),
            pltpu.SemaphoreType.DMA((3 * len(shares),)),
            pltpu.SemaphoreType.DMA((2,)),
        ],
        compiler_params=ROOMY,
        name="experts",
    )
    done = experts(arrived, *shares)
    returned = lax.all_to_all(
        done.reshape(sp, slots // sp, width), "sp", split_axis=0, concat_axis=0, tiled=True
    )
    return pl.pallas_call(
        combine_kernel,
        out_shape=shape((rows, width), BF16),
        in_specs=[whole()] * 4,
        out_specs=whole(),
        compiler_params=pltpu.CompilerParams(vmem_limit_bytes=16 * 1024 * 1024),
        name="combine",
    )(returned.reshape(slots, width), stream, norm_gain, table)


def solution(mesh):
    return jax.shard_map(
        layer,
        mesh=mesh,
        in_specs=(
            P("sp", "tp"),
            P("sp", "tp"),
            P(None, "tp"),
            P("tp"),
            P(None, "tp"),
            P(None, "tp", None, None),
            P(None, "tp"),
            P(None, "tp", None, None),
            P(None, "tp"),
            P(("sp", "tp"), None),
            P(),
            P(),
            P("sp", None),
            P("sp", None),
            P("sp", None, "tp"),
            P("sp", None, "tp"),
            P("sp", "tp", None),
        ),
        out_specs=P(("sp", "tp"), None),
        check_vma=False,
    )
```

```python
import functools

import jax
import jax.numpy as jnp
from jax import lax
from jax.experimental import pallas as pl
from jax.experimental.pallas import tpu as pltpu
from jax.sharding import PartitionSpec as P


EPSILON = 1e-06
F32 = jnp.float32
BF16 = jnp.bfloat16
SEGS = 8
VMEM = pltpu.MemorySpace.VMEM


def whole():
    return pl.BlockSpec(memory_space=VMEM)


FULL = pltpu.CompilerParams(vmem_limit_bytes=67043328)
ROOMY = pltpu.CompilerParams(vmem_limit_bytes=40 * 1024 * 1024)


def anywhere():
    return pl.BlockSpec(memory_space=pl.ANY)


def in_hbm():
    return pl.BlockSpec(memory_space=pltpu.MemorySpace.HBM)


def fetched(sources, buffers, sems, first=0):
    copies = [pltpu.make_async_copy(src, dst, sems.at[first + k]) for k, (src, dst) in enumerate(zip(sources, buffers))]
    for copy in copies:
        copy.start()
    return copies


def one_minus_square(log_decay, decay):
    y = 2.0 * log_decay
    series = 1.0 + y * (1.0 / 7.0)
    for k in (6.0, 5.0, 4.0, 3.0, 2.0):
        series = 1.0 + y * (1.0 / k) * series
    return jnp.where(y > -0.5, -y * series, 1.0 - decay * decay)


def softplus_of(x):
    u = jnp.exp(-jnp.abs(x))
    z = u / (2.0 + u)
    z2 = z * z
    series = jnp.full_like(z, 1.0 / 17.0)
    for k in (15.0, 13.0, 11.0, 9.0, 7.0, 5.0, 3.0, 1.0):
        series = 1.0 / k + z2 * series
    return jnp.maximum(x, 0.0) + 2.0 * z * series


def scan_kernel(
    mix_h, before_h, after_h, conv_w_h, conv_b_h, decay_param_h, recur_gate_h, recur_bias_h, input_gate_h, input_bias_h,
    h_h, p_f_h, p_b_h, seg_h, total_h,
    padded, conv, split, wide, pre, a_f, b_f, a_b, b_b,
    mix, before, after, conv_w, conv_b, decay_param, recur_gate, recur_bias, input_gate, input_bias,
    h, p_f, p_b, seg, total, sems,
):
    loads = fetched(
        (
            mix_h, before_h, after_h, conv_w_h, conv_b_h, decay_param_h,
            recur_gate_h, recur_bias_h, input_gate_h, input_bias_h,
        ),
        (mix, before, after, conv_w, conv_b, decay_param, recur_gate, recur_bias, input_gate, input_bias),
        sems,
    )
    for copy in loads[3:]:
        copy.wait()
    length = mix.shape[0]
    step = length // SEGS
    stride = step + 8
    zero = jnp.zeros((64, 64), F32)
    columns = []
    for sense in range(2):
        for gate in (recur_gate, input_gate):
            columns.append(
                jnp.concatenate(
                    [
                        jnp.concatenate([gate[sense, 0], zero], axis=1),
                        jnp.concatenate([zero, gate[sense, 1]], axis=1),
                    ],
                    axis=0,
                )
            )
    maps = jnp.concatenate(columns, axis=1)
    high = maps.astype(BF16)
    wide[0:128, :] = high
    wide[128:256, :] = high
    wide[256:384, :] = (maps - high.astype(F32)).astype(BF16)
    for copy in loads[:3]:
        copy.wait()
    padded[0:8, :] = jnp.zeros((8, 128), F32)
    padded[6:8, :] = before[...].astype(F32)
    padded[8 : 8 + length, :] = mix[...].astype(F32)
    padded[8 + length : 16 + length, :] = jnp.zeros((8, 128), F32)
    padded[8 + length : 10 + length, :] = after[...].astype(F32)

    rows = 64

    def convolve(k, carry):
        at = pl.multiple_of(k * rows, rows)
        out = conv_b[...] + padded[pl.ds(at + 6, rows), :] * conv_w[0:1, :]
        for tap in range(1, 4):
            out = out + padded[pl.ds(at + 6 + tap, rows), :] * conv_w[tap : tap + 1, :]
        conv[pl.ds(at, rows), :] = out
        top = out.astype(BF16)
        split[pl.ds(at, rows), 0:128] = top
        split[pl.ds(at, rows), 128:256] = (out - top.astype(F32)).astype(BF16)
        split[pl.ds(at, rows), 256:384] = top
        return carry

    lax.fori_loop(0, length // rows, convolve, 0)
    pre[...] = jnp.dot(split[...], wide[...], preferred_element_type=F32)
    rate = -8.0 * softplus_of(-decay_param[...])

    per = step // rows

    def gates(k, carry):
        at = pl.multiple_of(k * rows, rows)
        to = pl.multiple_of((k // per) * stride + (k % per) * rows, 8)
        signal = conv[pl.ds(at, rows), :]
        for sense, (a_ref, b_ref) in enumerate(((a_f, b_f), (a_b, b_b))):
            base = sense * 256
            recur = jax.nn.sigmoid(pre[pl.ds(at, rows), base : base + 128] + recur_bias[sense : sense + 1, :])
            inner = jax.nn.sigmoid(pre[pl.ds(at, rows), base + 128 : base + 256] + input_bias[sense : sense + 1, :])
            log_decay = recur * rate[sense : sense + 1, :]
            decay = jnp.exp(log_decay)
            a_ref[pl.ds(to, rows), :] = decay
            b_ref[pl.ds(to, rows), :] = jnp.sqrt(one_minus_square(log_decay, decay)) * (inner * signal)
        return carry

    lax.fori_loop(0, length // rows, gates, 0)

    def advance(t, carry, meet):
        hf, pf, hb, pb = carry
        back = step - 1 - t
        af = a_f[pl.ds(t, SEGS, stride=stride), :]
        bf = b_f[pl.ds(t, SEGS, stride=stride), :]
        ab = a_b[pl.ds(back, SEGS, stride=stride), :]
        bb = b_b[pl.ds(back, SEGS, stride=stride), :]
        hf = af * hf + bf
        pf = pf * af
        hb = ab * hb + bb
        pb = pb * ab
        here = pl.ds(pl.multiple_of(t * SEGS, SEGS), SEGS)
        there = pl.ds(pl.multiple_of(back * SEGS, SEGS), SEGS)
        h[here, :] = hf + h[here, :] if meet else hf
        h[there, :] = hb + h[there, :] if meet else hb
        p_f[here, :] = pf
        p_b[there, :] = pb
        return hf, pf, hb, pb

    none = jnp.zeros((SEGS, 128), F32)
    ones = jnp.ones((SEGS, 128), F32)
    half = step // 2
    state = (none, ones, none, ones)
    state = lax.fori_loop(0, half, functools.partial(advance, meet=False), state, unroll=8)
    low, high = pl.ds(0, length // 2), pl.ds(length // 2, length // 2)
    sent = fetched((p_f.at[low], p_b.at[high]), (p_f_h.at[low], p_b_h.at[high]), sems, 10)
    hf, pf, hb, pb = lax.fori_loop(half, step, functools.partial(advance, meet=True), state, unroll=8)
    sent += fetched((h, p_f.at[high], p_b.at[low]), (h_h, p_f_h.at[high], p_b_h.at[low]), sems, 12)

    sums = []
    for base, last, p, order in ((0, hf, pf, range(SEGS)), (16, hb, pb, reversed(range(SEGS)))):
        enter = jnp.zeros((1, 128), F32)
        factor = jnp.ones((1, 128), F32)
        for s in order:
            seg[base + s : base + s + 1, :] = enter
            seg[base + 8 + s : base + 9 + s, :] = factor
            enter = p[s : s + 1, :] * enter + last[s : s + 1, :]
            factor = p[s : s + 1, :] * factor
        sums += [factor, enter]
    both = jnp.concatenate(sums + [jnp.zeros((4, 128), F32)], axis=0)
    total[...] = jnp.broadcast_to(both[None], total.shape)
    sent += fetched((seg, total), (seg_h, total_h), sems, 15)
    for copy in sent:
        copy.wait()


def mix_kernel(*refs):
    sources, out_h, natural, buffers, out, sems = refs[:6], refs[6], refs[7], refs[8:14], refs[14], refs[15]
    h, p_f, p_b, seg, totals, gate_in = buffers
    for copy in fetched(sources, buffers, sems):
        copy.wait()
    length = out.shape[0]
    step = length // SEGS
    stride = step + 8
    count = totals.shape[0]
    here = lax.axis_index("sp")
    enter_f = jnp.zeros((1, 128), F32)
    enter_b = jnp.zeros((1, 128), F32)
    for j in range(count):
        enter_f = jnp.where(j < here, totals[j, 0:1, :] * enter_f + totals[j, 1:2, :], enter_f)
        k = count - 1 - j
        enter_b = jnp.where(k > here, totals[k, 2:3, :] * enter_b + totals[k, 3:4, :], enter_b)
    into_f = seg[0:8, :] + seg[8:16, :] * enter_f
    into_b = seg[16:24, :] + seg[24:32, :] * enter_b

    def place(t, carry):
        at = pl.multiple_of(t * SEGS, SEGS)
        rows = pl.ds(at, SEGS)
        natural[pl.ds(t, SEGS, stride=stride), :] = (
            h[rows, :] + p_f[rows, :] * into_f + p_b[rows, :] * into_b
        )
        return carry

    lax.fori_loop(0, step, place, 0, unroll=8)
    sent = []
    for s in range(SEGS):
        gate = gate_in[s * step : (s + 1) * step, :].astype(F32)
        out[s * step : (s + 1) * step, :] = (
            natural[s * stride : s * stride + step, :] * jax.nn.gelu(gate)
        ).astype(BF16)
        part = pl.ds(s * step, step)
        sent += fetched((out.at[part],), (out_h.at[part],), sems, 6 + s)
    for copy in sent:
        copy.wait()


def scaled(values, gain):
    return values * lax.rsqrt(jnp.mean(values * values, axis=-1, keepdims=True) + EPSILON) * gain


def slots_of(first, second, axis, capacity, experts):
    rows = first.size
    ids = lax.broadcasted_iota(jnp.int32, (experts, rows) if axis == 0 else (rows, experts), axis)
    hit0 = (ids == first).astype(F32)
    hit1 = (ids == second).astype(F32)
    r = lax.broadcasted_iota(jnp.int32, (rows, rows), 0)
    c = lax.broadcasted_iota(jnp.int32, (rows, rows), 1)
    both = (hit0 + hit1).astype(BF16)
    if axis == 0:
        earlier = jnp.dot(both, (r < c).astype(BF16), preferred_element_type=F32)
    else:
        earlier = jnp.dot((c < r).astype(BF16), both, preferred_element_type=F32)
    return tuple(
        ids0 * capacity + jnp.sum(hit * earlier, axis=axis, keepdims=True).astype(jnp.int32)
        for ids0, hit in ((first, hit0), (second, hit1))
    )


def proj_kernel(
    mixed_h, weights_h, residual_h, gain_h, routes_h, columns_h, route_wt_h, stream_h, outgoing_h, table_h,
    mixed, weights, residual, gain, routes, columns, route_wt, stream_out, outgoing, table_out, sems,
):
    small = fetched((routes_h, columns_h, route_wt_h), (routes, columns, route_wt), sems)
    (mixed_copy,) = fetched((mixed_h,), (mixed,), sems, 9)
    width = weights.shape[0]
    blocks = 8
    block = width // blocks
    parts = [(weights_h.at[pl.ds(k * block, block)], weights.at[pl.ds(k * block, block)]) for k in range(blocks)]
    loads = fetched(*zip(*parts), sems, 12)
    others = fetched((residual_h, gain_h), (residual, gain), sems, 10)
    rows = residual.shape[0]
    slots = outgoing.shape[0]
    experts = 16
    capacity = slots // experts
    for copy in small:
        copy.wait()
    slot0, slot1 = slots_of(columns[:, 0:1], columns[:, 1:2], 1, capacity, experts)
    places = lax.broadcasted_iota(jnp.int32, (rows, slots), 1)
    table = jnp.where(places == slot0, route_wt[:, 0:1], 0.0) + jnp.where(
        places == slot1, route_wt[:, 1:2], 0.0
    )
    high = table.astype(BF16)
    rest = table - high.astype(F32)
    mid = rest.astype(BF16)
    table_out[0:rows, :] = high
    table_out[rows : 2 * rows, :] = mid
    table_out[2 * rows : 3 * rows, :] = (rest - mid.astype(F32)).astype(BF16)
    sent = fetched((table_out,), (table_h,), sems, 3)
    slot0, slot1 = slots_of(routes[0:1, :], routes[1:2, :], 0, capacity, experts)
    places = lax.broadcasted_iota(jnp.int32, (slots, rows), 0)
    pick = jnp.where(jnp.logical_or(places == slot0, places == slot1), 1.0, 0.0).astype(BF16)
    mixed_copy.wait()
    acc = jnp.zeros(residual.shape, F32)
    per = mixed.shape[0] // blocks
    for k in range(blocks):
        lanes = jnp.concatenate([mixed[k * per + j] for j in range(per)], axis=1)
        loads[k].wait()
        acc = acc + jnp.dot(lanes, weights[k * block : (k + 1) * block, :], preferred_element_type=F32)
    for copy in others:
        copy.wait()
    proj = acc.astype(BF16).astype(F32)
    stream = (residual[...].astype(F32) + scaled(proj, gain[0:1, :])).astype(BF16)
    stream_out[...] = stream
    sent += fetched((stream_out,), (stream_h,), sems, 4)
    normed = scaled(stream.astype(F32), gain[1:2, :]).astype(BF16)
    for k in range(4):
        part = slice(k * width // 4, (k + 1) * width // 4)
        outgoing[:, part] = jnp.dot(pick, normed[:, part], preferred_element_type=F32).astype(BF16)
        sent += fetched([outgoing.at[:, part]], [outgoing_h.at[:, part]], sems, 5 + k)
    for copy in sent:
        copy.wait()


def pack_kernel(gate, up, down, out, buffer, sems):
    ff = gate.shape[0]
    refs = (gate, up, down)
    parts = [pl.ds(j * ff, ff) for j in range(3)]
    inward = fetched(refs, [buffer.at[part] for part in parts], sems)
    outward = []
    for copy, part in zip(inward, parts):
        copy.wait()
        outward += fetched([buffer.at[part]], [out.at[part]], sems, 3 + len(outward))
    for copy in outward:
        copy.wait()


def expert_kernel(*refs):
    tokens, ready, shares = refs[0], refs[1:5], refs[5:-5]
    out, gate_w, up_w, down_w, sems = refs[-5:]
    ff = shares[0].shape[0] // 3
    copies = [
        fetched(
            [share.at[pl.ds(j * ff, ff)] for j in range(3)],
            [w.at[pl.ds(at * ff, ff)] for w in (gate_w, up_w, down_w)],
            sems,
            3 * at,
        )
        for at, share in enumerate(shares)
    ]
    x = tokens[...]
    block = len(ready) * ff
    last = (((1,), (1,)), ((), ()))

    def part(gate_rows, up_rows, down_rows):
        gate = lax.dot_general(x, gate_rows, last, preferred_element_type=F32)
        up = lax.dot_general(x, up_rows, last, preferred_element_type=F32)
        hidden = (jax.nn.silu(gate) * up).astype(BF16)
        return jnp.dot(hidden, down_rows, preferred_element_type=F32)

    acc = part(*(jnp.concatenate([p[j * ff : (j + 1) * ff, :] for p in ready], axis=0) for j in range(3)))
    for k in range(len(shares) * ff // block):
        for piece in range(k * block // ff, (k + 1) * block // ff):
            for copy in copies[piece]:
                copy.wait()
        rows = slice(k * block, (k + 1) * block)
        acc = acc + part(gate_w[rows, :], up_w[rows, :], down_w[rows, :])
    out[...] = acc.astype(BF16)


def combine_kernel(values, stream, gain, table, out):
    rows = stream.shape[0]
    parts = jnp.dot(table[...], values[...], preferred_element_type=F32)
    mixture = parts[0:rows] + (parts[rows : 2 * rows] + parts[2 * rows : 3 * rows])
    mixture = mixture.astype(BF16).astype(F32)
    out[...] = (stream[...].astype(F32) + scaled(mixture, gain[2:3, :])).astype(BF16)


def shape(dims, dtype):
    return jax.ShapeDtypeStruct(dims, dtype)


def layer(
    mix_in,
    gate_in,
    conv_w,
    conv_b,
    decay_param,
    recur_gate,
    recur_bias,
    input_gate,
    input_bias,
    residual,
    out_proj,
    norm_gain,
    routes,
    route_wt,
    exp_gate,
    exp_up,
    exp_down,
):
    length, channels = mix_in.shape
    rows, width = residual.shape
    sp = lax.axis_size("sp")
    tp = lax.axis_size("tp")
    ends = sp - 1
    before = lax.ppermute(mix_in[length - 2 :], "sp", [(i, i + 1) for i in range(ends)])
    after = lax.ppermute(mix_in[:2], "sp", [(i + 1, i) for i in range(ends)])
    ff_own = exp_down.shape[1]
    piece = shape((3 * ff_own, width), BF16)
    own = pl.pallas_call(
        pack_kernel,
        out_shape=piece,
        in_specs=[in_hbm()] * 3,
        out_specs=in_hbm(),
        scratch_shapes=[pltpu.VMEM(piece.shape, BF16), pltpu.SemaphoreType.DMA((6,))],
        compiler_params=FULL,
        name="pack",
    )(jnp.swapaxes(exp_gate, 1, 2)[0], jnp.swapaxes(exp_up, 1, 2)[0], exp_down[0])

    def around(part):
        return lax.ppermute(part, "tp", [(i, (i + 2 - 4 * (i % 2)) % tp) for i in range(tp)])

    def across(part):
        return lax.ppermute(part, "tp", [(i, i ^ 1) for i in range(tp)])

    other = across(own)
    r1a = around(own)
    r1b = around(other)
    step = length // SEGS
    lines = SEGS * (step + 8)
    state = shape((length, channels), F32)
    h, p_f, p_b, seg, total = pl.pallas_call(
        scan_kernel,
        out_shape=(state, state, state, shape((32, 128), F32), shape((sp, 8, 128), F32)),
        in_specs=[anywhere()] * 10,
        out_specs=(anywhere(),) * 5,
        scratch_shapes=[
            pltpu.VMEM((length + 16, 128), F32),
            pltpu.VMEM((length, 128), F32),
            pltpu.VMEM((length, 384), BF16),
            pltpu.VMEM((384, 512), BF16),
            pltpu.VMEM((length, 512), F32),
            pltpu.VMEM((lines, 128), F32),
            pltpu.VMEM((lines, 128), F32),
            pltpu.VMEM((lines, 128), F32),
            pltpu.VMEM((lines, 128), F32),
            pltpu.VMEM(mix_in.shape, BF16),
            pltpu.VMEM(before.shape, BF16),
            pltpu.VMEM(after.shape, BF16),
            pltpu.VMEM(conv_w.shape, F32),
            pltpu.VMEM((1, 128), F32),
            pltpu.VMEM(decay_param.shape, F32),
            pltpu.VMEM(recur_gate.shape, F32),
            pltpu.VMEM(recur_bias.shape, F32),
            pltpu.VMEM(input_gate.shape, F32),
            pltpu.VMEM(input_bias.shape, F32),
            pltpu.VMEM(state.shape, F32),
            pltpu.VMEM(state.shape, F32),
            pltpu.VMEM(state.shape, F32),
            pltpu.VMEM((32, 128), F32),
            pltpu.VMEM((sp, 8, 128), F32),
            pltpu.SemaphoreType.DMA((17,)),
        ],
        compiler_params=FULL,
        name="scan",
    )(mix_in, before, after, conv_w, conv_b[None], decay_param, recur_gate, recur_bias, input_gate, input_bias)
    total, r1a = lax.optimization_barrier((total, r1a))
    r2a, e1a = around(r1a), across(r1a)
    totals = lax.all_to_all(total, "sp", split_axis=0, concat_axis=0, tiled=True)
    totals, r1b = lax.optimization_barrier((totals, r1b))
    r2b, e1b = around(r1b), across(r1b)
    mix = pl.pallas_call(
        mix_kernel,
        out_shape=shape((length, channels), BF16),
        in_specs=[anywhere()] * 6,
        out_specs=anywhere(),
        scratch_shapes=[pltpu.VMEM((lines, 128), F32)]
        + [pltpu.VMEM(state.shape, F32)] * 3
        + [
            pltpu.VMEM((32, 128), F32),
            pltpu.VMEM((sp, 8, 128), F32),
            pltpu.VMEM((length, channels), BF16),
            pltpu.VMEM((length, channels), BF16),
            pltpu.SemaphoreType.DMA((14,)),
        ],
        compiler_params=FULL,
        name="mix",
    )
    mixed = mix(h, p_f, p_b, seg, totals, gate_in)
    token_rows = lax.all_to_all(
        mixed.reshape(tp, rows, channels), "tp", split_axis=0, concat_axis=0, tiled=True
    )
    r3a, e2a = around(r2a), across(r2a)
    r3b, e2b = around(r2b), across(r2b)
    first_row = lax.axis_index("tp") * rows
    own_routes = lax.dynamic_slice_in_dim(routes, first_row, rows, 0)
    own_weights = lax.dynamic_slice_in_dim(route_wt, first_row, rows, 0)
    slots = 2 * rows * routes.shape[1]
    project = pl.pallas_call(
        proj_kernel,
        out_shape=(
            shape((rows, width), BF16),
            shape((slots, width), BF16),
            shape((3 * rows, slots), BF16),
        ),
        in_specs=[anywhere()] * 7,
        out_specs=(anywhere(),) * 3,
        scratch_shapes=[
            pltpu.VMEM(token_rows.shape, BF16),
            pltpu.VMEM(out_proj.shape, BF16),
            pltpu.VMEM(residual.shape, BF16),
            pltpu.VMEM(norm_gain.shape, F32),
            pltpu.VMEM((routes.shape[1], rows), jnp.int32),
            pltpu.VMEM(own_routes.shape, jnp.int32),
            pltpu.VMEM(own_weights.shape, F32),
            pltpu.VMEM(residual.shape, BF16),
            pltpu.VMEM((slots, width), BF16),
            pltpu.VMEM((3 * rows, slots), BF16),
            pltpu.SemaphoreType.DMA((20,)),
        ],
        compiler_params=FULL,
        name="proj",
    )
    stream, outgoing, table = project(token_rows, out_proj, residual, norm_gain, own_routes.T, own_routes, own_weights)
    r4, e3a = around(r3a), across(r3a)
    e3b, e4 = across(r3b), across(r4)
    arrived = lax.all_to_all(outgoing.reshape(sp, slots // sp, width), "sp", split_axis=0, concat_axis=0, tiled=True)
    arrived = arrived.reshape(slots, width)

    ready = (e3a, e3b, r4, e4)
    shares = (own, other, r1a, e1a, r1b, e1b, r2a, e2a, r2b, e2b, r3a, r3b)
    experts = pl.pallas_call(
        expert_kernel,
        out_shape=shape((slots, width), BF16),
        in_specs=[whole()] * (1 + len(ready)) + [anywhere()] * len(shares),
        out_specs=whole(),
        scratch_shapes=[pltpu.VMEM((len(shares) * ff_own, width), BF16)] * 3
        + [pltpu.SemaphoreType.DMA((3 * len(shares),))],
        compiler_params=ROOMY,
        name="experts",
    )
    done = experts(arrived, *ready, *shares)
    returned = lax.all_to_all(
        done.reshape(sp, slots // sp, width), "sp", split_axis=0, concat_axis=0, tiled=True
    )
    return pl.pallas_call(
        combine_kernel,
        out_shape=shape((rows, width), BF16),
        in_specs=[whole()] * 4,
        out_specs=whole(),
        compiler_params=pltpu.CompilerParams(vmem_limit_bytes=16 * 1024 * 1024),
        name="combine",
    )(returned.reshape(slots, width), stream, norm_gain, table)


def solution(mesh):
    return jax.shard_map(
        layer,
        mesh=mesh,
        in_specs=(
            P("sp", "tp"),
            P("sp", "tp"),
            P(None, "tp"),
            P("tp"),
            P(None, "tp"),
            P(None, "tp", None, None),
            P(None, "tp"),
            P(None, "tp", None, None),
            P(None, "tp"),
            P(("sp", "tp"), None),
            P(),
            P(),
            P("sp", None),
            P("sp", None),
            P("sp", None, "tp"),
            P("sp", None, "tp"),
            P("sp", "tp", None),
        ),
        out_specs=P(("sp", "tp"), None),
        check_vma=False,
    )
```

```python
import functools

import jax
import jax.numpy as jnp
from jax import lax
from jax.experimental import pallas as pl
from jax.experimental.pallas import tpu as pltpu
from jax.sharding import PartitionSpec as P


EPSILON = 1e-06
F32 = jnp.float32
BF16 = jnp.bfloat16
SEGS = 8
VMEM = pltpu.MemorySpace.VMEM


def whole():
    return pl.BlockSpec(memory_space=VMEM)


FULL = pltpu.CompilerParams(vmem_limit_bytes=67043328)
ROOMY = pltpu.CompilerParams(vmem_limit_bytes=30 * 1024 * 1024)


def anywhere():
    return pl.BlockSpec(memory_space=pl.ANY)


def in_hbm():
    return pl.BlockSpec(memory_space=pltpu.MemorySpace.HBM)


def fetched(sources, buffers, sems, first=0):
    copies = [pltpu.make_async_copy(src, dst, sems.at[first + k]) for k, (src, dst) in enumerate(zip(sources, buffers))]
    for copy in copies:
        copy.start()
    return copies


def one_minus_square(log_decay, decay):
    y = 2.0 * log_decay
    series = 1.0 + y * (1.0 / 7.0)
    for k in (6.0, 5.0, 4.0, 3.0, 2.0):
        series = 1.0 + y * (1.0 / k) * series
    return jnp.where(y > -0.5, -y * series, 1.0 - decay * decay)


def softplus_of(x):
    u = jnp.exp(-jnp.abs(x))
    z = u / (2.0 + u)
    z2 = z * z
    series = jnp.full_like(z, 1.0 / 17.0)
    for k in (15.0, 13.0, 11.0, 9.0, 7.0, 5.0, 3.0, 1.0):
        series = 1.0 / k + z2 * series
    return jnp.maximum(x, 0.0) + 2.0 * z * series


def scan_kernel(
    mix_h, before_h, after_h, conv_w_h, conv_b_h, decay_param_h, recur_gate_h, recur_bias_h, input_gate_h, input_bias_h,
    h_h, p_f_h, p_b_h, seg_h, total_h,
    padded, conv, split, wide, pre, a_f, b_f, a_b, b_b,
    mix, before, after, conv_w, conv_b, decay_param, recur_gate, recur_bias, input_gate, input_bias,
    h, p_f, p_b, seg, total, sems,
):
    loads = fetched(
        (
            mix_h, before_h, after_h, conv_w_h, conv_b_h, decay_param_h,
            recur_gate_h, recur_bias_h, input_gate_h, input_bias_h,
        ),
        (mix, before, after, conv_w, conv_b, decay_param, recur_gate, recur_bias, input_gate, input_bias),
        sems,
    )
    for copy in loads[3:]:
        copy.wait()
    length = mix.shape[0]
    step = length // SEGS
    stride = step + 8
    zero = jnp.zeros((64, 64), F32)
    columns = []
    for sense in range(2):
        for gate in (recur_gate, input_gate):
            columns.append(
                jnp.concatenate(
                    [
                        jnp.concatenate([gate[sense, 0], zero], axis=1),
                        jnp.concatenate([zero, gate[sense, 1]], axis=1),
                    ],
                    axis=0,
                )
            )
    maps = jnp.concatenate(columns, axis=1)
    high = maps.astype(BF16)
    wide[0:128, :] = high
    wide[128:256, :] = high
    wide[256:384, :] = (maps - high.astype(F32)).astype(BF16)
    for copy in loads[:3]:
        copy.wait()
    padded[0:8, :] = jnp.zeros((8, 128), F32)
    padded[6:8, :] = before[...].astype(F32)
    padded[8 : 8 + length, :] = mix[...].astype(F32)
    padded[8 + length : 16 + length, :] = jnp.zeros((8, 128), F32)
    padded[8 + length : 10 + length, :] = after[...].astype(F32)

    rows = 64

    def convolve(k, carry):
        at = pl.multiple_of(k * rows, rows)
        out = conv_b[...] + padded[pl.ds(at + 6, rows), :] * conv_w[0:1, :]
        for tap in range(1, 4):
            out = out + padded[pl.ds(at + 6 + tap, rows), :] * conv_w[tap : tap + 1, :]
        conv[pl.ds(at, rows), :] = out
        top = out.astype(BF16)
        split[pl.ds(at, rows), 0:128] = top
        split[pl.ds(at, rows), 128:256] = (out - top.astype(F32)).astype(BF16)
        split[pl.ds(at, rows), 256:384] = top
        return carry

    lax.fori_loop(0, length // rows, convolve, 0)
    pre[...] = jnp.dot(split[...], wide[...], preferred_element_type=F32)
    rate = -8.0 * softplus_of(-decay_param[...])

    per = step // rows

    def gates(k, carry):
        at = pl.multiple_of(k * rows, rows)
        to = pl.multiple_of((k // per) * stride + (k % per) * rows, 8)
        signal = conv[pl.ds(at, rows), :]
        for sense, (a_ref, b_ref) in enumerate(((a_f, b_f), (a_b, b_b))):
            base = sense * 256
            recur = jax.nn.sigmoid(pre[pl.ds(at, rows), base : base + 128] + recur_bias[sense : sense + 1, :])
            inner = jax.nn.sigmoid(pre[pl.ds(at, rows), base + 128 : base + 256] + input_bias[sense : sense + 1, :])
            log_decay = recur * rate[sense : sense + 1, :]
            decay = jnp.exp(log_decay)
            a_ref[pl.ds(to, rows), :] = decay
            b_ref[pl.ds(to, rows), :] = jnp.sqrt(one_minus_square(log_decay, decay)) * (inner * signal)
        return carry

    lax.fori_loop(0, length // rows, gates, 0)

    def advance(t, carry, meet):
        hf, pf, hb, pb = carry
        back = step - 1 - t
        af = a_f[pl.ds(t, SEGS, stride=stride), :]
        bf = b_f[pl.ds(t, SEGS, stride=stride), :]
        ab = a_b[pl.ds(back, SEGS, stride=stride), :]
        bb = b_b[pl.ds(back, SEGS, stride=stride), :]
        hf = af * hf + bf
        pf = pf * af
        hb = ab * hb + bb
        pb = pb * ab
        here = pl.ds(pl.multiple_of(t * SEGS, SEGS), SEGS)
        there = pl.ds(pl.multiple_of(back * SEGS, SEGS), SEGS)
        h[here, :] = hf + h[here, :] if meet else hf
        h[there, :] = hb + h[there, :] if meet else hb
        p_f[here, :] = pf
        p_b[there, :] = pb
        return hf, pf, hb, pb

    none = jnp.zeros((SEGS, 128), F32)
    ones = jnp.ones((SEGS, 128), F32)
    half = step // 2
    state = (none, ones, none, ones)
    state = lax.fori_loop(0, half, functools.partial(advance, meet=False), state, unroll=8)
    low, high = pl.ds(0, length // 2), pl.ds(length // 2, length // 2)
    sent = fetched((p_f.at[low], p_b.at[high]), (p_f_h.at[low], p_b_h.at[high]), sems, 10)
    hf, pf, hb, pb = lax.fori_loop(half, step, functools.partial(advance, meet=True), state, unroll=8)
    sent += fetched((h, p_f.at[high], p_b.at[low]), (h_h, p_f_h.at[high], p_b_h.at[low]), sems, 12)

    sums = []
    for base, last, p, order in ((0, hf, pf, range(SEGS)), (16, hb, pb, reversed(range(SEGS)))):
        enter = jnp.zeros((1, 128), F32)
        factor = jnp.ones((1, 128), F32)
        for s in order:
            seg[base + s : base + s + 1, :] = enter
            seg[base + 8 + s : base + 9 + s, :] = factor
            enter = p[s : s + 1, :] * enter + last[s : s + 1, :]
            factor = p[s : s + 1, :] * factor
        sums += [factor, enter]
    both = jnp.concatenate(sums + [jnp.zeros((4, 128), F32)], axis=0)
    total[...] = jnp.broadcast_to(both[None], total.shape)
    sent += fetched((seg, total), (seg_h, total_h), sems, 15)
    for copy in sent:
        copy.wait()


def mix_kernel(*refs):
    sources, out_h, natural, buffers, out, sems = refs[:6], refs[6], refs[7], refs[8:14], refs[14], refs[15]
    h, p_f, p_b, seg, totals, gate_in = buffers
    for copy in fetched(sources, buffers, sems):
        copy.wait()
    length = out.shape[0]
    step = length // SEGS
    stride = step + 8
    count = totals.shape[0]
    here = lax.axis_index("sp")
    enter_f = jnp.zeros((1, 128), F32)
    enter_b = jnp.zeros((1, 128), F32)
    for j in range(count):
        enter_f = jnp.where(j < here, totals[j, 0:1, :] * enter_f + totals[j, 1:2, :], enter_f)
        k = count - 1 - j
        enter_b = jnp.where(k > here, totals[k, 2:3, :] * enter_b + totals[k, 3:4, :], enter_b)
    into_f = seg[0:8, :] + seg[8:16, :] * enter_f
    into_b = seg[16:24, :] + seg[24:32, :] * enter_b

    def place(t, carry):
        at = pl.multiple_of(t * SEGS, SEGS)
        rows = pl.ds(at, SEGS)
        natural[pl.ds(t, SEGS, stride=stride), :] = (
            h[rows, :] + p_f[rows, :] * into_f + p_b[rows, :] * into_b
        )
        return carry

    lax.fori_loop(0, step, place, 0, unroll=8)
    sent = []
    for s in range(SEGS):
        gate = gate_in[s * step : (s + 1) * step, :].astype(F32)
        out[s * step : (s + 1) * step, :] = (
            natural[s * stride : s * stride + step, :] * jax.nn.gelu(gate)
        ).astype(BF16)
        part = pl.ds(s * step, step)
        sent += fetched((out.at[part],), (out_h.at[part],), sems, 6 + s)
    for copy in sent:
        copy.wait()


def scaled(values, gain):
    return values * lax.rsqrt(jnp.mean(values * values, axis=-1, keepdims=True) + EPSILON) * gain


def slots_of(first, second, axis, capacity, experts):
    rows = first.size
    ids = lax.broadcasted_iota(jnp.int32, (experts, rows) if axis == 0 else (rows, experts), axis)
    hit0 = (ids == first).astype(F32)
    hit1 = (ids == second).astype(F32)
    r = lax.broadcasted_iota(jnp.int32, (rows, rows), 0)
    c = lax.broadcasted_iota(jnp.int32, (rows, rows), 1)
    both = (hit0 + hit1).astype(BF16)
    if axis == 0:
        earlier = jnp.dot(both, (r < c).astype(BF16), preferred_element_type=F32)
    else:
        earlier = jnp.dot((c < r).astype(BF16), both, preferred_element_type=F32)
    return tuple(
        ids0 * capacity + jnp.sum(hit * earlier, axis=axis, keepdims=True).astype(jnp.int32)
        for ids0, hit in ((first, hit0), (second, hit1))
    )


def proj_kernel(
    mixed_h, weights_h, residual_h, gain_h, routes_h, columns_h, route_wt_h, stream_h, outgoing_h, table_h,
    mixed, weights, residual, gain, routes, columns, route_wt, stream_out, outgoing, table_out, sems,
):
    small = fetched((routes_h, columns_h, route_wt_h), (routes, columns, route_wt), sems)
    (mixed_copy,) = fetched((mixed_h,), (mixed,), sems, 9)
    width = weights.shape[0]
    blocks = 8
    block = width // blocks
    parts = [(weights_h.at[pl.ds(k * block, block)], weights.at[pl.ds(k * block, block)]) for k in range(blocks)]
    loads = fetched(*zip(*parts), sems, 12)
    others = fetched((residual_h, gain_h), (residual, gain), sems, 10)
    rows = residual.shape[0]
    slots = outgoing.shape[0]
    experts = 16
    capacity = slots // experts
    for copy in small:
        copy.wait()
    slot0, slot1 = slots_of(columns[:, 0:1], columns[:, 1:2], 1, capacity, experts)
    places = lax.broadcasted_iota(jnp.int32, (rows, slots), 1)
    table = jnp.where(places == slot0, route_wt[:, 0:1], 0.0) + jnp.where(
        places == slot1, route_wt[:, 1:2], 0.0
    )
    high = table.astype(BF16)
    rest = table - high.astype(F32)
    mid = rest.astype(BF16)
    table_out[0:rows, :] = high
    table_out[rows : 2 * rows, :] = mid
    table_out[2 * rows : 3 * rows, :] = (rest - mid.astype(F32)).astype(BF16)
    sent = fetched((table_out,), (table_h,), sems, 3)
    slot0, slot1 = slots_of(routes[0:1, :], routes[1:2, :], 0, capacity, experts)
    places = lax.broadcasted_iota(jnp.int32, (slots, rows), 0)
    pick = jnp.where(jnp.logical_or(places == slot0, places == slot1), 1.0, 0.0).astype(BF16)
    mixed_copy.wait()
    acc = jnp.zeros(residual.shape, F32)
    per = mixed.shape[0] // blocks
    for k in range(blocks):
        lanes = jnp.concatenate([mixed[k * per + j] for j in range(per)], axis=1)
        loads[k].wait()
        acc = acc + jnp.dot(lanes, weights[k * block : (k + 1) * block, :], preferred_element_type=F32)
    for copy in others:
        copy.wait()
    proj = acc.astype(BF16).astype(F32)
    stream = (residual[...].astype(F32) + scaled(proj, gain[0:1, :])).astype(BF16)
    stream_out[...] = stream
    sent += fetched((stream_out,), (stream_h,), sems, 4)
    normed = scaled(stream.astype(F32), gain[1:2, :]).astype(BF16)
    for k in range(4):
        part = slice(k * width // 4, (k + 1) * width // 4)
        outgoing[:, part] = jnp.dot(pick, normed[:, part], preferred_element_type=F32).astype(BF16)
        sent += fetched([outgoing.at[:, part]], [outgoing_h.at[:, part]], sems, 5 + k)
    for copy in sent:
        copy.wait()


def pack_kernel(gate, up, down, out, buffer, sems):
    ff = gate.shape[0]
    refs = (gate, up, down)
    parts = [pl.ds(j * ff, ff) for j in range(3)]
    inward = fetched(refs, [buffer.at[part] for part in parts], sems)
    outward = []
    for copy, part in zip(inward, parts):
        copy.wait()
        outward += fetched([buffer.at[part]], [out.at[part]], sems, 3 + len(outward))
    for copy in outward:
        copy.wait()


def expert_kernel(*refs):
    tokens, shares = refs[0], refs[1:-5]
    out, gate_w, up_w, down_w, sems = refs[-5:]
    ff = shares[0].shape[0] // 3
    copies = [
        fetched(
            [share.at[pl.ds(j * ff, ff)] for j in range(3)],
            [w.at[pl.ds(at * ff, ff)] for w in (gate_w, up_w, down_w)],
            sems,
            3 * at,
        )
        for at, share in enumerate(shares)
    ]
    x = tokens[...]
    acc = jnp.zeros(x.shape, F32)
    block = 256
    last = (((1,), (1,)), ((), ()))
    for k in range(len(shares) * ff // block):
        for piece in range(k * block // ff, (k + 1) * block // ff):
            for copy in copies[piece]:
                copy.wait()
        rows = slice(k * block, (k + 1) * block)
        gate = lax.dot_general(x, gate_w[rows, :], last, preferred_element_type=F32)
        up = lax.dot_general(x, up_w[rows, :], last, preferred_element_type=F32)
        hidden = (jax.nn.silu(gate) * up).astype(BF16)
        acc = acc + jnp.dot(hidden, down_w[rows, :], preferred_element_type=F32)
    out[...] = acc.astype(BF16)


def combine_kernel(values, stream, gain, table, out):
    rows = stream.shape[0]
    parts = jnp.dot(table[...], values[...], preferred_element_type=F32)
    mixture = parts[0:rows] + (parts[rows : 2 * rows] + parts[2 * rows : 3 * rows])
    mixture = mixture.astype(BF16).astype(F32)
    out[...] = (stream[...].astype(F32) + scaled(mixture, gain[2:3, :])).astype(BF16)


def shape(dims, dtype):
    return jax.ShapeDtypeStruct(dims, dtype)


def layer(
    mix_in,
    gate_in,
    conv_w,
    conv_b,
    decay_param,
    recur_gate,
    recur_bias,
    input_gate,
    input_bias,
    residual,
    out_proj,
    norm_gain,
    routes,
    route_wt,
    exp_gate,
    exp_up,
    exp_down,
):
    length, channels = mix_in.shape
    rows, width = residual.shape
    sp = lax.axis_size("sp")
    tp = lax.axis_size("tp")
    ends = sp - 1
    before = lax.ppermute(mix_in[length - 2 :], "sp", [(i, i + 1) for i in range(ends)])
    after = lax.ppermute(mix_in[:2], "sp", [(i + 1, i) for i in range(ends)])
    ff_own = exp_down.shape[1]
    piece = shape((3 * ff_own, width), BF16)
    own = pl.pallas_call(
        pack_kernel,
        out_shape=piece,
        in_specs=[in_hbm()] * 3,
        out_specs=in_hbm(),
        scratch_shapes=[pltpu.VMEM(piece.shape, BF16), pltpu.SemaphoreType.DMA((6,))],
        compiler_params=FULL,
        name="pack",
    )(jnp.swapaxes(exp_gate, 1, 2)[0], jnp.swapaxes(exp_up, 1, 2)[0], exp_down[0])

    def around(part):
        return lax.ppermute(part, "tp", [(i, (i + 2 - 4 * (i % 2)) % tp) for i in range(tp)])

    def across(part):
        return lax.ppermute(part, "tp", [(i, i ^ 1) for i in range(tp)])

    other = across(own)
    r1a = around(own)
    r1b = around(other)
    step = length // SEGS
    lines = SEGS * (step + 8)
    state = shape((length, channels), F32)
    h, p_f, p_b, seg, total = pl.pallas_call(
        scan_kernel,
        out_shape=(state, state, state, shape((32, 128), F32), shape((sp, 8, 128), F32)),
        in_specs=[anywhere()] * 10,
        out_specs=(anywhere(),) * 5,
        scratch_shapes=[
            pltpu.VMEM((length + 16, 128), F32),
            pltpu.VMEM((length, 128), F32),
            pltpu.VMEM((length, 384), BF16),
            pltpu.VMEM((384, 512), BF16),
            pltpu.VMEM((length, 512), F32),
            pltpu.VMEM((lines, 128), F32),
            pltpu.VMEM((lines, 128), F32),
            pltpu.VMEM((lines, 128), F32),
            pltpu.VMEM((lines, 128), F32),
            pltpu.VMEM(mix_in.shape, BF16),
            pltpu.VMEM(before.shape, BF16),
            pltpu.VMEM(after.shape, BF16),
            pltpu.VMEM(conv_w.shape, F32),
            pltpu.VMEM((1, 128), F32),
            pltpu.VMEM(decay_param.shape, F32),
            pltpu.VMEM(recur_gate.shape, F32),
            pltpu.VMEM(recur_bias.shape, F32),
            pltpu.VMEM(input_gate.shape, F32),
            pltpu.VMEM(input_bias.shape, F32),
            pltpu.VMEM(state.shape, F32),
            pltpu.VMEM(state.shape, F32),
            pltpu.VMEM(state.shape, F32),
            pltpu.VMEM((32, 128), F32),
            pltpu.VMEM((sp, 8, 128), F32),
            pltpu.SemaphoreType.DMA((17,)),
        ],
        compiler_params=FULL,
        name="scan",
    )(mix_in, before, after, conv_w, conv_b[None], decay_param, recur_gate, recur_bias, input_gate, input_bias)
    total, r1a = lax.optimization_barrier((total, r1a))
    r2a, e1a = around(r1a), across(r1a)
    totals = lax.all_to_all(total, "sp", split_axis=0, concat_axis=0, tiled=True)
    totals, r1b = lax.optimization_barrier((totals, r1b))
    r2b, e1b = around(r1b), across(r1b)
    mix = pl.pallas_call(
        mix_kernel,
        out_shape=shape((length, channels), BF16),
        in_specs=[anywhere()] * 6,
        out_specs=anywhere(),
        scratch_shapes=[pltpu.VMEM((lines, 128), F32)]
        + [pltpu.VMEM(state.shape, F32)] * 3
        + [
            pltpu.VMEM((32, 128), F32),
            pltpu.VMEM((sp, 8, 128), F32),
            pltpu.VMEM((length, channels), BF16),
            pltpu.VMEM((length, channels), BF16),
            pltpu.SemaphoreType.DMA((14,)),
        ],
        compiler_params=FULL,
        name="mix",
    )
    mixed = mix(h, p_f, p_b, seg, totals, gate_in)
    token_rows = lax.all_to_all(
        mixed.reshape(tp, rows, channels), "tp", split_axis=0, concat_axis=0, tiled=True
    )
    r3a, e2a = around(r2a), across(r2a)
    r3b, e2b = around(r2b), across(r2b)
    first_row = lax.axis_index("tp") * rows
    own_routes = lax.dynamic_slice_in_dim(routes, first_row, rows, 0)
    own_weights = lax.dynamic_slice_in_dim(route_wt, first_row, rows, 0)
    slots = 2 * rows * routes.shape[1]
    project = pl.pallas_call(
        proj_kernel,
        out_shape=(
            shape((rows, width), BF16),
            shape((slots, width), BF16),
            shape((3 * rows, slots), BF16),
        ),
        in_specs=[anywhere()] * 7,
        out_specs=(anywhere(),) * 3,
        scratch_shapes=[
            pltpu.VMEM(token_rows.shape, BF16),
            pltpu.VMEM(out_proj.shape, BF16),
            pltpu.VMEM(residual.shape, BF16),
            pltpu.VMEM(norm_gain.shape, F32),
            pltpu.VMEM((routes.shape[1], rows), jnp.int32),
            pltpu.VMEM(own_routes.shape, jnp.int32),
            pltpu.VMEM(own_weights.shape, F32),
            pltpu.VMEM(residual.shape, BF16),
            pltpu.VMEM((slots, width), BF16),
            pltpu.VMEM((3 * rows, slots), BF16),
            pltpu.SemaphoreType.DMA((20,)),
        ],
        compiler_params=FULL,
        name="proj",
    )
    stream, outgoing, table = project(token_rows, out_proj, residual, norm_gain, own_routes.T, own_routes, own_weights)
    r4, e3a = around(r3a), across(r3a)
    e3b, e4 = across(r3b), across(r4)
    arrived = lax.all_to_all(outgoing.reshape(sp, slots // sp, width), "sp", split_axis=0, concat_axis=0, tiled=True)
    arrived = arrived.reshape(slots, width)

    shares = (own, other, r1a, e1a, r1b, e1b, r2a, e2a, r2b, e2b, r3a, r3b, e3a, e3b, r4, e4)
    experts = pl.pallas_call(
        expert_kernel,
        out_shape=shape((slots, width), BF16),
        in_specs=[whole()] + [anywhere()] * len(shares),
        out_specs=whole(),
        scratch_shapes=[pltpu.VMEM((len(shares) * ff_own, width), BF16)] * 3
        + [pltpu.SemaphoreType.DMA((3 * len(shares),))],
        compiler_params=ROOMY,
        name="experts",
    )
    done = experts(arrived, *shares)
    returned = lax.all_to_all(
        done.reshape(sp, slots // sp, width), "sp", split_axis=0, concat_axis=0, tiled=True
    )
    return pl.pallas_call(
        combine_kernel,
        out_shape=shape((rows, width), BF16),
        in_specs=[whole()] * 4,
        out_specs=whole(),
        compiler_params=pltpu.CompilerParams(vmem_limit_bytes=16 * 1024 * 1024),
        name="combine",
    )(returned.reshape(slots, width), stream, norm_gain, table)


def solution(mesh):
    return jax.shard_map(
        layer,
        mesh=mesh,
        in_specs=(
            P("sp", "tp"),
            P("sp", "tp"),
            P(None, "tp"),
            P("tp"),
            P(None, "tp"),
            P(None, "tp", None, None),
            P(None, "tp"),
            P(None, "tp", None, None),
            P(None, "tp"),
            P(("sp", "tp"), None),
            P(),
            P(),
            P("sp", None),
            P("sp", None),
            P("sp", None, "tp"),
            P("sp", None, "tp"),
            P("sp", "tp", None),
        ),
        out_specs=P(("sp", "tp"), None),
        check_vma=False,
    )
```
